128 devices in a mesh: kv: 16 (over z, y), tp: 8 (over x, core).
Axes of the slice: x: 4, y: 4, z: 4, core: 2. Of those that a mesh axis runs over, the one named last changes fastest.
Arguments:
- tokens: bfloat16 [16, 4096], P(None, 'kv'), may hold values from -6 to 6
- norm_gain: float32 [4096], P('kv'), may hold values from 0.1 to 1.9
- query_weight: bfloat16 [4096, 2048], P('kv', 'tp'), may hold values from -1 to 1
- key_weight: bfloat16 [4096, 2048], P('kv', 'tp'), may hold values from -0.09375 to 0.09375
- value_weight: bfloat16 [4096, 2048], P('kv', 'tp'), may hold values from -0.09375 to 0.09375
- out_weight: bfloat16 [2048, 4096], P('tp', 'kv'), may hold values from -0.125 to 0.125
- lambdas: float32 [16], P('tp'), may hold values from 0.3 to 0.8
- head_gain: float32 [128], replicated, may hold values from 0.1 to 1.9
- lengths: int32 [16], replicated, may hold values from 1 to 16383, as said below
- key_cache: bfloat16 [16, 16384, 16, 128], P(None, 'kv', 'tp'), may hold values from -48 to 48, as said below
- value_cache: bfloat16 [16, 16384, 16, 128], P(None, 'kv', 'tp'), may hold values from -6 to 6
Outputs:
- attended: bfloat16 [16, 4096], P(None, 'kv')
The draws below stay inside these ranges and needn't reach their ends.
Inputs may be any that keep to these rules, and one draw needn't show every extreme that they name: `lengths`: each sequence has 1 to 16383 cached tokens. `key_cache`: cached keys lie between -48 and 48.
All inputs are finite; a program needn't handle non-finite values.
Results may differ from the reference program's by a relative error of at most 0.012.
The reference program's roundings to bfloat16 on the way (of `normed`, `fresh_value`, `weights` and `head_out`) count: a program that leaves them out, or rounds other values in their place, can miss the bound.
Values may be sent and summed in bfloat16 or wider, within the bound.
No kernel may reach another device: no remote copies, remote signals or barrier semaphores. Data moves between devices by JAX's collectives and lax.ppermute only.
A program may use at most 64 MiB of HBM per device.

```python
import jax
import jax.numpy as jnp
from jax import lax

D = 4096
H = 16
DH = 64
SEQS = 16
POS_DEV = 1024
CACHE_LEN = 16384
N_KV = 16


def token_values(key):
    base = jax.random.fold_in(key, 11)
    drawn = jnp.clip(jax.random.normal(base, (SEQS, D), jnp.float32), -6.0, 6.0)
    return drawn.astype(jnp.bfloat16)


def gain_values(key):
    base = jax.random.fold_in(key, 12)
    drawn = 1.0 + 0.18 * jnp.clip(jax.random.normal(base, (D,), jnp.float32), -5.0, 5.0)
    return drawn


def weight_values(key):
    base = jax.random.fold_in(key, 13)
    whole_shape = (D, H * 2 * DH)
    drawn = jnp.clip(jax.random.normal(base, whole_shape, jnp.float32), -6.0, 6.0)
    return (drawn * D ** (-0.5)).astype(jnp.bfloat16)


def length_values(key):
    base = jax.random.fold_in(key, 14)
    return jax.random.randint(base, (SEQS,), 1, CACHE_LEN).astype(jnp.int32)


def draw_tokens(key, part):
    return token_values(key)


def draw_norm_gain(key, part):
    return gain_values(key)


def draw_query_weight(key, part):
    return weight_values(key)


def draw_lengths(key, part):
    return length_values(key)


def draw_key_cache(key, part):
    base = jax.random.fold_in(key, 15)
    whole_shape = (SEQS, CACHE_LEN, H, 2 * DH)
    drawn = jnp.clip(1.5 * jax.random.normal(base, whole_shape, jnp.float32), -9.0, 9.0)
    return drawn.astype(jnp.bfloat16)


def levels(rng, shape, cuts, low, largest):
    factor_of, own = 1.0, jax.random.fold_in(rng, 6)
    for dim, shards_of in cuts:
        heights = jnp.exp(jax.random.uniform(jax.random.fold_in(own, dim), (shards_of,), jnp.float32, low / len(cuts), largest / len(cuts)))
        factor_of = factor_of * jnp.repeat(heights, shape[dim] // shards_of).reshape([-1 if axis == dim else 1 for axis in range(len(shape))])
    return factor_of


def centred(stream_key, shape, deviation, reach, pieces=(), kind=jnp.bfloat16):
    gain = levels(stream_key, shape, pieces, -0.22, 0.18) if pieces else 1.0
    entries = jax.random.normal(stream_key, shape, jnp.float32) * deviation * gain
    return jnp.minimum(jnp.maximum(entries, -reach), reach).astype(kind)


def setup_inputs(seed: int = 0) -> dict:
    splits = jax.random.split(jax.random.key(seed), 12)
    tokens = draw_tokens(jax.random.fold_in(splits[11], 71), 0)
    norm_gain = draw_norm_gain(jax.random.fold_in(splits[11], 71), 0)
    query_weight = draw_query_weight(jax.random.fold_in(splits[11], 71), 0)
    key_weight = centred(splits[3], (D, H * 2 * DH), D ** -0.5, 0.09375, ((0, 16), (1, 8)))
    value_weight = centred(splits[4], (D, H * 2 * DH), D ** -0.5, 0.09375, ((0, 16), (1, 8)))
    out_weight = centred(splits[5], (H * 2 * DH, D), (H * 2 * DH) ** -0.5, 0.125, ((0, 8), (1, 16)))
    lambdas = jnp.clip(0.3 + 0.5 * jax.random.uniform(splits[6], (H,), jnp.float32) ** levels(splits[6], (H,), ((0, 8),), -0.2, 0.2), 0.3, 0.8)
    head_gain = jnp.clip(1.0 + 0.18 * jax.random.normal(splits[7], (2 * DH,), jnp.float32), 0.1, 1.9)
    lengths = draw_lengths(jax.random.fold_in(splits[11], 71), 0)
    key_cache = draw_key_cache(jax.random.fold_in(splits[11], 71), 0)
    value_cache = centred(splits[10], (SEQS, CACHE_LEN, H, 2 * DH), 1.0, 6.0, ((1, 16), (2, 8)))
    return {"tokens": tokens, "norm_gain": norm_gain, "query_weight": query_weight, "key_weight": key_weight, "value_weight": value_weight, "out_weight": out_weight, "lambdas": lambdas, "head_gain": head_gain, "lengths": lengths, "key_cache": key_cache, "value_cache": value_cache}


epsilon = 1e-05
theta_base = 500000.0
floor_value = -1e+30

def angles_for(positions, width):
    halfway = width // 2
    frequency = theta_base ** (-jnp.arange(halfway, dtype=jnp.float32) / halfway)
    return positions.astype(jnp.float32)[:, None] * frequency[None, :]

def rotate(values_in, angles):
    halfway = values_in.shape[-1] // 2
    cosine = jnp.cos(angles)[:, None, None, :]
    sine_part = jnp.sin(angles)[:, None, None, :]
    former = values_in[..., :halfway]
    latter = values_in[..., halfway:]
    return jnp.concatenate([former * cosine - latter * sine_part, latter * cosine + former * sine_part], axis=-1)

def reference(tokens, norm_gain, query_weight, key_weight, value_weight, out_weight, lambdas, head_gain, lengths, key_cache, value_cache):
    widened = tokens.astype(jnp.float32)
    row_scale = lax.rsqrt(lax.optimization_barrier(jnp.sum(widened * widened, axis=1)) / D + epsilon)
    normed = (widened * norm_gain[None, :]).astype(jnp.bfloat16)

    def project(weight):
        return jnp.dot(normed, weight, preferred_element_type=jnp.float32) * row_scale[:, None]
    angles = angles_for(lengths, DH)
    query = rotate(project(query_weight).reshape(SEQS, H, 2, DH), angles).astype(jnp.bfloat16)
    fresh_key = rotate(project(key_weight).reshape(SEQS, H, 2, DH), angles).astype(jnp.bfloat16)
    fresh_value = project(value_weight).reshape(SEQS, H, 2 * DH).astype(jnp.bfloat16)

    def per_block(block_index):
        offset = block_index * POS_DEV
        positions = offset + jnp.arange(POS_DEV, dtype=jnp.int32)
        key_block = lax.dynamic_slice_in_dim(key_cache, offset, POS_DEV, 1).reshape(SEQS, POS_DEV, H, 2, DH)
        value_block = lax.dynamic_slice_in_dim(value_cache, offset, POS_DEV, 1)
        at_length = positions[None, :] == lengths[:, None]
        key_block = jnp.where(at_length[:, :, None, None, None], fresh_key[:, None], key_block)
        value_block = jnp.where(at_length[:, :, None, None], fresh_value[:, None], value_block)
        scores = jnp.einsum('shjd,sphjd->shjp', query.astype(jnp.float32), key_block.astype(jnp.float32)) * DH ** (-0.5)
        visible = (positions[None, :] <= lengths[:, None])[:, None, None, :]
        masked = jnp.where(visible, scores, floor_value)
        block_max = lax.optimization_barrier(jnp.max(masked, axis=-1))
        weights = jnp.where(visible, jnp.exp(masked - block_max[..., None]), 0.0).astype(jnp.bfloat16)
        block_total = lax.optimization_barrier(jnp.sum(weights.astype(jnp.float32), axis=-1))
        block_values = jnp.einsum('shjp,sphe->shje', weights.astype(jnp.float32), value_block.astype(jnp.float32))
        return (block_max, block_total, block_values)
    maxima, totals, valued = lax.map(per_block, jnp.arange(N_KV, dtype=jnp.int32))
    highest = lax.optimization_barrier(jnp.max(maxima, axis=0))
    factor = jnp.exp(maxima - highest[None])
    total = lax.optimization_barrier(jnp.sum(totals * factor, axis=0))
    weighted = lax.optimization_barrier(jnp.sum(valued * factor[..., None], axis=0))
    mixed_heads = weighted[:, :, 0] / total[:, :, 0, None] - lambdas[None, :, None] * weighted[:, :, 1] / total[:, :, 1, None]
    head_out = mixed_heads * lax.rsqrt(lax.optimization_barrier(jnp.mean(mixed_heads * mixed_heads, axis=-1, keepdims=True)) + epsilon) * head_gain
    head_out = head_out.astype(jnp.bfloat16).reshape(SEQS, H * 2 * DH)
    return jnp.dot(head_out, out_weight, preferred_element_type=jnp.float32).astype(jnp.bfloat16)
```

```python
import jax
import jax.numpy as jnp
from jax import lax
from jax.experimental import pallas as pl
from jax.experimental.pallas import tpu as pltpu
from jax.sharding import PartitionSpec as P

D = 4096
DH = 64
HEADS = 2
SEQS = 16
LANES = 128

epsilon = 1e-05
theta_base = 500000.0
floor_value = -1e30

VM = pl.BlockSpec(memory_space=pltpu.VMEM)
SM = pl.BlockSpec(memory_space=pltpu.SMEM)
ANY = pl.BlockSpec(memory_space=pl.ANY)
F32 = jnp.float32
BF16 = jnp.bfloat16
LOADP = pltpu.CompilerParams(vmem_limit_bytes=30 * 1024 * 1024)
BIG = pltpu.CompilerParams(vmem_limit_bytes=30 * 1024 * 1024)


def iotas(rows):
    shape = (rows, LANES)
    return lax.broadcasted_iota(jnp.int32, shape, 0), lax.broadcasted_iota(jnp.int32, shape, 1)


def project_kernel(tokens, gain, query_weight, key_weight, value_weight, out):
    widened = tokens[...].astype(F32)
    squares = jnp.sum(widened * widened, axis=1, keepdims=True)
    normed = (widened * gain[...]).astype(BF16)
    query = jnp.dot(normed, query_weight[...], preferred_element_type=F32)
    key = jnp.dot(normed, key_weight[...], preferred_element_type=F32)
    value = jnp.dot(normed, value_weight[...], preferred_element_type=F32)
    row, lane = iotas(SEQS)
    square_row = jnp.sum(jnp.where(row == lane, squares, 0.0), axis=0, keepdims=True)
    blank = jnp.zeros((3, LANES), F32)
    for dest in range(SEQS):
        out[dest, 0:16, :] = query[:, :LANES]
        out[dest, 16:32, :] = query[:, LANES:]
        out[dest, 32:40, :] = jnp.concatenate(
            [
                square_row,
                key[dest : dest + 1, :LANES],
                key[dest : dest + 1, LANES:],
                value[dest : dest + 1, :LANES],
                value[dest : dest + 1, LANES:],
                blank,
            ],
            axis=0,
        )


def load_kernel(key_in, value_in, key_out, value_out, sems):
    pieces = 4
    size = SEQS // pieces
    copies = []
    for n in range(pieces):
        part = pl.ds(n * size, size)
        copies.append(pltpu.make_async_copy(key_in.at[part], key_out.at[part], sems.at[0, n]))
        copies.append(pltpu.make_async_copy(value_in.at[part], value_out.at[part], sems.at[1, n]))
    for copy in copies:
        copy.start()
    for copy in copies:
        copy.wait()


def turned(x, cosine, sine):
    lane = lax.broadcasted_iota(jnp.int32, x.shape, 1)
    partner = jnp.where(
        (lane // 32) % 2 == 0, pltpu.roll(x, LANES - 32, 1), pltpu.roll(x, 32, 1)
    )
    return (x * cosine + partner * sine).astype(BF16)


def attend_kernel(lengths, own, got, cosine, sine, keys, values, out, query_rows, scale_rows):
    me = own[0]
    base = me * 1024
    summed = jnp.sum(got[...], axis=0)
    row, lane = iotas(SEQS)
    squares = jnp.sum(jnp.where(row == lane, summed[32:33, :], 0.0), axis=1, keepdims=True)
    scaling = jnp.broadcast_to(lax.rsqrt(squares / D + epsilon), (SEQS, LANES))
    scale_rows[...] = scaling
    for head in range(HEADS):
        turned_query = turned(
            summed[16 * head : 16 * head + 16, :] * scaling, cosine[...], sine[...]
        )
        query_rows[head * SEQS : (head + 1) * SEQS, :] = turned_query.astype(F32)
    sub, lane8 = iotas(8)
    map_lanes = (lane8 // DH) == (sub % 2)
    columns = lax.broadcasted_iota(jnp.int32, (8, 2048), 1)
    subs = lax.broadcasted_iota(jnp.int32, (8, 2048), 0)
    own_head = (columns % 2) == ((subs // 2) % 2)
    maxima = jnp.zeros((8, LANES), F32)
    totals = jnp.zeros((8, LANES), F32)
    for pair in range(SEQS // 2):
        first, second = 2 * pair, 2 * pair + 1

        def row_of(head, seq):
            at = head * SEQS + seq
            return jnp.broadcast_to(query_rows[at : at + 1, :], (8, LANES))

        left = jnp.where(sub < 2, row_of(0, first), row_of(1, first))
        left = jnp.where(map_lanes & (sub < 4), left, 0.0)
        right = jnp.where(sub < 6, row_of(0, second), row_of(1, second))
        right = jnp.where(map_lanes & (sub >= 4), right, 0.0)
        queries = jnp.concatenate([left, right], axis=1).astype(BF16)
        both_keys = jnp.concatenate([keys[first], keys[second]], axis=1)
        scores = lax.dot_general(
            queries, both_keys, (((1,), (1,)), ((), ())), preferred_element_type=F32
        ) * DH ** (-0.5)
        limit = jnp.where(
            subs[:, :1] < 4, 2 * (lengths[first] - base), 2 * (lengths[second] - base)
        )
        visible = own_head & (columns < limit)
        masked = jnp.where(visible, scores, floor_value)
        highest = jnp.max(masked, axis=1, keepdims=True)
        weights = jnp.where(visible, jnp.exp(masked - highest), 0.0).astype(BF16)
        total = jnp.sum(weights.astype(F32), axis=1, keepdims=True)
        both_values = jnp.concatenate([values[first], values[second]], axis=1)
        valued = jnp.dot(weights, both_values, preferred_element_type=F32)
        valued = jnp.where(sub < 4, valued[:, :LANES], valued[:, LANES:])
        place = lane8 == pair * 8 + sub
        maxima = maxima + jnp.where(place, highest, 0.0)
        totals = totals + jnp.where(place, total, 0.0)
        for dest in range(SEQS):
            out[dest, pair * 8 : pair * 8 + 8, :] = valued
    scale = scale_rows[pl.ds(me, 1), :]
    row_cosine = cosine[pl.ds(me, 1), :]
    row_sine = sine[pl.ds(me, 1), :]
    lane1 = lax.broadcasted_iota(jnp.int32, (1, LANES), 1)
    fresh_scores = jnp.zeros((1, LANES), F32)
    for head in range(HEADS):
        query = query_rows[pl.ds(head * SEQS + me, 1), :]
        fresh_key = turned(summed[33 + head : 34 + head, :] * scale, row_cosine, row_sine)
        product = query * fresh_key.astype(F32)
        for side in range(2):
            score = jnp.sum(
                jnp.where(lane1 // DH == side, product, 0.0), axis=1, keepdims=True
            ) * DH ** (-0.5)
            at = me * 4 + head * 2 + side
            fresh_scores = fresh_scores + jnp.where(lane1 == at, score, 0.0)
    fresh_value = (summed[35:37, :] * scale).astype(BF16).astype(F32)
    tail = jnp.concatenate(
        [
            jnp.sum(maxima, axis=0, keepdims=True),
            jnp.sum(totals, axis=0, keepdims=True),
            fresh_scores,
            fresh_value,
            jnp.zeros((3, LANES), F32),
        ],
        axis=0,
    )
    for dest in range(SEQS):
        out[dest, 64:72, :] = tail


def finish_kernel(got, block, share, head_gain, out_weight, out, factors, joined):
    rows16, _ = iotas(SEQS)
    maxima = got[:, 64, :]
    totals = got[:, 65, :]
    fresh = jnp.sum(got[:, 66, :], axis=0, keepdims=True)
    in_block = jnp.max(
        jnp.where(rows16 == block[...], maxima, floor_value), axis=0, keepdims=True
    )
    in_block = jnp.maximum(in_block, fresh)
    top = jnp.maximum(jnp.max(maxima, axis=0, keepdims=True), fresh)
    factor = jnp.exp(maxima - top)
    fresh_factor = jnp.exp(fresh - in_block).astype(BF16).astype(F32) * jnp.exp(in_block - top)
    total = jnp.sum(totals * factor, axis=0, keepdims=True) + fresh_factor
    part = share[...] / total
    factors[...] = jnp.zeros((LANES, LANES), F32)
    factors[0:SEQS, :] = factor * part
    factors[SEQS : SEQS + 1, :] = fresh_factor * part
    columns = factors[...].T
    sub, _ = iotas(8)
    for pair in range(SEQS // 2):
        at = pl.ds(pair * 8, 8)

        def row_of(head, seq):
            return jnp.broadcast_to(got[seq, 67 + head : 68 + head, :], (8, LANES))

        first, second = 2 * pair, 2 * pair + 1
        fresh_value = jnp.where(
            sub < 4,
            jnp.where(sub < 2, row_of(0, first), row_of(1, first)),
            jnp.where(sub < 6, row_of(0, second), row_of(1, second)),
        )
        here = columns[pair * 8 : pair * 8 + 8, :]
        joint = here[:, SEQS : SEQS + 1] * fresh_value
        for peer in range(SEQS):
            joint = joint + here[:, peer : peer + 1] * got[peer, at, :]
        joined[at, :] = joint
    sides = []
    for head in range(HEADS):
        mixed = joined[pl.ds(2 * head, SEQS, 4), :] + joined[pl.ds(2 * head + 1, SEQS, 4), :]
        mean = jnp.mean(mixed * mixed, axis=1, keepdims=True)
        sides.append((mixed * lax.rsqrt(mean + epsilon) * head_gain[...]).astype(BF16))
    head_out = jnp.concatenate(sides, axis=1)
    partial_out = jnp.dot(head_out, out_weight[...], preferred_element_type=F32)
    for dest in range(8):
        out[dest] = partial_out


def local(
    tokens,
    norm_gain,
    query_weight,
    key_weight,
    value_weight,
    out_weight,
    lambdas,
    head_gain,
    lengths,
    key_cache,
    value_cache,
):
    sent = pl.pallas_call(
        project_kernel,
        in_specs=[VM] * 5,
        out_specs=VM,
        out_shape=jax.ShapeDtypeStruct((SEQS, 40, LANES), F32),
        name="project",
    )(tokens, norm_gain.reshape(1, -1), query_weight, key_weight, value_weight)
    got = lax.all_to_all(sent, "kv", split_axis=0, concat_axis=0, tiled=True)
    cache_shape = (SEQS, 2048, LANES)
    keys, values = pl.pallas_call(
        load_kernel,
        in_specs=[ANY, ANY],
        out_specs=[VM, VM],
        out_shape=[pltpu.VMEM(cache_shape, BF16), pltpu.VMEM(cache_shape, BF16)],
        scratch_shapes=[pltpu.SemaphoreType.DMA((2, 4))],
        compiler_params=LOADP,
        name="load",
    )(key_cache.reshape(cache_shape), value_cache.reshape(cache_shape))
    halfway = DH // 2
    frequency = theta_base ** (-jnp.arange(halfway, dtype=F32) / halfway)
    angles = lengths.astype(F32)[:, None] * frequency[None, :]
    cosine = jnp.tile(jnp.cos(angles), (1, 4))
    sine = jnp.sin(angles)
    sine = jnp.tile(jnp.concatenate([-sine, sine], axis=1), (1, 2))
    own = lax.axis_index("kv").astype(jnp.int32).reshape(1)
    shared = pl.pallas_call(
        attend_kernel,
        in_specs=[SM, SM, VM, VM, VM, VM, VM],
        out_specs=VM,
        out_shape=jax.ShapeDtypeStruct((SEQS, 72, LANES), F32),
        scratch_shapes=[pltpu.VMEM((32, LANES), F32), pltpu.VMEM((SEQS, LANES), F32)],
        compiler_params=BIG,
        name="attend",
    )(lengths, own, got, cosine, sine, keys, values)
    everyone = lax.all_to_all(shared, "kv", split_axis=0, concat_axis=0, tiled=True)
    block = jnp.pad(jnp.repeat(lengths // 1024, 4), (0, 64)).reshape(1, LANES)
    share = jnp.tile(
        jnp.stack([jnp.ones_like(lambdas), -lambdas], axis=1).reshape(1, 4), (1, 32)
    )
    partial_out = pl.pallas_call(
        finish_kernel,
        in_specs=[VM] * 5,
        out_specs=VM,
        out_shape=jax.ShapeDtypeStruct((8, SEQS, 256), F32),
        scratch_shapes=[pltpu.VMEM((LANES, LANES), F32), pltpu.VMEM((64, LANES), F32)],
        name="finish",
    )(everyone, block, share, head_gain.reshape(1, -1), out_weight)
    shares = lax.all_to_all(partial_out, "tp", split_axis=0, concat_axis=0, tiled=True)
    return shares.sum(axis=0).astype(BF16)


def solution(mesh):
    return jax.shard_map(
        local,
        mesh=mesh,
        in_specs=(
            P(None, "kv"),
            P("kv"),
            P("kv", "tp"),
            P("kv", "tp"),
            P("kv", "tp"),
            P("tp", "kv"),
            P("tp"),
            P(),
            P(),
            P(None, "kv", "tp", None),
            P(None, "kv", "tp", None),
        ),
        out_specs=P(None, "kv"),
        check_vma=False,
    )
```

```python
import jax
import jax.numpy as jnp
from jax import lax
from jax.experimental import pallas as pl
from jax.experimental.pallas import tpu as pltpu
from jax.sharding import PartitionSpec as P

D = 4096
DH = 64
HEADS = 2
SEQS = 16
LANES = 128

epsilon = 1e-05
theta_base = 500000.0
floor_value = -1e30

VM = pl.BlockSpec(memory_space=pltpu.VMEM)
SM = pl.BlockSpec(memory_space=pltpu.SMEM)
ANY = pl.BlockSpec(memory_space=pl.ANY)
F32 = jnp.float32
BF16 = jnp.bfloat16
SMALL = pltpu.CompilerParams(vmem_limit_bytes=8 * 1024 * 1024)
BIG = pltpu.CompilerParams(vmem_limit_bytes=30 * 1024 * 1024)


def iotas(rows):
    shape = (rows, LANES)
    return lax.broadcasted_iota(jnp.int32, shape, 0), lax.broadcasted_iota(jnp.int32, shape, 1)


def project_kernel(tokens, gain, query_weight, key_weight, value_weight, out):
    widened = tokens[...].astype(F32)
    squares = jnp.sum(widened * widened, axis=1, keepdims=True)
    normed = (widened * gain[...]).astype(BF16)
    query = jnp.dot(normed, query_weight[...], preferred_element_type=F32)
    key = jnp.dot(normed, key_weight[...], preferred_element_type=F32)
    value = jnp.dot(normed, value_weight[...], preferred_element_type=F32)
    row, lane = iotas(SEQS)
    square_row = jnp.sum(jnp.where(row == lane, squares, 0.0), axis=0, keepdims=True)
    blank = jnp.zeros((3, LANES), F32)
    for dest in range(SEQS):
        out[dest, 0:16, :] = query[:, :LANES]
        out[dest, 16:32, :] = query[:, LANES:]
        out[dest, 32:40, :] = jnp.concatenate(
            [
                square_row,
                key[dest : dest + 1, :LANES],
                key[dest : dest + 1, LANES:],
                value[dest : dest + 1, :LANES],
                value[dest : dest + 1, LANES:],
                blank,
            ],
            axis=0,
        )


def turned(x, cosine, sine):
    lane = lax.broadcasted_iota(jnp.int32, x.shape, 1)
    partner = jnp.where(
        (lane // 32) % 2 == 0, pltpu.roll(x, LANES - 32, 1), pltpu.roll(x, 32, 1)
    )
    return (x * cosine + partner * sine).astype(BF16)


def attend_kernel(
    lengths, own, got, cosine, sine, keys_in, values_in, out, keys, values, arrived, query_rows,
    scale_rows, score_rows, weight_rows
):
    copies = []
    for kind, (source, target) in enumerate(((keys_in, keys), (values_in, values))):
        for seq in range(SEQS):
            copies.append(
                pltpu.make_async_copy(source.at[seq], target.at[seq], arrived.at[kind, seq])
            )
    for copy in copies:
        copy.start()
    me = own[0]
    base = me * 1024
    summed = jnp.sum(got[...], axis=0)
    row, lane = iotas(SEQS)
    squares = jnp.sum(jnp.where(row == lane, summed[32:33, :], 0.0), axis=1, keepdims=True)
    scaling = jnp.broadcast_to(lax.rsqrt(squares / D + epsilon), (SEQS, LANES))
    scale_rows[...] = scaling
    for head in range(HEADS):
        turned_query = turned(
            summed[16 * head : 16 * head + 16, :] * scaling, cosine[...], sine[...]
        )
        query_rows[head * SEQS : (head + 1) * SEQS, :] = turned_query.astype(F32)
    sub, lane8 = iotas(8)
    map_lanes = (lane8 // DH) == (sub % 2)
    limits = []
    for pair in range(SEQS // 2):
        first, second = 2 * pair, 2 * pair + 1

        def row_of(head, seq):
            at = head * SEQS + seq
            return jnp.broadcast_to(query_rows[at : at + 1, :], (8, LANES))

        left = jnp.where(sub < 2, row_of(0, first), row_of(1, first))
        left = jnp.where(map_lanes & (sub < 4), left, 0.0)
        right = jnp.where(sub < 6, row_of(0, second), row_of(1, second))
        right = jnp.where(map_lanes & (sub >= 4), right, 0.0)
        queries = jnp.concatenate([left, right], axis=1).astype(BF16)
        copies[first].wait()
        copies[second].wait()
        both_keys = jnp.concatenate([keys[first], keys[second]], axis=1)
        score_rows[pair * 8 : pair * 8 + 8, :] = lax.dot_general(
            queries, both_keys, (((1,), (1,)), ((), ())), preferred_element_type=F32
        )
    columns = lax.broadcasted_iota(jnp.int32, (8, 2048), 1)
    subs = lax.broadcasted_iota(jnp.int32, (8, 2048), 0)
    own_head = (columns % 2) == ((subs // 2) % 2)
    maxima = jnp.zeros((8, LANES), F32)
    totals = jnp.zeros((8, LANES), F32)
    for pair in range(SEQS // 2):
        first, second = 2 * pair, 2 * pair + 1
        at = slice(pair * 8, pair * 8 + 8)
        limit = jnp.where(
            subs[:, :1] < 4, 2 * (lengths[first] - base), 2 * (lengths[second] - base)
        )
        visible = own_head & (columns < limit)
        masked = jnp.where(visible, score_rows[at, :] * DH ** (-0.5), floor_value)
        highest = jnp.max(masked, axis=1, keepdims=True)
        weights = jnp.where(visible, jnp.exp(masked - highest), 0.0).astype(BF16)
        total = jnp.sum(weights.astype(F32), axis=1, keepdims=True)
        weight_rows[at, :] = weights
        place = lane8 == pair * 8 + sub
        maxima = maxima + jnp.where(place, highest, 0.0)
        totals = totals + jnp.where(place, total, 0.0)
    scale = scale_rows[pl.ds(me, 1), :]
    row_cosine = cosine[pl.ds(me, 1), :]
    row_sine = sine[pl.ds(me, 1), :]
    lane1 = lax.broadcasted_iota(jnp.int32, (1, LANES), 1)
    fresh_scores = jnp.zeros((1, LANES), F32)
    for head in range(HEADS):
        query = query_rows[pl.ds(head * SEQS + me, 1), :]
        fresh_key = turned(summed[33 + head : 34 + head, :] * scale, row_cosine, row_sine)
        product = query * fresh_key.astype(F32)
        for side in range(2):
            score = jnp.sum(
                jnp.where(lane1 // DH == side, product, 0.0), axis=1, keepdims=True
            ) * DH ** (-0.5)
            at = me * 4 + head * 2 + side
            fresh_scores = fresh_scores + jnp.where(lane1 == at, score, 0.0)
    fresh_value = (summed[35:37, :] * scale).astype(BF16).astype(F32)
    tail = jnp.concatenate(
        [
            *thirds(jnp.sum(maxima, axis=0, keepdims=True)),
            *thirds(jnp.sum(totals, axis=0, keepdims=True)),
            *thirds(fresh_scores),
            fresh_value,
            jnp.zeros((5, LANES), F32),
        ],
        axis=0,
    ).astype(BF16)
    for dest in range(SEQS):
        out[dest, 64:80, :] = tail
    for two in range(SEQS // 4):
        parts = []
        for pair in (2 * two, 2 * two + 1):
            first, second = 2 * pair, 2 * pair + 1
            copies[SEQS + first].wait()
            copies[SEQS + second].wait()
            both_values = jnp.concatenate([values[first], values[second]], axis=1)
            valued = jnp.dot(
                weight_rows[pair * 8 : pair * 8 + 8, :],
                both_values,
                preferred_element_type=F32,
            )
            parts.append(jnp.where(sub < 4, valued[:, :LANES], valued[:, LANES:]))
        sixteen = jnp.concatenate(parts, axis=0).astype(BF16)
        for dest in range(SEQS):
            out[dest, two * 16 : two * 16 + 16, :] = sixteen


def thirds(x):
    high = x.astype(BF16).astype(F32)
    middle = (x - high).astype(BF16).astype(F32)
    return high, middle, x - high - middle


def finish_kernel(got, block, share, head_gain, out_weight, out, factors, joined):
    rows16, _ = iotas(SEQS)
    tails = got[:, 64:80, :].astype(F32)

    def whole(at):
        return tails[:, at, :] + tails[:, at + 1, :] + tails[:, at + 2, :]

    maxima = whole(0)
    totals = whole(3)
    fresh = jnp.sum(whole(6), axis=0, keepdims=True)
    in_block = jnp.max(
        jnp.where(rows16 == block[...], maxima, floor_value), axis=0, keepdims=True
    )
    in_block = jnp.maximum(in_block, fresh)
    top = jnp.maximum(jnp.max(maxima, axis=0, keepdims=True), fresh)
    factor = jnp.exp(maxima - top)
    fresh_factor = jnp.exp(fresh - in_block).astype(BF16).astype(F32) * jnp.exp(in_block - top)
    total = jnp.sum(totals * factor, axis=0, keepdims=True) + fresh_factor
    part = share[...] / total
    factors[...] = jnp.zeros((LANES, LANES), F32)
    factors[0:SEQS, :] = factor * part
    factors[SEQS : SEQS + 1, :] = fresh_factor * part
    columns = factors[...].T
    sub, _ = iotas(16)
    for four in range(SEQS // 4):
        here = columns[four * 16 : four * 16 + 16, :]
        fresh_value = jnp.zeros((16, LANES), F32)
        for n in range(8):
            line = tails[four * 4 + n // 2, 9 + n % 2 : 10 + n % 2, :]
            fresh_value = jnp.where(sub // 2 == n, line, fresh_value)
        joint = here[:, SEQS : SEQS + 1] * fresh_value
        for peer in range(SEQS):
            joint = joint + here[:, peer : peer + 1] * got[
                peer, four * 16 : four * 16 + 16, :
            ].astype(F32)
        joined[four * 16 : four * 16 + 16, :] = joint
    sides = []
    for head in range(HEADS):
        mixed = joined[pl.ds(2 * head, SEQS, 4), :] + joined[pl.ds(2 * head + 1, SEQS, 4), :]
        mean = jnp.mean(mixed * mixed, axis=1, keepdims=True)
        sides.append((mixed * lax.rsqrt(mean + epsilon) * head_gain[...]).astype(BF16))
    head_out = jnp.concatenate(sides, axis=1)
    partial_out = jnp.dot(head_out, out_weight[...], preferred_element_type=F32)
    for dest in range(8):
        out[dest] = partial_out


def local(
    tokens,
    norm_gain,
    query_weight,
    key_weight,
    value_weight,
    out_weight,
    lambdas,
    head_gain,
    lengths,
    key_cache,
    value_cache,
):
    sent = pl.pallas_call(
        project_kernel,
        in_specs=[VM] * 5,
        out_specs=VM,
        out_shape=jax.ShapeDtypeStruct((SEQS, 40, LANES), F32),
        compiler_params=SMALL,
        name="project",
    )(tokens, norm_gain.reshape(1, -1), query_weight, key_weight, value_weight)
    got = lax.all_to_all(sent, "kv", split_axis=0, concat_axis=0, tiled=True)
    cache_shape = (SEQS, 2048, LANES)
    halfway = DH // 2
    frequency = theta_base ** (-jnp.arange(halfway, dtype=F32) / halfway)
    angles = lengths.astype(F32)[:, None] * frequency[None, :]
    cosine = jnp.tile(jnp.cos(angles), (1, 4))
    sine = jnp.sin(angles)
    sine = jnp.tile(jnp.concatenate([-sine, sine], axis=1), (1, 2))
    own = lax.axis_index("kv").astype(jnp.int32).reshape(1)
    shared = pl.pallas_call(
        attend_kernel,
        in_specs=[SM, SM, VM, VM, VM, ANY, ANY],
        out_specs=VM,
        out_shape=jax.ShapeDtypeStruct((SEQS, 80, LANES), BF16),
        scratch_shapes=[
            pltpu.VMEM(cache_shape, BF16),
            pltpu.VMEM(cache_shape, BF16),
            pltpu.SemaphoreType.DMA((2, SEQS)),
            pltpu.VMEM((32, LANES), F32),
            pltpu.VMEM((SEQS, LANES), F32),
            pltpu.VMEM((64, 2048), F32),
            pltpu.VMEM((64, 2048), BF16),
        ],
        compiler_params=BIG,
        name="attend",
    )(
        lengths,
        own,
        got,
        cosine,
        sine,
        key_cache.reshape(cache_shape),
        value_cache.reshape(cache_shape),
    )
    everyone = lax.all_to_all(shared, "kv", split_axis=0, concat_axis=0, tiled=True)
    block = jnp.pad(jnp.repeat(lengths // 1024, 4), (0, 64)).reshape(1, LANES)
    share = jnp.tile(
        jnp.stack([jnp.ones_like(lambdas), -lambdas], axis=1).reshape(1, 4), (1, 32)
    )
    partial_out = pl.pallas_call(
        finish_kernel,
        in_specs=[VM] * 5,
        out_specs=VM,
        out_shape=jax.ShapeDtypeStruct((8, SEQS, 256), F32),
        scratch_shapes=[pltpu.VMEM((LANES, LANES), F32), pltpu.VMEM((64, LANES), F32)],
        compiler_params=SMALL,
        name="finish",
    )(everyone, block, share, head_gain.reshape(1, -1), out_weight)
    shares = lax.all_to_all(partial_out, "tp", split_axis=0, concat_axis=0, tiled=True)
    return shares.sum(axis=0).astype(BF16)


def solution(mesh):
    return jax.shard_map(
        local,
        mesh=mesh,
        in_specs=(
            P(None, "kv"),
            P("kv"),
            P("kv", "tp"),
            P("kv", "tp"),
            P("kv", "tp"),
            P("tp", "kv"),
            P("tp"),
            P(),
            P(),
            P(None, "kv", "tp", None),
            P(None, "kv", "tp", None),
        ),
        out_specs=P(None, "kv"),
        check_vma=False,
    )
```

```python
import jax
import jax.numpy as jnp
from jax import lax
from jax.experimental import pallas as pl
from jax.experimental.pallas import tpu as pltpu
from jax.sharding import PartitionSpec as P

D = 4096
DH = 64
HEADS = 2
SEQS = 16
LANES = 128

epsilon = 1e-05
theta_base = 500000.0
floor_value = -1e30

VM = pl.BlockSpec(memory_space=pltpu.VMEM)
SM = pl.BlockSpec(memory_space=pltpu.SMEM)
ANY = pl.BlockSpec(memory_space=pltpu.HBM)
F32 = jnp.float32
BF16 = jnp.bfloat16
SMALL = pltpu.CompilerParams(vmem_limit_bytes=8 * 1024 * 1024)
BIG = pltpu.CompilerParams(vmem_limit_bytes=30 * 1024 * 1024)


def in_hbm(x):
    return pltpu.with_memory_space_constraint(x, pltpu.HBM)


def iotas(rows):
    shape = (rows, LANES)
    return lax.broadcasted_iota(jnp.int32, shape, 0), lax.broadcasted_iota(jnp.int32, shape, 1)


def project_kernel(
    tokens_in, gain_in, query_in, key_in, value_in, out, tokens, gain, weights, small, large
):
    near = (
        pltpu.make_async_copy(tokens_in, tokens, small.at[0]),
        pltpu.make_async_copy(gain_in, gain, small.at[1]),
    )
    far = [
        pltpu.make_async_copy(source, weights.at[n], large.at[n])
        for n, source in enumerate((query_in, key_in, value_in))
    ]
    for copy in (*near, *far):
        copy.start()
    for copy in near:
        copy.wait()
    widened = tokens[...].astype(F32)
    squares = jnp.sum(widened * widened, axis=1, keepdims=True)
    normed = (widened * gain[...]).astype(BF16)
    products = []
    for n in range(3):
        far[n].wait()
        products.append(jnp.dot(normed, weights[n], preferred_element_type=F32))
    query, key, value = products
    row, lane = iotas(SEQS)
    square_row = jnp.sum(jnp.where(row == lane, squares, 0.0), axis=0, keepdims=True)
    blank = jnp.zeros((3, LANES), F32)
    for dest in range(SEQS):
        out[dest, 0:16, :] = query[:, :LANES]
        out[dest, 16:32, :] = query[:, LANES:]
        out[dest, 32:40, :] = jnp.concatenate(
            [
                square_row,
                key[dest : dest + 1, :LANES],
                key[dest : dest + 1, LANES:],
                value[dest : dest + 1, :LANES],
                value[dest : dest + 1, LANES:],
                blank,
            ],
            axis=0,
        )


def turned(x, cosine, sine):
    lane = lax.broadcasted_iota(jnp.int32, x.shape, 1)
    partner = jnp.where(
        (lane // 32) % 2 == 0, pltpu.roll(x, LANES - 32, 1), pltpu.roll(x, 32, 1)
    )
    return (x * cosine + partner * sine).astype(BF16)


def attend_kernel(
    own, limits, got, cosine, sine, keys_in, values_in, out, keys, values, arrived, query_rows,
    scale_rows, score_rows, weight_rows
):
    copies = []
    for kind, (source, target) in enumerate(((keys_in, keys), (values_in, values))):
        for seq in range(SEQS):
            copies.append(
                pltpu.make_async_copy(source.at[seq], target.at[seq], arrived.at[kind, seq])
            )
    for copy in copies:
        copy.start()
    me = own[0]
    summed = jnp.sum(got[...], axis=0)
    row, lane = iotas(SEQS)
    squares = jnp.sum(jnp.where(row == lane, summed[32:33, :], 0.0), axis=1, keepdims=True)
    scaling = jnp.broadcast_to(lax.rsqrt(squares / D + epsilon), (SEQS, LANES))
    scale_rows[...] = scaling
    for head in range(HEADS):
        turned_query = turned(
            summed[16 * head : 16 * head + 16, :] * scaling, cosine[...], sine[...]
        )
        query_rows[head * SEQS : (head + 1) * SEQS, :] = turned_query.astype(F32)
    sub, lane8 = iotas(8)
    map_lanes = (lane8 // DH) == (sub % 2)
    for pair in range(SEQS // 2):
        first, second = 2 * pair, 2 * pair + 1

        def row_of(head, seq):
            at = head * SEQS + seq
            return jnp.broadcast_to(query_rows[at : at + 1, :], (8, LANES))

        left = jnp.where(sub < 2, row_of(0, first), row_of(1, first))
        left = jnp.where(map_lanes & (sub < 4), left, 0.0)
        right = jnp.where(sub < 6, row_of(0, second), row_of(1, second))
        right = jnp.where(map_lanes & (sub >= 4), right, 0.0)
        queries = jnp.concatenate([left, right], axis=1).astype(BF16)
        copies[first].wait()
        copies[second].wait()
        both_keys = jnp.concatenate([keys[first], keys[second]], axis=1)
        score_rows[pair * 8 : pair * 8 + 8, :] = lax.dot_general(
            queries, both_keys, (((1,), (1,)), ((), ())), preferred_element_type=F32
        )
    columns = lax.broadcasted_iota(jnp.int32, (8, 2048), 1)
    subs = lax.broadcasted_iota(jnp.int32, (8, 2048), 0)
    own_head = (columns % 2) == ((subs // 2) % 2)
    maxima = jnp.zeros((8, LANES), F32)
    totals = jnp.zeros((8, LANES), F32)
    for pair in range(SEQS // 2):
        first, second = 2 * pair, 2 * pair + 1
        at = slice(pair * 8, pair * 8 + 8)
        visible = own_head & (columns < limits[at, :1])
        masked = jnp.where(visible, score_rows[at, :] * DH ** (-0.5), floor_value)
        highest = jnp.max(masked, axis=1, keepdims=True)
        weights = jnp.where(visible, jnp.exp(masked - highest), 0.0).astype(BF16)
        total = jnp.sum(weights.astype(F32), axis=1, keepdims=True)
        weight_rows[at, :] = weights
        place = lane8 == pair * 8 + sub
        maxima = maxima + jnp.where(place, highest, 0.0)
        totals = totals + jnp.where(place, total, 0.0)
    scale = scale_rows[pl.ds(me, 1), :]
    row_cosine = cosine[pl.ds(me, 1), :]
    row_sine = sine[pl.ds(me, 1), :]
    lane1 = lax.broadcasted_iota(jnp.int32, (1, LANES), 1)
    fresh_scores = jnp.zeros((1, LANES), F32)
    for head in range(HEADS):
        query = query_rows[pl.ds(head * SEQS + me, 1), :]
        fresh_key = turned(summed[33 + head : 34 + head, :] * scale, row_cosine, row_sine)
        product = query * fresh_key.astype(F32)
        for side in range(2):
            score = jnp.sum(
                jnp.where(lane1 // DH == side, product, 0.0), axis=1, keepdims=True
            ) * DH ** (-0.5)
            at = me * 4 + head * 2 + side
            fresh_scores = fresh_scores + jnp.where(lane1 == at, score, 0.0)
    fresh_value = (summed[35:37, :] * scale).astype(BF16).astype(F32)
    tail = jnp.concatenate(
        [
            *thirds(jnp.sum(maxima, axis=0, keepdims=True)),
            *thirds(jnp.sum(totals, axis=0, keepdims=True)),
            *thirds(fresh_scores),
            fresh_value,
            jnp.zeros((5, LANES), F32),
        ],
        axis=0,
    ).astype(BF16)
    for dest in range(SEQS):
        out[dest, 64:80, :] = tail
    for two in range(SEQS // 4):
        parts = []
        for pair in (2 * two, 2 * two + 1):
            first, second = 2 * pair, 2 * pair + 1
            copies[SEQS + first].wait()
            copies[SEQS + second].wait()
            both_values = jnp.concatenate([values[first], values[second]], axis=1)
            valued = jnp.dot(
                weight_rows[pair * 8 : pair * 8 + 8, :],
                both_values,
                preferred_element_type=F32,
            )
            parts.append(jnp.where(sub < 4, valued[:, :LANES], valued[:, LANES:]))
        sixteen = jnp.concatenate(parts, axis=0).astype(BF16)
        for dest in range(SEQS):
            out[dest, two * 16 : two * 16 + 16, :] = sixteen


def thirds(x):
    high = x.astype(BF16).astype(F32)
    middle = (x - high).astype(BF16).astype(F32)
    return high, middle, x - high - middle


def finish_kernel(got, block, share, head_gain, out_weight, out, factors, joined):
    rows16, _ = iotas(SEQS)
    tails = got[:, 64:80, :].astype(F32)

    def whole(at):
        return tails[:, at, :] + tails[:, at + 1, :] + tails[:, at + 2, :]

    maxima = whole(0)
    totals = whole(3)
    fresh = jnp.sum(whole(6), axis=0, keepdims=True)
    in_block = jnp.max(
        jnp.where(rows16 == block[...], maxima, floor_value), axis=0, keepdims=True
    )
    in_block = jnp.maximum(in_block, fresh)
    top = jnp.maximum(jnp.max(maxima, axis=0, keepdims=True), fresh)
    factor = jnp.exp(maxima - top)
    fresh_factor = jnp.exp(fresh - in_block).astype(BF16).astype(F32) * jnp.exp(in_block - top)
    total = jnp.sum(totals * factor, axis=0, keepdims=True) + fresh_factor
    part = share[...] / total
    factors[...] = jnp.zeros((LANES, LANES), F32)
    factors[0:SEQS, :] = factor * part
    factors[SEQS : SEQS + 1, :] = fresh_factor * part
    columns = factors[...].T
    sub, _ = iotas(16)
    for four in range(SEQS // 4):
        here = columns[four * 16 : four * 16 + 16, :]
        fresh_value = jnp.zeros((16, LANES), F32)
        for n in range(8):
            line = tails[four * 4 + n // 2, 9 + n % 2 : 10 + n % 2, :]
            fresh_value = jnp.where(sub // 2 == n, line, fresh_value)
        joint = here[:, SEQS : SEQS + 1] * fresh_value
        for peer in range(SEQS):
            joint = joint + here[:, peer : peer + 1] * got[
                peer, four * 16 : four * 16 + 16, :
            ].astype(F32)
        joined[four * 16 : four * 16 + 16, :] = joint
    sides = []
    for head in range(HEADS):
        mixed = joined[pl.ds(2 * head, SEQS, 4), :] + joined[pl.ds(2 * head + 1, SEQS, 4), :]
        mean = jnp.mean(mixed * mixed, axis=1, keepdims=True)
        sides.append((mixed * lax.rsqrt(mean + epsilon) * head_gain[...]).astype(BF16))
    head_out = jnp.concatenate(sides, axis=1)
    partial_out = jnp.dot(head_out, out_weight[...], preferred_element_type=F32)
    for dest in range(8):
        out[dest] = partial_out


def local(
    tokens,
    norm_gain,
    query_weight,
    key_weight,
    value_weight,
    out_weight,
    lambdas,
    head_gain,
    lengths,
    key_cache,
    value_cache,
):
    sent = pl.pallas_call(
        project_kernel,
        in_specs=[ANY] * 5,
        out_specs=VM,
        out_shape=jax.ShapeDtypeStruct((SEQS, 40, LANES), F32),
        scratch_shapes=[
            pltpu.VMEM((SEQS, 256), BF16),
            pltpu.VMEM((1, 256), F32),
            pltpu.VMEM((3, 256, 256), BF16),
            pltpu.SemaphoreType.DMA((2,)),
            pltpu.SemaphoreType.DMA((3,)),
        ],
        compiler_params=SMALL,
        name="project",
    )(
        in_hbm(tokens),
        in_hbm(norm_gain.reshape(1, -1)),
        in_hbm(query_weight),
        in_hbm(key_weight),
        in_hbm(value_weight),
    )
    got = lax.all_to_all(sent, "kv", split_axis=0, concat_axis=0, tiled=True)
    cache_shape = (SEQS, 2048, LANES)
    halfway = DH // 2
    frequency = theta_base ** (-jnp.arange(halfway, dtype=F32) / halfway)
    angles = lengths.astype(F32)[:, None] * frequency[None, :]
    cosine = jnp.tile(jnp.cos(angles), (1, 4))
    sine = jnp.sin(angles)
    sine = jnp.tile(jnp.concatenate([-sine, sine], axis=1), (1, 2))
    own = lax.axis_index("kv").astype(jnp.int32).reshape(1)
    limits = jnp.broadcast_to(
        jnp.repeat(2 * (lengths - own * 1024), 4).reshape(64, 1), (64, LANES)
    )
    shared = pl.pallas_call(
        attend_kernel,
        in_specs=[SM, VM, VM, VM, VM, ANY, ANY],
        out_specs=VM,
        out_shape=jax.ShapeDtypeStruct((SEQS, 80, LANES), BF16),
        scratch_shapes=[
            pltpu.VMEM(cache_shape, BF16),
            pltpu.VMEM(cache_shape, BF16),
            pltpu.SemaphoreType.DMA((2, SEQS)),
            pltpu.VMEM((32, LANES), F32),
            pltpu.VMEM((SEQS, LANES), F32),
            pltpu.VMEM((64, 2048), F32),
            pltpu.VMEM((64, 2048), BF16),
        ],
        compiler_params=BIG,
        name="attend",
    )(
        own,
        limits,
        got,
        cosine,
        sine,
        in_hbm(key_cache.reshape(cache_shape)),
        in_hbm(value_cache.reshape(cache_shape)),
    )
    everyone = lax.all_to_all(shared, "kv", split_axis=0, concat_axis=0, tiled=True)
    block = jnp.pad(jnp.repeat(lengths // 1024, 4), (0, 64)).reshape(1, LANES)
    share = jnp.tile(
        jnp.stack([jnp.ones_like(lambdas), -lambdas], axis=1).reshape(1, 4), (1, 32)
    )
    partial_out = pl.pallas_call(
        finish_kernel,
        in_specs=[VM] * 5,
        out_specs=VM,
        out_shape=jax.ShapeDtypeStruct((8, SEQS, 256), F32),
        scratch_shapes=[pltpu.VMEM((LANES, LANES), F32), pltpu.VMEM((64, LANES), F32)],
        compiler_params=SMALL,
        name="finish",
    )(everyone, block, share, head_gain.reshape(1, -1), out_weight)
    shares = lax.all_to_all(partial_out, "tp", split_axis=0, concat_axis=0, tiled=True)
    return shares.sum(axis=0).astype(BF16)


def solution(mesh):
    return jax.shard_map(
        local,
        mesh=mesh,
        in_specs=(
            P(None, "kv"),
            P("kv"),
            P("kv", "tp"),
            P("kv", "tp"),
            P("kv", "tp"),
            P("tp", "kv"),
            P("tp"),
            P(),
            P(),
            P(None, "kv", "tp", None),
            P(None, "kv", "tp", None),
        ),
        out_specs=P(None, "kv"),
        check_vma=False,
    )
```

```python
import jax
import jax.numpy as jnp
import numpy as np
from jax import lax
from jax.experimental import pallas as pl
from jax.experimental.pallas import tpu as pltpu
from jax.sharding import PartitionSpec as P

D = 4096
DH = 64
HEADS = 2
SEQS = 16
LANES = 128

epsilon = 1e-05
theta_base = 500000.0
floor_value = -1e30
AHEAD = 10

VM = pl.BlockSpec(memory_space=pltpu.VMEM)
SM = pl.BlockSpec(memory_space=pltpu.SMEM)
ANY = pl.BlockSpec(memory_space=pltpu.HBM)
F32 = jnp.float32
BF16 = jnp.bfloat16
SMALL = pltpu.CompilerParams(vmem_limit_bytes=8 * 1024 * 1024)
BIG = pltpu.CompilerParams(vmem_limit_bytes=30 * 1024 * 1024)


def in_hbm(x):
    return pltpu.with_memory_space_constraint(x, pltpu.HBM)


def iotas(rows):
    shape = (rows, LANES)
    return lax.broadcasted_iota(jnp.int32, shape, 0), lax.broadcasted_iota(jnp.int32, shape, 1)


def project_kernel(
    tokens_in, gain_in, lengths_in, lambdas_in, rates_in, query_in, key_in, value_in, out, tables,
    tokens, gain, lengths, lambdas, rates, weights, small, large,
):
    near = [
        pltpu.make_async_copy(source, target, small.at[n])
        for n, (source, target) in enumerate(
            (
                (tokens_in, tokens),
                (gain_in, gain),
                (lengths_in, lengths),
                (lambdas_in, lambdas),
                (rates_in, rates),
            )
        )
    ]
    far = [
        pltpu.make_async_copy(source, weights.at[n], large.at[n])
        for n, source in enumerate((query_in, key_in, value_in))
    ]
    for copy in (*near, *far):
        copy.start()
    for copy in near:
        copy.wait()
    widened = tokens[...].astype(F32)
    squares = jnp.sum(widened * widened, axis=1, keepdims=True)
    normed = (widened * gain[...]).astype(BF16)
    row, lane = iotas(SEQS)
    square_row = jnp.sum(jnp.where(row == lane, squares, 0.0), axis=0, keepdims=True)
    row16 = lax.broadcasted_iota(jnp.int32, (SEQS, SEQS), 0)
    lane16 = lax.broadcasted_iota(jnp.int32, (SEQS, SEQS), 1)
    held = lengths[...].astype(F32)
    held_column = jnp.sum(jnp.where(row16 == lane16, held, 0.0), axis=1, keepdims=True)
    angles = held_column * rates[...]
    tables[0:16, :] = jnp.cos(angles)
    sine = jnp.sin(angles)
    tables[16:32, :] = jnp.where((lane // 32) % 2 == 0, -sine, sine)
    lane1 = lax.broadcasted_iota(jnp.int32, (1, LANES), 1)
    lambda_row = jnp.where((lane1 // 2) % 2 == 0, lambdas[:, 0:1], lambdas[:, 1:2])
    tables[32:40, :] = jnp.concatenate(
        [
            jnp.sum(jnp.where(row == lane // 4, held_column, 0.0), axis=0, keepdims=True),
            jnp.where(lane1 % 2 == 0, 1.0, -lambda_row),
            jnp.zeros((6, LANES), F32),
        ],
        axis=0,
    )
    products = []
    for n in range(3):
        far[n].wait()
        products.append(jnp.dot(normed, weights[n], preferred_element_type=F32))
    query, key, value = products
    blank = jnp.zeros((3, LANES), F32)
    for dest in range(SEQS):
        out[dest, 0:16, :] = query[:, :LANES]
        out[dest, 16:32, :] = query[:, LANES:]
        out[dest, 32:40, :] = jnp.concatenate(
            [
                square_row,
                key[dest : dest + 1, :LANES],
                key[dest : dest + 1, LANES:],
                value[dest : dest + 1, :LANES],
                value[dest : dest + 1, LANES:],
                blank,
            ],
            axis=0,
        )


def turned(x, cosine, sine):
    lane = lax.broadcasted_iota(jnp.int32, x.shape, 1)
    partner = jnp.where(
        (lane // 32) % 2 == 0, pltpu.roll(x, LANES - 32, 1), pltpu.roll(x, 32, 1)
    )
    return (x * cosine + partner * sine).astype(BF16)


def attend_kernel(
    tables, got, keys_in, values_in, out, keys, values, arrived, query_rows, scale_rows,
    score_rows, weight_rows,
):
    copies = []
    for kind, (source, target) in enumerate(((keys_in, keys), (values_in, values))):
        for seq in range(SEQS):
            copies.append(
                pltpu.make_async_copy(source.at[seq], target.at[seq], arrived.at[kind, seq])
            )
    for copy in copies[:AHEAD]:
        copy.start()

    def arrive(kind, seq):
        at = kind * SEQS + seq
        copies[at].wait()
        if at + AHEAD < 2 * SEQS:
            copies[at + AHEAD].start()

    me = lax.axis_index("kv")
    cosine, sine = tables[0:16, :], tables[16:32, :]
    summed = jnp.sum(got[...], axis=0)
    row, lane = iotas(SEQS)
    squares = jnp.sum(jnp.where(row == lane, summed[32:33, :], 0.0), axis=1, keepdims=True)
    scaling = jnp.broadcast_to(lax.rsqrt(squares / D + epsilon), (SEQS, LANES))
    scale_rows[...] = scaling
    for head in range(HEADS):
        turned_query = turned(
            summed[16 * head : 16 * head + 16, :] * scaling, cosine, sine
        )
        query_rows[head * SEQS : (head + 1) * SEQS, :] = turned_query.astype(F32)
    sub, lane8 = iotas(8)
    map_lanes = (lane8 // DH) == (sub % 2)
    for pair in range(SEQS // 2):
        first, second = 2 * pair, 2 * pair + 1

        def row_of(head, seq):
            at = head * SEQS + seq
            return jnp.broadcast_to(query_rows[at : at + 1, :], (8, LANES))

        left = jnp.where(sub < 2, row_of(0, first), row_of(1, first))
        left = jnp.where(map_lanes & (sub < 4), left, 0.0)
        right = jnp.where(sub < 6, row_of(0, second), row_of(1, second))
        right = jnp.where(map_lanes & (sub >= 4), right, 0.0)
        queries = jnp.concatenate([left, right], axis=1).astype(BF16)
        arrive(0, first)
        arrive(0, second)
        both_keys = jnp.concatenate([keys[first], keys[second]], axis=1)
        score_rows[pair * 8 : pair * 8 + 8, :] = lax.dot_general(
            queries, both_keys, (((1,), (1,)), ((), ())), preferred_element_type=F32
        )
    columns = lax.broadcasted_iota(jnp.int32, (8, 2048), 1)
    subs = lax.broadcasted_iota(jnp.int32, (8, 2048), 0)
    own_head = (columns % 2) == ((subs // 2) % 2)
    maxima = jnp.zeros((8, LANES), F32)
    totals = jnp.zeros((8, LANES), F32)
    for pair in range(SEQS // 2):
        first, second = 2 * pair, 2 * pair + 1
        at = slice(pair * 8, pair * 8 + 8)
        limit = jnp.sum(
            jnp.where(lane8 == pair * 8 + sub, tables[32:33, :], 0.0), axis=1, keepdims=True
        ).astype(jnp.int32)
        visible = own_head & (columns < 2 * (limit - me * 1024))
        masked = jnp.where(visible, score_rows[at, :] * DH ** (-0.5), floor_value)
        highest = jnp.max(masked, axis=1, keepdims=True)
        weights = jnp.where(visible, jnp.exp(masked - highest), 0.0).astype(BF16)
        total = jnp.sum(weights.astype(F32), axis=1, keepdims=True)
        weight_rows[at, :] = weights
        place = lane8 == pair * 8 + sub
        maxima = maxima + jnp.where(place, highest, 0.0)
        totals = totals + jnp.where(place, total, 0.0)
    scale = scale_rows[pl.ds(me, 1), :]
    row_cosine = tables[pl.ds(me, 1), :]
    row_sine = tables[pl.ds(SEQS + me, 1), :]
    lane1 = lax.broadcasted_iota(jnp.int32, (1, LANES), 1)
    fresh_scores = jnp.zeros((1, LANES), F32)
    for head in range(HEADS):
        query = query_rows[pl.ds(head * SEQS + me, 1), :]
        fresh_key = turned(summed[33 + head : 34 + head, :] * scale, row_cosine, row_sine)
        product = query * fresh_key.astype(F32)
        for side in range(2):
            score = jnp.sum(
                jnp.where(lane1 // DH == side, product, 0.0), axis=1, keepdims=True
            ) * DH ** (-0.5)
            at = me * 4 + head * 2 + side
            fresh_scores = fresh_scores + jnp.where(lane1 == at, score, 0.0)
    fresh_value = (summed[35:37, :] * scale).astype(BF16).astype(F32)
    tail = jnp.concatenate(
        [
            *thirds(jnp.sum(maxima, axis=0, keepdims=True)),
            *thirds(jnp.sum(totals, axis=0, keepdims=True)),
            *thirds(fresh_scores),
            fresh_value,
            jnp.zeros((5, LANES), F32),
        ],
        axis=0,
    ).astype(BF16)
    for dest in range(SEQS):
        out[dest, 64:80, :] = tail
    for two in range(SEQS // 4):
        parts = []
        for pair in (2 * two, 2 * two + 1):
            first, second = 2 * pair, 2 * pair + 1
            arrive(1, first)
            arrive(1, second)
            both_values = jnp.concatenate([values[first], values[second]], axis=1)
            valued = jnp.dot(
                weight_rows[pair * 8 : pair * 8 + 8, :],
                both_values,
                preferred_element_type=F32,
            )
            parts.append(jnp.where(sub < 4, valued[:, :LANES], valued[:, LANES:]))
        sixteen = jnp.concatenate(parts, axis=0).astype(BF16)
        for dest in range(SEQS):
            out[dest, two * 16 : two * 16 + 16, :] = sixteen


def thirds(x):
    high = x.astype(BF16).astype(F32)
    middle = (x - high).astype(BF16).astype(F32)
    return high, middle, x - high - middle


def finish_kernel(got, tables, head_gain, out_weight, out, factors, joined):
    rows16, _ = iotas(SEQS)
    tails = got[:, 64:80, :].astype(F32)

    def whole(at):
        return tails[:, at, :] + tails[:, at + 1, :] + tails[:, at + 2, :]

    maxima = whole(0)
    totals = whole(3)
    fresh = jnp.sum(whole(6), axis=0, keepdims=True)
    block = tables[32:33, :].astype(jnp.int32) // 1024
    in_block = jnp.max(
        jnp.where(rows16 == block, maxima, floor_value), axis=0, keepdims=True
    )
    in_block = jnp.maximum(in_block, fresh)
    top = jnp.maximum(jnp.max(maxima, axis=0, keepdims=True), fresh)
    factor = jnp.exp(maxima - top)
    fresh_factor = jnp.exp(fresh - in_block).astype(BF16).astype(F32) * jnp.exp(in_block - top)
    total = jnp.sum(totals * factor, axis=0, keepdims=True) + fresh_factor
    part = tables[33:34, :] / total
    factors[...] = jnp.zeros((LANES, LANES), F32)
    factors[0:SEQS, :] = factor * part
    factors[SEQS : SEQS + 1, :] = fresh_factor * part
    columns = factors[...].T
    sub, _ = iotas(16)
    for four in range(SEQS // 4):
        here = columns[four * 16 : four * 16 + 16, :]
        fresh_value = jnp.zeros((16, LANES), F32)
        for n in range(8):
            line = tails[four * 4 + n // 2, 9 + n % 2 : 10 + n % 2, :]
            fresh_value = jnp.where(sub // 2 == n, line, fresh_value)
        joint = here[:, SEQS : SEQS + 1] * fresh_value
        for peer in range(SEQS):
            joint = joint + here[:, peer : peer + 1] * got[
                peer, four * 16 : four * 16 + 16, :
            ].astype(F32)
        joined[four * 16 : four * 16 + 16, :] = joint
    sides = []
    for head in range(HEADS):
        mixed = joined[pl.ds(2 * head, SEQS, 4), :] + joined[pl.ds(2 * head + 1, SEQS, 4), :]
        mean = jnp.mean(mixed * mixed, axis=1, keepdims=True)
        sides.append((mixed * lax.rsqrt(mean + epsilon) * head_gain[...]).astype(BF16))
    head_out = jnp.concatenate(sides, axis=1)
    partial_out = jnp.dot(head_out, out_weight[...], preferred_element_type=F32)
    for dest in range(8):
        out[dest] = partial_out


def local(
    tokens,
    norm_gain,
    query_weight,
    key_weight,
    value_weight,
    out_weight,
    lambdas,
    head_gain,
    lengths,
    key_cache,
    value_cache,
):
    rates = np.tile(theta_base ** (-np.arange(DH // 2) / (DH // 2)), 4)
    sent, tables = pl.pallas_call(
        project_kernel,
        in_specs=[ANY] * 8,
        out_specs=[VM, VM],
        out_shape=[
            jax.ShapeDtypeStruct((SEQS, 40, LANES), F32),
            jax.ShapeDtypeStruct((40, LANES), F32),
        ],
        scratch_shapes=[
            pltpu.VMEM((SEQS, 256), BF16),
            pltpu.VMEM((1, 256), F32),
            pltpu.VMEM((1, SEQS), jnp.int32),
            pltpu.VMEM((1, HEADS), F32),
            pltpu.VMEM((1, LANES), F32),
            pltpu.VMEM((3, 256, 256), BF16),
            pltpu.SemaphoreType.DMA((5,)),
            pltpu.SemaphoreType.DMA((3,)),
        ],
        compiler_params=SMALL,
        name="project",
    )(
        in_hbm(tokens),
        in_hbm(norm_gain.reshape(1, -1)),
        in_hbm(lengths.reshape(1, -1)),
        in_hbm(lambdas.reshape(1, -1)),
        in_hbm(jnp.asarray(rates, F32).reshape(1, -1)),
        in_hbm(query_weight),
        in_hbm(key_weight),
        in_hbm(value_weight),
    )
    got = lax.all_to_all(sent, "kv", split_axis=0, concat_axis=0, tiled=True)
    cache_shape = (SEQS, 2048, LANES)
    shared = pl.pallas_call(
        attend_kernel,
        in_specs=[VM, VM, ANY, ANY],
        out_specs=VM,
        out_shape=jax.ShapeDtypeStruct((SEQS, 80, LANES), BF16),
        scratch_shapes=[
            pltpu.VMEM(cache_shape, BF16),
            pltpu.VMEM(cache_shape, BF16),
            pltpu.SemaphoreType.DMA((2, SEQS)),
            pltpu.VMEM((32, LANES), F32),
            pltpu.VMEM((SEQS, LANES), F32),
            pltpu.VMEM((64, 2048), F32),
            pltpu.VMEM((64, 2048), BF16),
        ],
        compiler_params=BIG,
        name="attend",
    )(
        tables,
        got,
        in_hbm(key_cache.reshape(cache_shape)),
        in_hbm(value_cache.reshape(cache_shape)),
    )
    everyone = lax.all_to_all(shared, "kv", split_axis=0, concat_axis=0, tiled=True)
    partial_out = pl.pallas_call(
        finish_kernel,
        in_specs=[VM] * 4,
        out_specs=VM,
        out_shape=jax.ShapeDtypeStruct((8, SEQS, 256), F32),
        scratch_shapes=[pltpu.VMEM((LANES, LANES), F32), pltpu.VMEM((64, LANES), F32)],
        compiler_params=SMALL,
        name="finish",
    )(everyone, tables, head_gain.reshape(1, -1), out_weight)
    shares = lax.all_to_all(partial_out, "tp", split_axis=0, concat_axis=0, tiled=True)
    return shares.sum(axis=0).astype(BF16)


def solution(mesh):
    return jax.shard_map(
        local,
        mesh=mesh,
        in_specs=(
            P(None, "kv"),
            P("kv"),
            P("kv", "tp"),
            P("kv", "tp"),
            P("kv", "tp"),
            P("tp", "kv"),
            P("tp"),
            P(),
            P(),
            P(None, "kv", "tp", None),
            P(None, "kv", "tp", None),
        ),
        out_specs=P(None, "kv"),
        check_vma=False,
    )
```

```python
import jax
import jax.numpy as jnp
import numpy as np
from jax import lax
from jax.experimental import pallas as pl
from jax.experimental.pallas import tpu as pltpu
from jax.sharding import PartitionSpec as P

D = 4096
DH = 64
HEADS = 2
SEQS = 16
LANES = 128

epsilon = 1e-05
theta_base = 500000.0
floor_value = -1e30

VM = pl.BlockSpec(memory_space=pltpu.VMEM)
SM = pl.BlockSpec(memory_space=pltpu.SMEM)
ANY = pl.BlockSpec(memory_space=pltpu.HBM)
F32 = jnp.float32
BF16 = jnp.bfloat16
SMALL = pltpu.CompilerParams(vmem_limit_bytes=8 * 1024 * 1024)
BIG = pltpu.CompilerParams(vmem_limit_bytes=30 * 1024 * 1024)


def in_hbm(x):
    return pltpu.with_memory_space_constraint(x, pltpu.HBM)


def iotas(rows):
    shape = (rows, LANES)
    return lax.broadcasted_iota(jnp.int32, shape, 0), lax.broadcasted_iota(jnp.int32, shape, 1)


def project_kernel(
    tokens_in, gain_in, lengths_in, lambdas_in, rates_in, query_in, key_in, value_in, out, tables,
    tokens, gain, lengths, lambdas, rates, weights, small, large,
):
    near = [
        pltpu.make_async_copy(source, target, small.at[n])
        for n, (source, target) in enumerate(
            (
                (tokens_in, tokens),
                (gain_in, gain),
                (lengths_in, lengths),
                (lambdas_in, lambdas),
                (rates_in, rates),
            )
        )
    ]
    far = [
        pltpu.make_async_copy(source, weights.at[n], large.at[n])
        for n, source in enumerate((query_in, key_in, value_in))
    ]
    for copy in (*near, *far):
        copy.start()
    for copy in near:
        copy.wait()
    widened = tokens[...].astype(F32)
    squares = jnp.sum(widened * widened, axis=1, keepdims=True)
    normed = (widened * gain[...]).astype(BF16)
    row, lane = iotas(SEQS)
    square_row = jnp.sum(jnp.where(row == lane, squares, 0.0), axis=0, keepdims=True)
    row16 = lax.broadcasted_iota(jnp.int32, (SEQS, SEQS), 0)
    lane16 = lax.broadcasted_iota(jnp.int32, (SEQS, SEQS), 1)
    held = lengths[...].astype(F32)
    held_column = jnp.sum(jnp.where(row16 == lane16, held, 0.0), axis=1, keepdims=True)
    angles = held_column * rates[...]
    tables[0:16, :] = jnp.cos(angles)
    sine = jnp.sin(angles)
    tables[16:32, :] = jnp.where((lane // 32) % 2 == 0, -sine, sine)
    lane1 = lax.broadcasted_iota(jnp.int32, (1, LANES), 1)
    lambda_row = jnp.where((lane1 // 2) % 2 == 0, lambdas[:, 0:1], lambdas[:, 1:2])
    tables[32:40, :] = jnp.concatenate(
        [
            jnp.sum(jnp.where(row == lane // 4, held_column, 0.0), axis=0, keepdims=True),
            jnp.where(lane1 % 2 == 0, 1.0, -lambda_row),
            jnp.zeros((6, LANES), F32),
        ],
        axis=0,
    )
    products = []
    for n in range(3):
        far[n].wait()
        products.append(jnp.dot(normed, weights[n], preferred_element_type=F32))
    query, key, value = products
    blank = jnp.zeros((3, LANES), F32)
    for dest in range(SEQS):
        out[dest, 0:16, :] = query[:, :LANES]
        out[dest, 16:32, :] = query[:, LANES:]
        out[dest, 32:40, :] = jnp.concatenate(
            [
                square_row,
                key[dest : dest + 1, :LANES],
                key[dest : dest + 1, LANES:],
                value[dest : dest + 1, :LANES],
                value[dest : dest + 1, LANES:],
                blank,
            ],
            axis=0,
        )


def turned(x, cosine, sine):
    lane = lax.broadcasted_iota(jnp.int32, x.shape, 1)
    partner = jnp.where(
        (lane // 32) % 2 == 0, pltpu.roll(x, LANES - 32, 1), pltpu.roll(x, 32, 1)
    )
    return (x * cosine + partner * sine).astype(BF16)


def attend_kernel(
    tables, got, keys_in, values_in, out, keys, values, arrived, query_rows, scale_rows,
    asked_rows, score_rows, weight_rows,
):
    copies = []
    for kind, (source, target) in enumerate(((keys_in, keys), (values_in, values))):
        for seq in range(SEQS):
            copies.append(
                pltpu.make_async_copy(source.at[seq], target.at[seq], arrived.at[kind, seq])
            )
    for copy in copies:
        copy.start()
    me = lax.axis_index("kv")
    cosine, sine = tables[0:16, :], tables[16:32, :]
    summed = jnp.sum(got[...], axis=0)
    row, lane = iotas(SEQS)
    squares = jnp.sum(jnp.where(row == lane, summed[32:33, :], 0.0), axis=1, keepdims=True)
    scaling = jnp.broadcast_to(lax.rsqrt(squares / D + epsilon), (SEQS, LANES))
    scale_rows[...] = scaling
    for head in range(HEADS):
        turned_query = turned(
            summed[16 * head : 16 * head + 16, :] * scaling, cosine, sine
        )
        query_rows[head * SEQS : (head + 1) * SEQS, :] = turned_query.astype(F32)
    map_lanes = (lane // DH) == (row % 2)

    def row_of(head, seq):
        at = head * SEQS + seq
        return jnp.broadcast_to(query_rows[at : at + 1, :], (SEQS, LANES))

    for group in range(4):
        first = 4 * group
        left = jnp.where(
            row < 8,
            jnp.where(row < 2, row_of(0, first), row_of(1, first)),
            jnp.where(row < 10, row_of(0, first + 2), row_of(1, first + 2)),
        )
        right = jnp.where(
            row < 8,
            jnp.where(row < 6, row_of(0, first + 1), row_of(1, first + 1)),
            jnp.where(row < 14, row_of(0, first + 3), row_of(1, first + 3)),
        )
        left = jnp.where(map_lanes & (row % 8 < 4), left, 0.0)
        right = jnp.where(map_lanes & (row % 8 >= 4), right, 0.0)
        asked_rows[group * 16 : group * 16 + 16, :] = jnp.concatenate(
            [left, right], axis=1
        ).astype(BF16)

    columns = lax.broadcasted_iota(jnp.int32, (SEQS, 2048), 1)
    subs = lax.broadcasted_iota(jnp.int32, (SEQS, 2048), 0)
    own_head = (columns % 2) == ((subs // 2) % 2)
    lengths_of = tables[32:33, :].astype(jnp.int32)
    sums = [jnp.zeros((SEQS, LANES), F32), jnp.zeros((SEQS, LANES), F32)]

    def score(group):
        for copy in copies[4 * group : 4 * group + 4]:
            copy.wait()
        for pair in (2 * group, 2 * group + 1):
            at = slice(pair * 8, pair * 8 + 8)
            both_keys = jnp.concatenate([keys[2 * pair], keys[2 * pair + 1]], axis=1)
            score_rows[at, :] = lax.dot_general(
                asked_rows[at, :],
                both_keys,
                (((1,), (1,)), ((), ())),
                preferred_element_type=F32,
            )

    def weigh(group):
        at = slice(group * 16, group * 16 + 16)
        place = lane == group * 16 + row
        limit = jnp.sum(jnp.where(place, lengths_of, 0), axis=1, keepdims=True)
        visible = own_head & (columns < 2 * (limit - me * 1024))
        masked = jnp.where(visible, score_rows[at, :] * DH ** (-0.5), floor_value)
        highest = jnp.max(masked, axis=1, keepdims=True)
        weights = jnp.where(visible, jnp.exp(masked - highest), 0.0).astype(BF16)
        weight_rows[at, :] = weights
        total = jnp.sum(weights.astype(F32), axis=1, keepdims=True)
        sums[0] = sums[0] + jnp.where(place, highest, 0.0)
        sums[1] = sums[1] + jnp.where(place, total, 0.0)

    def value(pair):
        both_values = jnp.concatenate([values[2 * pair], values[2 * pair + 1]], axis=1)
        valued = jnp.dot(
            weight_rows[pair * 8 : pair * 8 + 8, :], both_values, preferred_element_type=F32
        )
        return jnp.where(row[:8] < 4, valued[:, :LANES], valued[:, LANES:])

    def arrive(seqs):
        for seq in seqs:
            copies[SEQS + seq].wait()

    def give(group, parts):
        sixteen = jnp.concatenate(parts, axis=0).astype(BF16)
        for dest in range(SEQS):
            out[dest, group * 16 : group * 16 + 16, :] = sixteen

    score(0)
    for group in range(1, 4):
        score(group)
        weigh(group - 1)
    arrive(range(4))
    give(0, [value(0), value(1)])
    weigh(3)
    scale = scale_rows[pl.ds(me, 1), :]
    row_cosine = tables[pl.ds(me, 1), :]
    row_sine = tables[pl.ds(SEQS + me, 1), :]
    lane1 = lax.broadcasted_iota(jnp.int32, (1, LANES), 1)
    fresh_scores = jnp.zeros((1, LANES), F32)
    for head in range(HEADS):
        query = query_rows[pl.ds(head * SEQS + me, 1), :]
        fresh_key = turned(summed[33 + head : 34 + head, :] * scale, row_cosine, row_sine)
        product = query * fresh_key.astype(F32)
        for side in range(2):
            fresh = jnp.sum(
                jnp.where(lane1 // DH == side, product, 0.0), axis=1, keepdims=True
            ) * DH ** (-0.5)
            at = me * 4 + head * 2 + side
            fresh_scores = fresh_scores + jnp.where(lane1 == at, fresh, 0.0)
    fresh_value = (summed[35:37, :] * scale).astype(BF16).astype(F32)
    tail = jnp.concatenate(
        [
            *thirds(jnp.sum(sums[0], axis=0, keepdims=True)),
            *thirds(jnp.sum(sums[1], axis=0, keepdims=True)),
            *thirds(fresh_scores),
            fresh_value,
            jnp.zeros((5, LANES), F32),
        ],
        axis=0,
    ).astype(BF16)
    for dest in range(SEQS):
        out[dest, 64:80, :] = tail
    for group in range(1, 3):
        arrive(range(4 * group, 4 * group + 4))
        give(group, [value(2 * group), value(2 * group + 1)])
    arrive((12, 13))
    early = value(6)
    arrive((14, 15))
    give(3, [early, value(7)])


def thirds(x):
    high = x.astype(BF16).astype(F32)
    middle = (x - high).astype(BF16).astype(F32)
    return high, middle, x - high - middle


def finish_kernel(got, tables, head_gain, out_weight, out, factors, joined):
    rows16, _ = iotas(SEQS)
    tails = got[:, 64:80, :].astype(F32)

    def whole(at):
        return tails[:, at, :] + tails[:, at + 1, :] + tails[:, at + 2, :]

    maxima = whole(0)
    totals = whole(3)
    fresh = jnp.sum(whole(6), axis=0, keepdims=True)
    block = tables[32:33, :].astype(jnp.int32) // 1024
    in_block = jnp.max(
        jnp.where(rows16 == block, maxima, floor_value), axis=0, keepdims=True
    )
    in_block = jnp.maximum(in_block, fresh)
    top = jnp.maximum(jnp.max(maxima, axis=0, keepdims=True), fresh)
    factor = jnp.exp(maxima - top)
    fresh_factor = jnp.exp(fresh - in_block).astype(BF16).astype(F32) * jnp.exp(in_block - top)
    total = jnp.sum(totals * factor, axis=0, keepdims=True) + fresh_factor
    part = tables[33:34, :] / total
    factors[...] = jnp.zeros((LANES, LANES), F32)
    factors[0:SEQS, :] = factor * part
    factors[SEQS : SEQS + 1, :] = fresh_factor * part
    columns = factors[...].T
    sub, _ = iotas(16)
    for four in range(SEQS // 4):
        here = columns[four * 16 : four * 16 + 16, :]
        fresh_value = jnp.zeros((16, LANES), F32)
        for n in range(8):
            line = tails[four * 4 + n // 2, 9 + n % 2 : 10 + n % 2, :]
            fresh_value = jnp.where(sub // 2 == n, line, fresh_value)
        joint = here[:, SEQS : SEQS + 1] * fresh_value
        for peer in range(SEQS):
            joint = joint + here[:, peer : peer + 1] * got[
                peer, four * 16 : four * 16 + 16, :
            ].astype(F32)
        joined[four * 16 : four * 16 + 16, :] = joint
    sides = []
    for head in range(HEADS):
        mixed = joined[pl.ds(2 * head, SEQS, 4), :] + joined[pl.ds(2 * head + 1, SEQS, 4), :]
        mean = jnp.mean(mixed * mixed, axis=1, keepdims=True)
        sides.append((mixed * lax.rsqrt(mean + epsilon) * head_gain[...]).astype(BF16))
    head_out = jnp.concatenate(sides, axis=1)
    partial_out = jnp.dot(head_out, out_weight[...], preferred_element_type=F32)
    for dest in range(8):
        out[dest] = partial_out


def attend_call(tables, got, keys, values, name):
    return pl.pallas_call(
        attend_kernel,
        in_specs=[VM, VM, ANY, ANY],
        out_specs=VM,
        out_shape=jax.ShapeDtypeStruct((SEQS, 80, LANES), BF16),
        scratch_shapes=[
            pltpu.VMEM(keys.shape, BF16),
            pltpu.VMEM(values.shape, BF16),
            pltpu.SemaphoreType.DMA((2, SEQS)),
            pltpu.VMEM((32, LANES), F32),
            pltpu.VMEM((SEQS, LANES), F32),
            pltpu.VMEM((64, 256), BF16),
            pltpu.VMEM((64, 2048), F32),
            pltpu.VMEM((64, 2048), BF16),
        ],
        compiler_params=BIG,
        name=name,
    )(tables, got, in_hbm(keys), in_hbm(values))


def local(
    tokens,
    norm_gain,
    query_weight,
    key_weight,
    value_weight,
    out_weight,
    lambdas,
    head_gain,
    lengths,
    key_cache,
    value_cache,
):
    rates = np.tile(theta_base ** (-np.arange(DH // 2) / (DH // 2)), 4)
    sent, tables = pl.pallas_call(
        project_kernel,
        in_specs=[ANY] * 8,
        out_specs=[VM, VM],
        out_shape=[
            jax.ShapeDtypeStruct((SEQS, 40, LANES), F32),
            jax.ShapeDtypeStruct((40, LANES), F32),
        ],
        scratch_shapes=[
            pltpu.VMEM((SEQS, 256), BF16),
            pltpu.VMEM((1, 256), F32),
            pltpu.VMEM((1, SEQS), jnp.int32),
            pltpu.VMEM((1, HEADS), F32),
            pltpu.VMEM((1, LANES), F32),
            pltpu.VMEM((3, 256, 256), BF16),
            pltpu.SemaphoreType.DMA((5,)),
            pltpu.SemaphoreType.DMA((3,)),
        ],
        compiler_params=SMALL,
        name="project",
    )(
        in_hbm(tokens),
        in_hbm(norm_gain.reshape(1, -1)),
        in_hbm(lengths.reshape(1, -1)),
        in_hbm(lambdas.reshape(1, -1)),
        in_hbm(jnp.asarray(rates, F32).reshape(1, -1)),
        in_hbm(query_weight),
        in_hbm(key_weight),
        in_hbm(value_weight),
    )
    got = lax.all_to_all(sent, "kv", split_axis=0, concat_axis=0, tiled=True)
    cache_shape = (SEQS, 2048, LANES)
    shared = attend_call(
        tables, got, key_cache.reshape(cache_shape), value_cache.reshape(cache_shape), "attend"
    )
    everyone = lax.all_to_all(shared, "kv", split_axis=0, concat_axis=0, tiled=True)
    partial_out = pl.pallas_call(
        finish_kernel,
        in_specs=[VM] * 4,
        out_specs=VM,
        out_shape=jax.ShapeDtypeStruct((8, SEQS, 256), F32),
        scratch_shapes=[pltpu.VMEM((LANES, LANES), F32), pltpu.VMEM((64, LANES), F32)],
        compiler_params=SMALL,
        name="finish",
    )(everyone, tables, head_gain.reshape(1, -1), out_weight)
    shares = lax.all_to_all(partial_out, "tp", split_axis=0, concat_axis=0, tiled=True)
    return shares.sum(axis=0).astype(BF16)


def solution(mesh):
    return jax.shard_map(
        local,
        mesh=mesh,
        in_specs=(
            P(None, "kv"),
            P("kv"),
            P("kv", "tp"),
            P("kv", "tp"),
            P("kv", "tp"),
            P("tp", "kv"),
            P("tp"),
            P(),
            P(),
            P(None, "kv", "tp", None),
            P(None, "kv", "tp", None),
        ),
        out_specs=P(None, "kv"),
        check_vma=False,
    )
```

```python
import jax
import jax.numpy as jnp
import numpy as np
from jax import lax
from jax.experimental import pallas as pl
from jax.experimental.pallas import tpu as pltpu
from jax.sharding import PartitionSpec as P

D = 4096
DH = 64
HEADS = 2
SEQS = 16
LANES = 128

epsilon = 1e-05
theta_base = 500000.0
floor_value = -1e30

VM = pl.BlockSpec(memory_space=pltpu.VMEM)
SM = pl.BlockSpec(memory_space=pltpu.SMEM)
ANY = pl.BlockSpec(memory_space=pltpu.HBM)
F32 = jnp.float32
BF16 = jnp.bfloat16
SMALL = pltpu.CompilerParams(vmem_limit_bytes=8 * 1024 * 1024)
BIG = pltpu.CompilerParams(vmem_limit_bytes=30 * 1024 * 1024)


def in_hbm(x):
    return pltpu.with_memory_space_constraint(x, pltpu.HBM)


def iotas(rows):
    shape = (rows, LANES)
    return lax.broadcasted_iota(jnp.int32, shape, 0), lax.broadcasted_iota(jnp.int32, shape, 1)


def project_kernel(
    tokens_in, gain_in, lengths_in, lambdas_in, rates_in, query_in, key_in, value_in, out, tables,
    tokens, gain, lengths, lambdas, rates, weights, small, large,
):
    near = [
        pltpu.make_async_copy(source, target, small.at[n])
        for n, (source, target) in enumerate(
            (
                (tokens_in, tokens),
                (gain_in, gain),
                (lengths_in, lengths),
                (lambdas_in, lambdas),
                (rates_in, rates),
            )
        )
    ]
    far = [
        pltpu.make_async_copy(source, weights.at[n], large.at[n])
        for n, source in enumerate((query_in, key_in, value_in))
    ]
    for copy in (*near, *far):
        copy.start()
    for copy in near:
        copy.wait()
    widened = tokens[...].astype(F32)
    squares = jnp.sum(widened * widened, axis=1, keepdims=True)
    normed = (widened * gain[...]).astype(BF16)
    row, lane = iotas(SEQS)
    square_row = jnp.sum(jnp.where(row == lane, squares, 0.0), axis=0, keepdims=True)
    row16 = lax.broadcasted_iota(jnp.int32, (SEQS, SEQS), 0)
    lane16 = lax.broadcasted_iota(jnp.int32, (SEQS, SEQS), 1)
    held = lengths[...].astype(F32)
    held_column = jnp.sum(jnp.where(row16 == lane16, held, 0.0), axis=1, keepdims=True)
    angles = held_column * rates[...]
    tables[0:16, :] = jnp.cos(angles)
    sine = jnp.sin(angles)
    tables[16:32, :] = jnp.where((lane // 32) % 2 == 0, -sine, sine)
    lane1 = lax.broadcasted_iota(jnp.int32, (1, LANES), 1)
    lambda_row = jnp.where((lane1 // 2) % 2 == 0, lambdas[:, 0:1], lambdas[:, 1:2])
    tables[32:40, :] = jnp.concatenate(
        [
            jnp.sum(jnp.where(row == lane // 4, held_column, 0.0), axis=0, keepdims=True),
            jnp.where(lane1 % 2 == 0, 1.0, -lambda_row),
            jnp.zeros((6, LANES), F32),
        ],
        axis=0,
    )
    products = []
    for n in range(3):
        far[n].wait()
        products.append(jnp.dot(normed, weights[n], preferred_element_type=F32))
    query, key, value = products
    blank = jnp.zeros((3, LANES), F32)
    for dest in range(SEQS):
        out[dest, 0:16, :] = query[:, :LANES]
        out[dest, 16:32, :] = query[:, LANES:]
        out[dest, 32:40, :] = jnp.concatenate(
            [
                square_row,
                key[dest : dest + 1, :LANES],
                key[dest : dest + 1, LANES:],
                value[dest : dest + 1, :LANES],
                value[dest : dest + 1, LANES:],
                blank,
            ],
            axis=0,
        )


def turned(x, cosine, sine):
    lane = lax.broadcasted_iota(jnp.int32, x.shape, 1)
    partner = jnp.where(
        (lane // 32) % 2 == 0, pltpu.roll(x, LANES - 32, 1), pltpu.roll(x, 32, 1)
    )
    return (x * cosine + partner * sine).astype(BF16)


def attend_kernel(
    tables, got, keys_in, values_in, out, keys, values, arrived, query_rows, scale_rows,
    asked_rows, score_rows, weight_rows,
):
    copies = []
    for kind, (source, target) in enumerate(((keys_in, keys), (values_in, values))):
        for seq in range(SEQS):
            copies.append(
                pltpu.make_async_copy(source.at[seq], target.at[seq], arrived.at[kind, seq])
            )
    for copy in copies:
        copy.start()
    me = lax.axis_index("kv")
    cosine, sine = tables[0:16, :], tables[16:32, :]
    summed = jnp.sum(got[...], axis=0)
    row, lane = iotas(SEQS)
    squares = jnp.sum(jnp.where(row == lane, summed[32:33, :], 0.0), axis=1, keepdims=True)
    scaling = jnp.broadcast_to(lax.rsqrt(squares / D + epsilon), (SEQS, LANES))
    scale_rows[...] = scaling
    for head in range(HEADS):
        turned_query = turned(
            summed[16 * head : 16 * head + 16, :] * scaling, cosine, sine
        )
        query_rows[head * SEQS : (head + 1) * SEQS, :] = turned_query.astype(F32)
    map_lanes = (lane // DH) == (row % 2)

    def row_of(head, seq):
        at = head * SEQS + seq
        return jnp.broadcast_to(query_rows[at : at + 1, :], (SEQS, LANES))

    for group in range(4):
        first = 4 * group
        left = jnp.where(
            row < 8,
            jnp.where(row < 2, row_of(0, first), row_of(1, first)),
            jnp.where(row < 10, row_of(0, first + 2), row_of(1, first + 2)),
        )
        right = jnp.where(
            row < 8,
            jnp.where(row < 6, row_of(0, first + 1), row_of(1, first + 1)),
            jnp.where(row < 14, row_of(0, first + 3), row_of(1, first + 3)),
        )
        left = jnp.where(map_lanes & (row % 8 < 4), left, 0.0)
        right = jnp.where(map_lanes & (row % 8 >= 4), right, 0.0)
        asked_rows[group * 16 : group * 16 + 16, :] = jnp.concatenate(
            [left, right], axis=1
        ).astype(BF16)

    columns = lax.broadcasted_iota(jnp.int32, (SEQS, 2048), 1)
    subs = lax.broadcasted_iota(jnp.int32, (SEQS, 2048), 0)
    own_head = (columns % 2) == ((subs // 2) % 2)
    lengths_of = tables[32:33, :].astype(jnp.int32)
    sums = [jnp.zeros((SEQS, LANES), F32)]

    def score(group):
        for copy in copies[4 * group : 4 * group + 4]:
            copy.wait()
        for pair in (2 * group, 2 * group + 1):
            at = slice(pair * 8, pair * 8 + 8)
            both_keys = jnp.concatenate([keys[2 * pair], keys[2 * pair + 1]], axis=1)
            score_rows[at, :] = lax.dot_general(
                asked_rows[at, :],
                both_keys,
                (((1,), (1,)), ((), ())),
                preferred_element_type=F32,
            )

    def weigh(group):
        at = slice(group * 16, group * 16 + 16)
        place = lane == group * 16 + row
        limit = jnp.sum(jnp.where(place, lengths_of, 0), axis=1, keepdims=True)
        visible = own_head & (columns < 2 * (limit - me * 1024))
        masked = jnp.where(visible, score_rows[at, :] * DH ** (-0.5), floor_value)
        highest = jnp.max(masked, axis=1, keepdims=True)
        weights = jnp.where(visible, jnp.exp(masked - highest), 0.0).astype(BF16)
        weight_rows[at, :] = weights
        total = jnp.sum(weights.astype(F32), axis=1, keepdims=True)
        beside = lane == 64 + group * 16 + row
        sums[0] = sums[0] + jnp.where(place, highest, jnp.where(beside, total, 0.0))

    def value(pair):
        both_values = jnp.concatenate([values[2 * pair], values[2 * pair + 1]], axis=1)
        valued = jnp.dot(
            weight_rows[pair * 8 : pair * 8 + 8, :], both_values, preferred_element_type=F32
        )
        return jnp.where(row[:8] < 4, valued[:, :LANES], valued[:, LANES:])

    def arrive(seqs):
        for seq in seqs:
            copies[SEQS + seq].wait()

    def give(group, parts):
        sixteen = jnp.concatenate(parts, axis=0).astype(BF16)
        for dest in range(SEQS):
            out[dest, group * 16 : group * 16 + 16, :] = sixteen

    score(0)
    for group in range(1, 4):
        score(group)
        weigh(group - 1)
    arrive(range(4))
    give(0, [value(0), value(1)])
    weigh(3)
    scale = scale_rows[pl.ds(me, 1), :]
    row_cosine = tables[pl.ds(me, 1), :]
    row_sine = tables[pl.ds(SEQS + me, 1), :]
    lane1 = lax.broadcasted_iota(jnp.int32, (1, LANES), 1)
    fresh_scores = jnp.zeros((1, LANES), F32)
    for head in range(HEADS):
        query = query_rows[pl.ds(head * SEQS + me, 1), :]
        fresh_key = turned(summed[33 + head : 34 + head, :] * scale, row_cosine, row_sine)
        product = query * fresh_key.astype(F32)
        for side in range(2):
            fresh = jnp.sum(
                jnp.where(lane1 // DH == side, product, 0.0), axis=1, keepdims=True
            ) * DH ** (-0.5)
            at = me * 4 + head * 2 + side
            fresh_scores = fresh_scores + jnp.where(lane1 == at, fresh, 0.0)
    fresh_value = (summed[35:37, :] * scale).astype(BF16).astype(F32)
    tail = jnp.concatenate(
        [
            *thirds(jnp.sum(sums[0], axis=0, keepdims=True)),
            *thirds(fresh_scores),
            fresh_value,
        ],
        axis=0,
    ).astype(BF16)
    for dest in range(SEQS):
        out[dest, 64:72, :] = tail
    for group in range(1, 3):
        arrive(range(4 * group, 4 * group + 4))
        give(group, [value(2 * group), value(2 * group + 1)])
    arrive((12, 13))
    early = value(6)
    arrive((14, 15))
    give(3, [early, value(7)])


def thirds(x):
    high = x.astype(BF16).astype(F32)
    middle = (x - high).astype(BF16).astype(F32)
    return high, middle, x - high - middle


def finish_kernel(got, tables, head_gain, out_weight, out, factors, joined):
    rows16, _ = iotas(SEQS)
    tails = got[:, 64:72, :].astype(F32)

    def whole(at):
        return tails[:, at, :] + tails[:, at + 1, :] + tails[:, at + 2, :]

    left = lax.broadcasted_iota(jnp.int32, (1, LANES), 1) < 64
    both = whole(0)
    maxima = jnp.where(left, both, 0.0)
    totals = jnp.where(left, pltpu.roll(both, 64, 1), 1.0)
    fresh = jnp.sum(whole(3), axis=0, keepdims=True)
    block = tables[32:33, :].astype(jnp.int32) // 1024
    in_block = jnp.max(
        jnp.where(rows16 == block, maxima, floor_value), axis=0, keepdims=True
    )
    in_block = jnp.maximum(in_block, fresh)
    top = jnp.maximum(jnp.max(maxima, axis=0, keepdims=True), fresh)
    factor = jnp.exp(maxima - top)
    fresh_factor = jnp.exp(fresh - in_block).astype(BF16).astype(F32) * jnp.exp(in_block - top)
    total = jnp.sum(totals * factor, axis=0, keepdims=True) + fresh_factor
    part = tables[33:34, :] / total
    factors[...] = jnp.zeros((LANES, LANES), F32)
    factors[0:SEQS, :] = factor * part
    factors[SEQS : SEQS + 1, :] = fresh_factor * part
    columns = factors[...].T
    sub, _ = iotas(16)
    for four in range(SEQS // 4):
        here = columns[four * 16 : four * 16 + 16, :]
        fresh_value = jnp.zeros((16, LANES), F32)
        for n in range(8):
            line = tails[four * 4 + n // 2, 6 + n % 2 : 7 + n % 2, :]
            fresh_value = jnp.where(sub // 2 == n, line, fresh_value)
        joint = here[:, SEQS : SEQS + 1] * fresh_value
        for peer in range(SEQS):
            joint = joint + here[:, peer : peer + 1] * got[
                peer, four * 16 : four * 16 + 16, :
            ].astype(F32)
        joined[four * 16 : four * 16 + 16, :] = joint
    sides = []
    for head in range(HEADS):
        mixed = joined[pl.ds(2 * head, SEQS, 4), :] + joined[pl.ds(2 * head + 1, SEQS, 4), :]
        mean = jnp.mean(mixed * mixed, axis=1, keepdims=True)
        sides.append((mixed * lax.rsqrt(mean + epsilon) * head_gain[...]).astype(BF16))
    head_out = jnp.concatenate(sides, axis=1)
    partial_out = jnp.dot(
        head_out, out_weight[...], preferred_element_type=F32
    ).astype(BF16)
    for dest in range(8):
        out[dest] = partial_out


def attend_call(tables, got, keys, values, name):
    return pl.pallas_call(
        attend_kernel,
        in_specs=[VM, VM, ANY, ANY],
        out_specs=VM,
        out_shape=jax.ShapeDtypeStruct((SEQS, 72, LANES), BF16),
        scratch_shapes=[
            pltpu.VMEM(keys.shape, BF16),
            pltpu.VMEM(values.shape, BF16),
            pltpu.SemaphoreType.DMA((2, SEQS)),
            pltpu.VMEM((32, LANES), F32),
            pltpu.VMEM((SEQS, LANES), F32),
            pltpu.VMEM((64, 256), BF16),
            pltpu.VMEM((64, 2048), F32),
            pltpu.VMEM((64, 2048), BF16),
        ],
        compiler_params=BIG,
        name=name,
    )(tables, got, in_hbm(keys), in_hbm(values))


def local(
    tokens,
    norm_gain,
    query_weight,
    key_weight,
    value_weight,
    out_weight,
    lambdas,
    head_gain,
    lengths,
    key_cache,
    value_cache,
):
    rates = np.tile(theta_base ** (-np.arange(DH // 2) / (DH // 2)), 4)
    sent, tables = pl.pallas_call(
        project_kernel,
        in_specs=[ANY] * 8,
        out_specs=[VM, VM],
        out_shape=[
            jax.ShapeDtypeStruct((SEQS, 40, LANES), F32),
            jax.ShapeDtypeStruct((40, LANES), F32),
        ],
        scratch_shapes=[
            pltpu.VMEM((SEQS, 256), BF16),
            pltpu.VMEM((1, 256), F32),
            pltpu.VMEM((1, SEQS), jnp.int32),
            pltpu.VMEM((1, HEADS), F32),
            pltpu.VMEM((1, LANES), F32),
            pltpu.VMEM((3, 256, 256), BF16),
            pltpu.SemaphoreType.DMA((5,)),
            pltpu.SemaphoreType.DMA((3,)),
        ],
        compiler_params=SMALL,
        name="project",
    )(
        in_hbm(tokens),
        in_hbm(norm_gain.reshape(1, -1)),
        in_hbm(lengths.reshape(1, -1)),
        in_hbm(lambdas.reshape(1, -1)),
        in_hbm(jnp.asarray(rates, F32).reshape(1, -1)),
        in_hbm(query_weight),
        in_hbm(key_weight),
        in_hbm(value_weight),
    )
    got = lax.all_to_all(sent, "kv", split_axis=0, concat_axis=0, tiled=True)
    cache_shape = (SEQS, 2048, LANES)
    shared = attend_call(
        tables, got, key_cache.reshape(cache_shape), value_cache.reshape(cache_shape), "attend"
    )
    everyone = lax.all_to_all(shared, "kv", split_axis=0, concat_axis=0, tiled=True)
    partial_out = pl.pallas_call(
        finish_kernel,
        in_specs=[VM] * 4,
        out_specs=VM,
        out_shape=jax.ShapeDtypeStruct((8, SEQS, 256), BF16),
        scratch_shapes=[pltpu.VMEM((LANES, LANES), F32), pltpu.VMEM((64, LANES), F32)],
        compiler_params=SMALL,
        name="finish",
    )(everyone, tables, head_gain.reshape(1, -1), out_weight)
    shares = lax.all_to_all(partial_out, "tp", split_axis=0, concat_axis=0, tiled=True)
    return shares.astype(F32).sum(axis=0).astype(BF16)


def solution(mesh):
    return jax.shard_map(
        local,
        mesh=mesh,
        in_specs=(
            P(None, "kv"),
            P("kv"),
            P("kv", "tp"),
            P("kv", "tp"),
            P("kv", "tp"),
            P("tp", "kv"),
            P("tp"),
            P(),
            P(),
            P(None, "kv", "tp", None),
            P(None, "kv", "tp", None),
        ),
        out_specs=P(None, "kv"),
        check_vma=False,
    )
```

```python
import jax
import jax.numpy as jnp
import numpy as np
from jax import lax
from jax.experimental import pallas as pl
from jax.experimental.pallas import tpu as pltpu
from jax.sharding import PartitionSpec as P

D = 4096
DH = 64
HEADS = 2
SEQS = 16
LANES = 128

epsilon = 1e-05
theta_base = 500000.0
floor_value = -1e30

VM = pl.BlockSpec(memory_space=pltpu.VMEM)
SM = pl.BlockSpec(memory_space=pltpu.SMEM)
ANY = pl.BlockSpec(memory_space=pltpu.HBM)
F32 = jnp.float32
BF16 = jnp.bfloat16
SMALL = pltpu.CompilerParams(vmem_limit_bytes=16 * 1024 * 1024)
BIG = pltpu.CompilerParams(vmem_limit_bytes=26 * 1024 * 1024)


def in_hbm(x):
    return pltpu.with_memory_space_constraint(x, pltpu.HBM)


def in_vmem(x):
    return pltpu.with_memory_space_constraint(x, pltpu.VMEM)


def iotas(rows):
    shape = (rows, LANES)
    return lax.broadcasted_iota(jnp.int32, shape, 0), lax.broadcasted_iota(jnp.int32, shape, 1)


def project_kernel(
    tokens_in, gain_in, lengths_in, lambdas_in, rates_in, query_in, key_in, value_in, out,
    out_one, out_two, out_three, tables,
    tokens, gain, lengths, lambdas, rates, weights, fresh, small, large,
):
    near = [
        pltpu.make_async_copy(source, target, small.at[n])
        for n, (source, target) in enumerate(
            (
                (tokens_in, tokens),
                (gain_in, gain),
                (lengths_in, lengths),
                (lambdas_in, lambdas),
                (rates_in, rates),
            )
        )
    ]
    far = [
        pltpu.make_async_copy(source, weights.at[n], large.at[n])
        for n, source in enumerate((query_in, key_in, value_in))
    ]
    for copy in (*near, *far):
        copy.start()
    for copy in near:
        copy.wait()
    widened = tokens[...].astype(F32)
    squares = jnp.sum(widened * widened, axis=1, keepdims=True)
    normed = (widened * gain[...]).astype(BF16)
    row, lane = iotas(SEQS)
    square_row = jnp.sum(jnp.where(row == lane, squares, 0.0), axis=0, keepdims=True)
    row16 = lax.broadcasted_iota(jnp.int32, (SEQS, SEQS), 0)
    lane16 = lax.broadcasted_iota(jnp.int32, (SEQS, SEQS), 1)
    held = lengths[...].astype(F32)
    held_column = jnp.sum(jnp.where(row16 == lane16, held, 0.0), axis=1, keepdims=True)
    angles = held_column * rates[...]
    tables[0:16, :] = jnp.cos(angles)
    sine = jnp.sin(angles)
    tables[16:32, :] = jnp.where((lane // 32) % 2 == 0, -sine, sine)
    lane1 = lax.broadcasted_iota(jnp.int32, (1, LANES), 1)
    lambda_row = jnp.where((lane1 // 2) % 2 == 0, lambdas[:, 0:1], lambdas[:, 1:2])
    tables[32:40, :] = jnp.concatenate(
        [
            jnp.sum(jnp.where(row == lane // 4, held_column, 0.0), axis=0, keepdims=True),
            jnp.where(lane1 % 2 == 0, 1.0, -lambda_row),
            jnp.zeros((6, LANES), F32),
        ],
        axis=0,
    )
    products = []
    for n in range(3):
        far[n].wait()
        products.append(jnp.dot(normed, weights[n], preferred_element_type=F32))
    query, key, value = products
    fresh[0:16, :] = key[:, :LANES]
    fresh[16:32, :] = key[:, LANES:]
    fresh[32:48, :] = value[:, :LANES]
    fresh[48:64, :] = value[:, LANES:]
    column = lax.axis_index("kv") % 4
    head = jnp.concatenate([square_row, jnp.zeros((7, LANES), F32)], axis=0)
    for turn, target in enumerate((out, out_one, out_two, out_three)):
        target[0:16, :] = query[:, :LANES]
        target[16:32, :] = query[:, LANES:]
        target[32:40, :] = head
        other = column ^ turn
        target[40:56, :] = jnp.concatenate(
            [fresh[pl.ds(16 * part + other, 4, 4), :] for part in range(4)], axis=0
        )


def halfway_kernel(mine, one, two, three, out, out_one, out_two, out_three, total):
    total[...] = (mine[...] + one[...]) + (two[...] + three[...])
    plane = lax.axis_index("kv") // 4
    blank = jnp.zeros((3, LANES), F32)
    for turn, target in enumerate((out, out_one, out_two, out_three)):
        target[0:32, :] = total[0:32, :]
        target[32:40, :] = jnp.concatenate(
            [total[32:33, :], total[pl.ds(40 + (plane ^ turn), 4, 4), :], blank], axis=0
        )


def swapped(arrays, step):
    mine, *others = arrays
    return [
        mine,
        *(
            lax.ppermute(x, "kv", [(i, i ^ (step * (n + 1))) for i in range(16)])
            for n, x in enumerate(others)
        ),
    ]


def turned(x, cosine, sine):
    lane = lax.broadcasted_iota(jnp.int32, x.shape, 1)
    partner = jnp.where(
        (lane // 32) % 2 == 0, pltpu.roll(x, LANES - 32, 1), pltpu.roll(x, 32, 1)
    )
    return (x * cosine + partner * sine).astype(BF16)


def attend_kernel(
    tables, mine, one, two, three, keys, values, out, query_rows, scale_rows, asked_rows,
    score_rows, weight_rows,
):
    me = lax.axis_index("kv")
    cosine, sine = tables[0:16, :], tables[16:32, :]
    summed = (mine[...] + one[...]) + (two[...] + three[...])
    row, lane = iotas(SEQS)
    squares = jnp.sum(jnp.where(row == lane, summed[32:33, :], 0.0), axis=1, keepdims=True)
    scaling = jnp.broadcast_to(lax.rsqrt(squares / D + epsilon), (SEQS, LANES))
    scale_rows[...] = scaling
    for head in range(HEADS):
        turned_query = turned(
            summed[16 * head : 16 * head + 16, :] * scaling, cosine, sine
        )
        query_rows[head * SEQS : (head + 1) * SEQS, :] = turned_query.astype(F32)
    map_lanes = (lane // DH) == (row % 2)

    def row_of(head, seq):
        at = head * SEQS + seq
        return jnp.broadcast_to(query_rows[at : at + 1, :], (SEQS, LANES))

    for group in range(4):
        first = 4 * group
        left = jnp.where(
            row < 8,
            jnp.where(row < 2, row_of(0, first), row_of(1, first)),
            jnp.where(row < 10, row_of(0, first + 2), row_of(1, first + 2)),
        )
        right = jnp.where(
            row < 8,
            jnp.where(row < 6, row_of(0, first + 1), row_of(1, first + 1)),
            jnp.where(row < 14, row_of(0, first + 3), row_of(1, first + 3)),
        )
        left = jnp.where(map_lanes & (row % 8 < 4), left, 0.0)
        right = jnp.where(map_lanes & (row % 8 >= 4), right, 0.0)
        asked_rows[group * 16 : group * 16 + 16, :] = jnp.concatenate(
            [left, right], axis=1
        ).astype(BF16)

    columns = lax.broadcasted_iota(jnp.int32, (SEQS, 2048), 1)
    subs = lax.broadcasted_iota(jnp.int32, (SEQS, 2048), 0)
    own_head = (columns % 2) == ((subs // 2) % 2)
    lengths_of = tables[32:33, :].astype(jnp.int32)
    sums = [jnp.zeros((SEQS, LANES), F32)]

    def score(group):
        for pair in (2 * group, 2 * group + 1):
            at = slice(pair * 8, pair * 8 + 8)
            both_keys = jnp.concatenate([keys[2 * pair], keys[2 * pair + 1]], axis=1)
            score_rows[at, :] = lax.dot_general(
                asked_rows[at, :],
                both_keys,
                (((1,), (1,)), ((), ())),
                preferred_element_type=F32,
            )

    def weigh(group):
        at = slice(group * 16, group * 16 + 16)
        place = lane == group * 16 + row
        limit = jnp.sum(jnp.where(place, lengths_of, 0), axis=1, keepdims=True)
        visible = own_head & (columns < 2 * (limit - me * 1024))
        masked = jnp.where(visible, score_rows[at, :] * DH ** (-0.5), floor_value)
        highest = jnp.max(masked, axis=1, keepdims=True)
        weights = jnp.where(visible, jnp.exp(masked - highest), 0.0).astype(BF16)
        weight_rows[at, :] = weights
        total = jnp.sum(weights.astype(F32), axis=1, keepdims=True)
        beside = lane == 64 + group * 16 + row
        sums[0] = sums[0] + jnp.where(place, highest, jnp.where(beside, total, 0.0))

    def value(pair):
        both_values = jnp.concatenate([values[2 * pair], values[2 * pair + 1]], axis=1)
        valued = jnp.dot(
            weight_rows[pair * 8 : pair * 8 + 8, :], both_values, preferred_element_type=F32
        )
        return jnp.where(row[:8] < 4, valued[:, :LANES], valued[:, LANES:])

    def give(group, parts):
        sixteen = jnp.concatenate(parts, axis=0).astype(BF16)
        for dest in range(SEQS):
            out[dest, group * 16 : group * 16 + 16, :] = sixteen

    score(0)
    for group in range(1, 4):
        score(group)
        weigh(group - 1)
    give(0, [value(0), value(1)])
    weigh(3)
    scale = scale_rows[pl.ds(me, 1), :]
    row_cosine = tables[pl.ds(me, 1), :]
    row_sine = tables[pl.ds(SEQS + me, 1), :]
    lane1 = lax.broadcasted_iota(jnp.int32, (1, LANES), 1)
    fresh_scores = jnp.zeros((1, LANES), F32)
    for head in range(HEADS):
        query = query_rows[pl.ds(head * SEQS + me, 1), :]
        fresh_key = turned(summed[33 + head : 34 + head, :] * scale, row_cosine, row_sine)
        product = query * fresh_key.astype(F32)
        for side in range(2):
            fresh = jnp.sum(
                jnp.where(lane1 // DH == side, product, 0.0), axis=1, keepdims=True
            ) * DH ** (-0.5)
            at = me * 4 + head * 2 + side
            fresh_scores = fresh_scores + jnp.where(lane1 == at, fresh, 0.0)
    fresh_value = (summed[35:37, :] * scale).astype(BF16).astype(F32)
    tail = jnp.concatenate(
        [
            *thirds(jnp.sum(sums[0], axis=0, keepdims=True)),
            *thirds(fresh_scores),
            fresh_value,
        ],
        axis=0,
    ).astype(BF16)
    for dest in range(SEQS):
        out[dest, 64:72, :] = tail
    for group in range(1, 4):
        give(group, [value(2 * group), value(2 * group + 1)])


def thirds(x):
    high = x.astype(BF16).astype(F32)
    middle = (x - high).astype(BF16).astype(F32)
    return high, middle, x - high - middle


def finish_kernel(got, tables, head_gain, out_weight, out, factors, joined):
    rows16, _ = iotas(SEQS)
    tails = got[:, 64:72, :].astype(F32)

    def whole(at):
        return tails[:, at, :] + tails[:, at + 1, :] + tails[:, at + 2, :]

    left = lax.broadcasted_iota(jnp.int32, (1, LANES), 1) < 64
    both = whole(0)
    maxima = jnp.where(left, both, 0.0)
    totals = jnp.where(left, pltpu.roll(both, 64, 1), 1.0)
    fresh = jnp.sum(whole(3), axis=0, keepdims=True)
    block = tables[32:33, :].astype(jnp.int32) // 1024
    in_block = jnp.max(
        jnp.where(rows16 == block, maxima, floor_value), axis=0, keepdims=True
    )
    in_block = jnp.maximum(in_block, fresh)
    top = jnp.maximum(jnp.max(maxima, axis=0, keepdims=True), fresh)
    factor = jnp.exp(maxima - top)
    fresh_factor = jnp.exp(fresh - in_block).astype(BF16).astype(F32) * jnp.exp(in_block - top)
    total = jnp.sum(totals * factor, axis=0, keepdims=True) + fresh_factor
    part = tables[33:34, :] / total
    factors[...] = jnp.zeros((LANES, LANES), F32)
    factors[0:SEQS, :] = factor * part
    factors[SEQS : SEQS + 1, :] = fresh_factor * part
    columns = factors[...].T
    sub, _ = iotas(16)
    for four in range(SEQS // 4):
        here = columns[four * 16 : four * 16 + 16, :]
        fresh_value = jnp.zeros((16, LANES), F32)
        for n in range(8):
            line = tails[four * 4 + n // 2, 6 + n % 2 : 7 + n % 2, :]
            fresh_value = jnp.where(sub // 2 == n, line, fresh_value)
        joint = here[:, SEQS : SEQS + 1] * fresh_value
        for peer in range(SEQS):
            joint = joint + here[:, peer : peer + 1] * got[
                peer, four * 16 : four * 16 + 16, :
            ].astype(F32)
        joined[four * 16 : four * 16 + 16, :] = joint
    sides = []
    for head in range(HEADS):
        mixed = joined[pl.ds(2 * head, SEQS, 4), :] + joined[pl.ds(2 * head + 1, SEQS, 4), :]
        mean = jnp.mean(mixed * mixed, axis=1, keepdims=True)
        sides.append((mixed * lax.rsqrt(mean + epsilon) * head_gain[...]).astype(BF16))
    head_out = jnp.concatenate(sides, axis=1)
    partial_out = jnp.dot(
        head_out, out_weight[...], preferred_element_type=F32
    ).astype(BF16)
    for dest in range(8):
        out[dest] = partial_out


def load_kernel(source, target, arrived):
    copies = [
        pltpu.make_async_copy(
            source.at[pl.ds(4 * n, 4)], target.at[pl.ds(4 * n, 4)], arrived.at[n]
        )
        for n in range(4)
    ]
    for copy in copies:
        copy.start()
    for copy in copies:
        copy.wait()


def load_call(source, name):
    return pl.pallas_call(
        load_kernel,
        in_specs=[ANY],
        out_specs=VM,
        out_shape=pltpu.VMEM(source.shape, BF16),
        scratch_shapes=[pltpu.SemaphoreType.DMA((4,))],
        compiler_params=SMALL,
        cost_estimate=pl.CostEstimate(flops=2**31, bytes_accessed=2**24, transcendentals=0),
        name=name,
    )(in_hbm(source))


def attend_call(tables, got, keys, values, name):
    return pl.pallas_call(
        attend_kernel,
        in_specs=[VM] * 7,
        out_specs=VM,
        out_shape=jax.ShapeDtypeStruct((SEQS, 72, LANES), BF16),
        scratch_shapes=[
            pltpu.VMEM((32, LANES), F32),
            pltpu.VMEM((SEQS, LANES), F32),
            pltpu.VMEM((64, 256), BF16),
            pltpu.VMEM((64, 2048), F32),
            pltpu.VMEM((64, 2048), BF16),
        ],
        compiler_params=BIG,
        name=name,
    )(tables, *got, keys, values)


def local(
    tokens,
    norm_gain,
    query_weight,
    key_weight,
    value_weight,
    out_weight,
    lambdas,
    head_gain,
    lengths,
    key_cache,
    value_cache,
):
    rates = np.tile(theta_base ** (-np.arange(DH // 2) / (DH // 2)), 4)
    *sent, tables = pl.pallas_call(
        project_kernel,
        in_specs=[ANY] * 8,
        out_specs=[VM] * 5,
        out_shape=[
            *[jax.ShapeDtypeStruct((56, LANES), F32)] * 4,
            jax.ShapeDtypeStruct((40, LANES), F32),
        ],
        scratch_shapes=[
            pltpu.VMEM((SEQS, 256), BF16),
            pltpu.VMEM((1, 256), F32),
            pltpu.VMEM((1, SEQS), jnp.int32),
            pltpu.VMEM((1, HEADS), F32),
            pltpu.VMEM((1, LANES), F32),
            pltpu.VMEM((3, 256, 256), BF16),
            pltpu.VMEM((64, LANES), F32),
            pltpu.SemaphoreType.DMA((5,)),
            pltpu.SemaphoreType.DMA((3,)),
        ],
        compiler_params=SMALL,
        name="project",
    )(
        in_hbm(tokens),
        in_hbm(norm_gain.reshape(1, -1)),
        in_hbm(lengths.reshape(1, -1)),
        in_hbm(lambdas.reshape(1, -1)),
        in_hbm(jnp.asarray(rates, F32).reshape(1, -1)),
        in_hbm(query_weight),
        in_hbm(key_weight),
        in_hbm(value_weight),
    )
    halves = pl.pallas_call(
        halfway_kernel,
        in_specs=[VM] * 4,
        out_specs=[VM] * 4,
        out_shape=[jax.ShapeDtypeStruct((40, LANES), F32)] * 4,
        scratch_shapes=[pltpu.VMEM((56, LANES), F32)],
        compiler_params=SMALL,
        name="halfway",
    )(*swapped(sent, 1))
    got = swapped(halves, 4)
    cache_shape = (SEQS, 2048, LANES)
    shared = attend_call(
        tables,
        got,
        load_call(key_cache.reshape(cache_shape), "keys"),
        load_call(value_cache.reshape(cache_shape), "values"),
        "attend",
    )
    everyone = lax.all_to_all(shared, "kv", split_axis=0, concat_axis=0, tiled=True)
    partial_out = pl.pallas_call(
        finish_kernel,
        in_specs=[VM] * 4,
        out_specs=VM,
        out_shape=jax.ShapeDtypeStruct((8, SEQS, 256), BF16),
        scratch_shapes=[pltpu.VMEM((LANES, LANES), F32), pltpu.VMEM((64, LANES), F32)],
        compiler_params=SMALL,
        name="finish",
    )(everyone, tables, head_gain.reshape(1, -1), out_weight)
    shares = lax.all_to_all(partial_out, "tp", split_axis=0, concat_axis=0, tiled=True)
    return shares.astype(F32).sum(axis=0).astype(BF16)


def solution(mesh):
    return jax.shard_map(
        local,
        mesh=mesh,
        in_specs=(
            P(None, "kv"),
            P("kv"),
            P("kv", "tp"),
            P("kv", "tp"),
            P("kv", "tp"),
            P("tp", "kv"),
            P("tp"),
            P(),
            P(),
            P(None, "kv", "tp", None),
            P(None, "kv", "tp", None),
        ),
        out_specs=P(None, "kv"),
        check_vma=False,
    )
```

```python
import jax
import jax.numpy as jnp
import numpy as np
from jax import lax
from jax.experimental import pallas as pl
from jax.experimental.pallas import tpu as pltpu
from jax.sharding import PartitionSpec as P

D = 4096
DH = 64
HEADS = 2
SEQS = 16
LANES = 128

epsilon = 1e-05
theta_base = 500000.0
floor_value = -1e30
EARLY = 5

VM = pl.BlockSpec(memory_space=pltpu.VMEM)
SM = pl.BlockSpec(memory_space=pltpu.SMEM)
ANY = pl.BlockSpec(memory_space=pltpu.HBM)
F32 = jnp.float32
BF16 = jnp.bfloat16
SMALL = pltpu.CompilerParams(vmem_limit_bytes=8 * 1024 * 1024)
BIG = pltpu.CompilerParams(vmem_limit_bytes=30 * 1024 * 1024)


def in_hbm(x):
    return pltpu.with_memory_space_constraint(x, pltpu.HBM)


def iotas(rows):
    shape = (rows, LANES)
    return lax.broadcasted_iota(jnp.int32, shape, 0), lax.broadcasted_iota(jnp.int32, shape, 1)


def project_kernel(
    tokens_in, gain_in, lengths_in, lambdas_in, rates_in, query_in, key_in, value_in, keys_in, out,
    tables, early_keys, tokens, gain, lengths, lambdas, rates, weights, small, large, early,
):
    near = [
        pltpu.make_async_copy(source, target, small.at[n])
        for n, (source, target) in enumerate(
            (
                (tokens_in, tokens),
                (gain_in, gain),
                (lengths_in, lengths),
                (lambdas_in, lambdas),
                (rates_in, rates),
            )
        )
    ]
    far = [
        pltpu.make_async_copy(source, weights.at[n], large.at[n])
        for n, source in enumerate((query_in, key_in, value_in))
    ]
    ahead = [
        pltpu.make_async_copy(keys_in.at[n], early_keys.at[n], early.at[n]) for n in range(EARLY)
    ]
    for copy in (*near, *far, *ahead):
        copy.start()
    for copy in near:
        copy.wait()
    widened = tokens[...].astype(F32)
    squares = jnp.sum(widened * widened, axis=1, keepdims=True)
    normed = (widened * gain[...]).astype(BF16)
    row, lane = iotas(SEQS)
    square_row = jnp.sum(jnp.where(row == lane, squares, 0.0), axis=0, keepdims=True)
    row16 = lax.broadcasted_iota(jnp.int32, (SEQS, SEQS), 0)
    lane16 = lax.broadcasted_iota(jnp.int32, (SEQS, SEQS), 1)
    held = lengths[...].astype(F32)
    held_column = jnp.sum(jnp.where(row16 == lane16, held, 0.0), axis=1, keepdims=True)
    angles = held_column * rates[...]
    tables[0:16, :] = jnp.cos(angles)
    sine = jnp.sin(angles)
    tables[16:32, :] = jnp.where((lane // 32) % 2 == 0, -sine, sine)
    lane1 = lax.broadcasted_iota(jnp.int32, (1, LANES), 1)
    lambda_row = jnp.where((lane1 // 2) % 2 == 0, lambdas[:, 0:1], lambdas[:, 1:2])
    tables[32:40, :] = jnp.concatenate(
        [
            jnp.sum(jnp.where(row == lane // 4, held_column, 0.0), axis=0, keepdims=True),
            jnp.where(lane1 % 2 == 0, 1.0, -lambda_row),
            jnp.zeros((6, LANES), F32),
        ],
        axis=0,
    )
    products = []
    for n in range(3):
        far[n].wait()
        products.append(jnp.dot(normed, weights[n], preferred_element_type=F32))
    query, key, value = products
    blank = jnp.zeros((3, LANES), F32)
    for dest in range(SEQS):
        out[dest, 0:16, :] = query[:, :LANES]
        out[dest, 16:32, :] = query[:, LANES:]
        out[dest, 32:40, :] = jnp.concatenate(
            [
                square_row,
                key[dest : dest + 1, :LANES],
                key[dest : dest + 1, LANES:],
                value[dest : dest + 1, :LANES],
                value[dest : dest + 1, LANES:],
                blank,
            ],
            axis=0,
        )
    for copy in ahead:
        copy.wait()


def turned(x, cosine, sine):
    lane = lax.broadcasted_iota(jnp.int32, x.shape, 1)
    partner = jnp.where(
        (lane // 32) % 2 == 0, pltpu.roll(x, LANES - 32, 1), pltpu.roll(x, 32, 1)
    )
    return (x * cosine + partner * sine).astype(BF16)


def attend_kernel(
    tables, got, early_keys, keys_in, values_in, out, keys, values, arrived, query_rows, scale_rows,
    asked_rows, score_rows, weight_rows,
):
    key_copies = {
        seq: pltpu.make_async_copy(keys_in.at[seq], keys.at[seq - EARLY], arrived.at[0, seq])
        for seq in range(EARLY, SEQS)
    }
    value_copies = [
        pltpu.make_async_copy(values_in.at[seq], values.at[seq], arrived.at[1, seq])
        for seq in range(SEQS)
    ]
    for copy in (*key_copies.values(), *value_copies):
        copy.start()

    def keys_of(seq):
        return early_keys[seq] if seq < EARLY else keys[seq - EARLY]

    me = lax.axis_index("kv")
    cosine, sine = tables[0:16, :], tables[16:32, :]
    summed = jnp.sum(got[...], axis=0)
    row, lane = iotas(SEQS)
    squares = jnp.sum(jnp.where(row == lane, summed[32:33, :], 0.0), axis=1, keepdims=True)
    scaling = jnp.broadcast_to(lax.rsqrt(squares / D + epsilon), (SEQS, LANES))
    scale_rows[...] = scaling
    for head in range(HEADS):
        turned_query = turned(
            summed[16 * head : 16 * head + 16, :] * scaling, cosine, sine
        )
        query_rows[head * SEQS : (head + 1) * SEQS, :] = turned_query.astype(F32)
    map_lanes = (lane // DH) == (row % 2)

    def row_of(head, seq):
        at = head * SEQS + seq
        return jnp.broadcast_to(query_rows[at : at + 1, :], (SEQS, LANES))

    for group in range(4):
        first = 4 * group
        left = jnp.where(
            row < 8,
            jnp.where(row < 2, row_of(0, first), row_of(1, first)),
            jnp.where(row < 10, row_of(0, first + 2), row_of(1, first + 2)),
        )
        right = jnp.where(
            row < 8,
            jnp.where(row < 6, row_of(0, first + 1), row_of(1, first + 1)),
            jnp.where(row < 14, row_of(0, first + 3), row_of(1, first + 3)),
        )
        left = jnp.where(map_lanes & (row % 8 < 4), left, 0.0)
        right = jnp.where(map_lanes & (row % 8 >= 4), right, 0.0)
        asked_rows[group * 16 : group * 16 + 16, :] = jnp.concatenate(
            [left, right], axis=1
        ).astype(BF16)

    columns = lax.broadcasted_iota(jnp.int32, (SEQS, 2048), 1)
    subs = lax.broadcasted_iota(jnp.int32, (SEQS, 2048), 0)
    own_head = (columns % 2) == ((subs // 2) % 2)
    lengths_of = tables[32:33, :].astype(jnp.int32)
    sums = [jnp.zeros((SEQS, LANES), F32)]

    def score(group):
        for seq in range(4 * group, 4 * group + 4):
            if seq >= EARLY:
                key_copies[seq].wait()
        for pair in (2 * group, 2 * group + 1):
            at = slice(pair * 8, pair * 8 + 8)
            both_keys = jnp.concatenate([keys_of(2 * pair), keys_of(2 * pair + 1)], axis=1)
            score_rows[at, :] = lax.dot_general(
                asked_rows[at, :],
                both_keys,
                (((1,), (1,)), ((), ())),
                preferred_element_type=F32,
            )

    def weigh(group):
        at = slice(group * 16, group * 16 + 16)
        place = lane == group * 16 + row
        limit = jnp.sum(jnp.where(place, lengths_of, 0), axis=1, keepdims=True)
        visible = own_head & (columns < 2 * (limit - me * 1024))
        masked = jnp.where(visible, score_rows[at, :] * DH ** (-0.5), floor_value)
        highest = jnp.max(masked, axis=1, keepdims=True)
        weights = jnp.where(visible, jnp.exp(masked - highest), 0.0).astype(BF16)
        weight_rows[at, :] = weights
        total = jnp.sum(weights.astype(F32), axis=1, keepdims=True)
        beside = lane == 64 + group * 16 + row
        sums[0] = sums[0] + jnp.where(place, highest, jnp.where(beside, total, 0.0))

    def value(pair):
        both_values = jnp.concatenate([values[2 * pair], values[2 * pair + 1]], axis=1)
        valued = jnp.dot(
            weight_rows[pair * 8 : pair * 8 + 8, :], both_values, preferred_element_type=F32
        )
        return jnp.where(row[:8] < 4, valued[:, :LANES], valued[:, LANES:])

    def arrive(seqs):
        for seq in seqs:
            value_copies[seq].wait()

    def give(group, parts):
        sixteen = jnp.concatenate(parts, axis=0).astype(BF16)
        for dest in range(SEQS):
            out[dest, group * 16 : group * 16 + 16, :] = sixteen

    score(0)
    for group in range(1, 4):
        score(group)
        weigh(group - 1)
    arrive(range(4))
    give(0, [value(0), value(1)])
    weigh(3)
    scale = scale_rows[pl.ds(me, 1), :]
    row_cosine = tables[pl.ds(me, 1), :]
    row_sine = tables[pl.ds(SEQS + me, 1), :]
    lane1 = lax.broadcasted_iota(jnp.int32, (1, LANES), 1)
    fresh_scores = jnp.zeros((1, LANES), F32)
    for head in range(HEADS):
        query = query_rows[pl.ds(head * SEQS + me, 1), :]
        fresh_key = turned(summed[33 + head : 34 + head, :] * scale, row_cosine, row_sine)
        product = query * fresh_key.astype(F32)
        for side in range(2):
            fresh = jnp.sum(
                jnp.where(lane1 // DH == side, product, 0.0), axis=1, keepdims=True
            ) * DH ** (-0.5)
            at = me * 4 + head * 2 + side
            fresh_scores = fresh_scores + jnp.where(lane1 == at, fresh, 0.0)
    fresh_value = (summed[35:37, :] * scale).astype(BF16).astype(F32)
    tail = jnp.concatenate(
        [
            *thirds(jnp.sum(sums[0], axis=0, keepdims=True)),
            *thirds(fresh_scores),
            fresh_value,
        ],
        axis=0,
    ).astype(BF16)
    for dest in range(SEQS):
        out[dest, 64:72, :] = tail
    for group in range(1, 3):
        arrive(range(4 * group, 4 * group + 4))
        give(group, [value(2 * group), value(2 * group + 1)])
    arrive((12, 13))
    early = value(6)
    arrive((14, 15))
    give(3, [early, value(7)])


def thirds(x):
    high = x.astype(BF16).astype(F32)
    middle = (x - high).astype(BF16).astype(F32)
    return high, middle, x - high - middle


def finish_kernel(got, tables, head_gain, out_weight, out, factors, joined):
    rows16, _ = iotas(SEQS)
    tails = got[:, 64:72, :].astype(F32)

    def whole(at):
        return tails[:, at, :] + tails[:, at + 1, :] + tails[:, at + 2, :]

    left = lax.broadcasted_iota(jnp.int32, (1, LANES), 1) < 64
    both = whole(0)
    maxima = jnp.where(left, both, 0.0)
    totals = jnp.where(left, pltpu.roll(both, 64, 1), 1.0)
    fresh = jnp.sum(whole(3), axis=0, keepdims=True)
    block = tables[32:33, :].astype(jnp.int32) // 1024
    in_block = jnp.max(
        jnp.where(rows16 == block, maxima, floor_value), axis=0, keepdims=True
    )
    in_block = jnp.maximum(in_block, fresh)
    top = jnp.maximum(jnp.max(maxima, axis=0, keepdims=True), fresh)
    factor = jnp.exp(maxima - top)
    fresh_factor = jnp.exp(fresh - in_block).astype(BF16).astype(F32) * jnp.exp(in_block - top)
    total = jnp.sum(totals * factor, axis=0, keepdims=True) + fresh_factor
    part = tables[33:34, :] / total
    factors[...] = jnp.zeros((LANES, LANES), F32)
    factors[0:SEQS, :] = factor * part
    factors[SEQS : SEQS + 1, :] = fresh_factor * part
    columns = factors[...].T
    sub, _ = iotas(16)
    for four in range(SEQS // 4):
        here = columns[four * 16 : four * 16 + 16, :]
        fresh_value = jnp.zeros((16, LANES), F32)
        for n in range(8):
            line = tails[four * 4 + n // 2, 6 + n % 2 : 7 + n % 2, :]
            fresh_value = jnp.where(sub // 2 == n, line, fresh_value)
        joint = here[:, SEQS : SEQS + 1] * fresh_value
        for peer in range(SEQS):
            joint = joint + here[:, peer : peer + 1] * got[
                peer, four * 16 : four * 16 + 16, :
            ].astype(F32)
        joined[four * 16 : four * 16 + 16, :] = joint
    sides = []
    for head in range(HEADS):
        mixed = joined[pl.ds(2 * head, SEQS, 4), :] + joined[pl.ds(2 * head + 1, SEQS, 4), :]
        mean = jnp.mean(mixed * mixed, axis=1, keepdims=True)
        sides.append((mixed * lax.rsqrt(mean + epsilon) * head_gain[...]).astype(BF16))
    head_out = jnp.concatenate(sides, axis=1)
    partial_out = jnp.dot(
        head_out, out_weight[...], preferred_element_type=F32
    ).astype(BF16)
    for dest in range(8):
        out[dest] = partial_out


def attend_call(tables, got, early_keys, keys, values, name):
    return pl.pallas_call(
        attend_kernel,
        in_specs=[VM, VM, VM, ANY, ANY],
        out_specs=VM,
        out_shape=jax.ShapeDtypeStruct((SEQS, 72, LANES), BF16),
        scratch_shapes=[
            pltpu.VMEM((SEQS - EARLY, *keys.shape[1:]), BF16),
            pltpu.VMEM(values.shape, BF16),
            pltpu.SemaphoreType.DMA((2, SEQS)),
            pltpu.VMEM((32, LANES), F32),
            pltpu.VMEM((SEQS, LANES), F32),
            pltpu.VMEM((64, 256), BF16),
            pltpu.VMEM((64, 2048), F32),
            pltpu.VMEM((64, 2048), BF16),
        ],
        compiler_params=BIG,
        name=name,
    )(tables, got, early_keys, in_hbm(keys), in_hbm(values))


def local(
    tokens,
    norm_gain,
    query_weight,
    key_weight,
    value_weight,
    out_weight,
    lambdas,
    head_gain,
    lengths,
    key_cache,
    value_cache,
):
    cache_shape = (SEQS, 2048, LANES)
    keys = key_cache.reshape(cache_shape)
    rates = np.tile(theta_base ** (-np.arange(DH // 2) / (DH // 2)), 4)
    sent, tables, early_keys = pl.pallas_call(
        project_kernel,
        in_specs=[ANY] * 9,
        out_specs=[VM] * 3,
        out_shape=[
            jax.ShapeDtypeStruct((SEQS, 40, LANES), F32),
            jax.ShapeDtypeStruct((40, LANES), F32),
            pltpu.VMEM((EARLY, *cache_shape[1:]), BF16),
        ],
        scratch_shapes=[
            pltpu.VMEM((SEQS, 256), BF16),
            pltpu.VMEM((1, 256), F32),
            pltpu.VMEM((1, SEQS), jnp.int32),
            pltpu.VMEM((1, HEADS), F32),
            pltpu.VMEM((1, LANES), F32),
            pltpu.VMEM((3, 256, 256), BF16),
            pltpu.SemaphoreType.DMA((5,)),
            pltpu.SemaphoreType.DMA((3,)),
            pltpu.SemaphoreType.DMA((EARLY,)),
        ],
        compiler_params=SMALL,
        name="project",
    )(
        in_hbm(tokens),
        in_hbm(norm_gain.reshape(1, -1)),
        in_hbm(lengths.reshape(1, -1)),
        in_hbm(lambdas.reshape(1, -1)),
        in_hbm(jnp.asarray(rates, F32).reshape(1, -1)),
        in_hbm(query_weight),
        in_hbm(key_weight),
        in_hbm(value_weight),
        in_hbm(keys),
    )
    got = lax.all_to_all(sent, "kv", split_axis=0, concat_axis=0, tiled=True)
    shared = attend_call(
        tables, got, early_keys, keys, value_cache.reshape(cache_shape), "attend"
    )
    everyone = lax.all_to_all(shared, "kv", split_axis=0, concat_axis=0, tiled=True)
    partial_out = pl.pallas_call(
        finish_kernel,
        in_specs=[VM] * 4,
        out_specs=VM,
        out_shape=jax.ShapeDtypeStruct((8, SEQS, 256), BF16),
        scratch_shapes=[pltpu.VMEM((LANES, LANES), F32), pltpu.VMEM((64, LANES), F32)],
        compiler_params=SMALL,
        name="finish",
    )(everyone, tables, head_gain.reshape(1, -1), out_weight)
    shares = lax.all_to_all(partial_out, "tp", split_axis=0, concat_axis=0, tiled=True)
    return shares.astype(F32).sum(axis=0).astype(BF16)


def solution(mesh):
    return jax.shard_map(
        local,
        mesh=mesh,
        in_specs=(
            P(None, "kv"),
            P("kv"),
            P("kv", "tp"),
            P("kv", "tp"),
            P("kv", "tp"),
            P("tp", "kv"),
            P("tp"),
            P(),
            P(),
            P(None, "kv", "tp", None),
            P(None, "kv", "tp", None),
        ),
        out_specs=P(None, "kv"),
        check_vma=False,
    )
```

```python
import jax
import jax.numpy as jnp
import numpy as np
from jax import lax
from jax.experimental import pallas as pl
from jax.experimental.pallas import tpu as pltpu
from jax.sharding import PartitionSpec as P

D = 4096
DH = 64
HEADS = 2
SEQS = 16
LANES = 128

epsilon = 1e-05
theta_base = 500000.0
floor_value = -1e30

VM = pl.BlockSpec(memory_space=pltpu.VMEM)
SM = pl.BlockSpec(memory_space=pltpu.SMEM)
ANY = pl.BlockSpec(memory_space=pltpu.HBM)
F32 = jnp.float32
BF16 = jnp.bfloat16
SMALL = pltpu.CompilerParams(vmem_limit_bytes=8 * 1024 * 1024)
BIG = pltpu.CompilerParams(vmem_limit_bytes=30 * 1024 * 1024)


def in_hbm(x):
    return pltpu.with_memory_space_constraint(x, pltpu.HBM)


def iotas(rows):
    shape = (rows, LANES)
    return lax.broadcasted_iota(jnp.int32, shape, 0), lax.broadcasted_iota(jnp.int32, shape, 1)


def project_kernel(
    tokens_in, gain_in, lengths_in, lambdas_in, rates_in, query_in, key_in, value_in, out, tables,
    tokens, gain, lengths, lambdas, rates, weights, small, large,
):
    near = [
        pltpu.make_async_copy(source, target, small.at[n])
        for n, (source, target) in enumerate(
            (
                (tokens_in, tokens),
                (gain_in, gain),
                (lengths_in, lengths),
                (lambdas_in, lambdas),
                (rates_in, rates),
            )
        )
    ]
    far = [
        pltpu.make_async_copy(source, weights.at[:, 256 * n : 256 * n + 256], large.at[n])
        for n, source in enumerate((query_in, key_in, value_in))
    ]
    for copy in (*near, *far):
        copy.start()
    for copy in near:
        copy.wait()
    widened = tokens[...].astype(F32)
    squares = jnp.sum(widened * widened, axis=1, keepdims=True)
    normed = (widened * gain[...]).astype(BF16)
    row, lane = iotas(SEQS)
    square_row = jnp.sum(jnp.where(row == lane, squares, 0.0), axis=0, keepdims=True)
    row16 = lax.broadcasted_iota(jnp.int32, (SEQS, SEQS), 0)
    lane16 = lax.broadcasted_iota(jnp.int32, (SEQS, SEQS), 1)
    held = lengths[...].astype(F32)
    held_column = jnp.sum(jnp.where(row16 == lane16, held, 0.0), axis=1, keepdims=True)
    angles = held_column * rates[...]
    tables[0:16, :] = jnp.cos(angles)
    sine = jnp.sin(angles)
    tables[16:32, :] = jnp.where((lane // 32) % 2 == 0, -sine, sine)
    lane1 = lax.broadcasted_iota(jnp.int32, (1, LANES), 1)
    lambda_row = jnp.where((lane1 // 2) % 2 == 0, lambdas[:, 0:1], lambdas[:, 1:2])
    tables[32:40, :] = jnp.concatenate(
        [
            jnp.sum(jnp.where(row == lane // 4, held_column, 0.0), axis=0, keepdims=True),
            jnp.where(lane1 % 2 == 0, 1.0, -lambda_row),
            jnp.zeros((6, LANES), F32),
        ],
        axis=0,
    )
    for copy in far:
        copy.wait()
    products = jnp.dot(normed, weights[...], preferred_element_type=F32)
    query, key, value = products[:, :256], products[:, 256:512], products[:, 512:]
    blank = jnp.zeros((3, LANES), F32)
    for dest in range(SEQS):
        out[dest, 0:16, :] = query[:, :LANES]
        out[dest, 16:32, :] = query[:, LANES:]
        out[dest, 32:40, :] = jnp.concatenate(
            [
                square_row,
                key[dest : dest + 1, :LANES],
                key[dest : dest + 1, LANES:],
                value[dest : dest + 1, :LANES],
                value[dest : dest + 1, LANES:],
                blank,
            ],
            axis=0,
        )


def turned(x, cosine, sine):
    lane = lax.broadcasted_iota(jnp.int32, x.shape, 1)
    partner = jnp.where(
        (lane // 32) % 2 == 0, pltpu.roll(x, LANES - 32, 1), pltpu.roll(x, 32, 1)
    )
    return (x * cosine + partner * sine).astype(BF16)


def attend_kernel(
    tables, got, keys_in, values_in, out, keys, values, arrived, query_rows, scale_rows,
    asked_rows, score_rows, weight_rows,
):
    copies = []
    for kind, (source, target) in enumerate(((keys_in, keys), (values_in, values))):
        for seq in range(SEQS):
            copies.append(
                pltpu.make_async_copy(source.at[seq], target.at[seq], arrived.at[kind, seq])
            )
    for copy in copies:
        copy.start()
    me = lax.axis_index("kv")
    cosine, sine = tables[0:16, :], tables[16:32, :]
    summed = jnp.sum(got[...], axis=0)
    row, lane = iotas(SEQS)
    squares = jnp.sum(jnp.where(row == lane, summed[32:33, :], 0.0), axis=1, keepdims=True)
    scaling = jnp.broadcast_to(lax.rsqrt(squares / D + epsilon), (SEQS, LANES))
    scale_rows[...] = scaling
    for head in range(HEADS):
        turned_query = turned(
            summed[16 * head : 16 * head + 16, :] * scaling, cosine, sine
        )
        query_rows[head * SEQS : (head + 1) * SEQS, :] = turned_query.astype(F32)
    map_lanes = (lane // DH) == (row % 2)

    def row_of(head, seq):
        at = head * SEQS + seq
        return jnp.broadcast_to(query_rows[at : at + 1, :], (SEQS, LANES))

    for group in range(4):
        first = 4 * group
        left = jnp.where(
            row < 8,
            jnp.where(row < 2, row_of(0, first), row_of(1, first)),
            jnp.where(row < 10, row_of(0, first + 2), row_of(1, first + 2)),
        )
        right = jnp.where(
            row < 8,
            jnp.where(row < 6, row_of(0, first + 1), row_of(1, first + 1)),
            jnp.where(row < 14, row_of(0, first + 3), row_of(1, first + 3)),
        )
        left = jnp.where(map_lanes & (row % 8 < 4), left, 0.0)
        right = jnp.where(map_lanes & (row % 8 >= 4), right, 0.0)
        asked_rows[group * 16 : group * 16 + 16, :] = jnp.concatenate(
            [left, right], axis=1
        ).astype(BF16)

    columns = lax.broadcasted_iota(jnp.int32, (SEQS, 2048), 1)
    subs = lax.broadcasted_iota(jnp.int32, (SEQS, 2048), 0)
    own_head = (columns % 2) == ((subs // 2) % 2)
    lengths_of = tables[32:33, :].astype(jnp.int32)
    sums = [jnp.zeros((SEQS, LANES), F32)]

    def score(group):
        for copy in copies[4 * group : 4 * group + 4]:
            copy.wait()
        for pair in (2 * group, 2 * group + 1):
            at = slice(pair * 8, pair * 8 + 8)
            both_keys = jnp.concatenate([keys[2 * pair], keys[2 * pair + 1]], axis=1)
            score_rows[at, :] = lax.dot_general(
                asked_rows[at, :],
                both_keys,
                (((1,), (1,)), ((), ())),
                preferred_element_type=F32,
            )

    def weigh(group):
        at = slice(group * 16, group * 16 + 16)
        place = lane == group * 16 + row
        limit = jnp.sum(jnp.where(place, lengths_of, 0), axis=1, keepdims=True)
        visible = own_head & (columns < 2 * (limit - me * 1024))
        masked = jnp.where(visible, score_rows[at, :] * DH ** (-0.5), floor_value)
        highest = jnp.max(masked, axis=1, keepdims=True)
        weights = jnp.where(visible, jnp.exp(masked - highest), 0.0).astype(BF16)
        weight_rows[at, :] = weights
        total = jnp.sum(weights.astype(F32), axis=1, keepdims=True)
        beside = lane == 64 + group * 16 + row
        sums[0] = sums[0] + jnp.where(place, highest, jnp.where(beside, total, 0.0))

    def value(pair):
        return sides_of(weighed(pair, slice(0, 2048)))

    def weighed(pair, part):
        both_values = jnp.concatenate(
            [values[2 * pair, part, :], values[2 * pair + 1, part, :]], axis=1
        )
        return jnp.dot(
            weight_rows[pair * 8 : pair * 8 + 8, part],
            both_values,
            preferred_element_type=F32,
        )

    def sides_of(valued):
        return jnp.where(row[:8] < 4, valued[:, :LANES], valued[:, LANES:])

    def arrive(seqs):
        for seq in seqs:
            copies[SEQS + seq].wait()

    def give(group, parts):
        sixteen = jnp.concatenate(parts, axis=0).astype(BF16)
        for dest in range(SEQS):
            out[dest, group * 16 : group * 16 + 16, :] = sixteen

    score(0)
    for group in range(1, 4):
        score(group)
        weigh(group - 1)
    arrive(range(4))
    give(0, [value(0), value(1)])
    weigh(3)
    scale = scale_rows[pl.ds(me, 1), :]
    row_cosine = tables[pl.ds(me, 1), :]
    row_sine = tables[pl.ds(SEQS + me, 1), :]
    lane1 = lax.broadcasted_iota(jnp.int32, (1, LANES), 1)
    fresh_scores = jnp.zeros((1, LANES), F32)
    for head in range(HEADS):
        query = query_rows[pl.ds(head * SEQS + me, 1), :]
        fresh_key = turned(summed[33 + head : 34 + head, :] * scale, row_cosine, row_sine)
        product = query * fresh_key.astype(F32)
        for side in range(2):
            fresh = jnp.sum(
                jnp.where(lane1 // DH == side, product, 0.0), axis=1, keepdims=True
            ) * DH ** (-0.5)
            at = me * 4 + head * 2 + side
            fresh_scores = fresh_scores + jnp.where(lane1 == at, fresh, 0.0)
    fresh_value = (summed[35:37, :] * scale).astype(BF16).astype(F32)
    tail = jnp.concatenate(
        [
            *thirds(jnp.sum(sums[0], axis=0, keepdims=True)),
            *thirds(fresh_scores),
            fresh_value,
        ],
        axis=0,
    ).astype(BF16)
    for dest in range(SEQS):
        out[dest, 64:72, :] = tail
    for group in range(1, 3):
        arrive(range(4 * group, 4 * group + 4))
        give(group, [value(2 * group), value(2 * group + 1)])
    arrive(range(12, 16))
    give(3, [value(6), value(7)])


def thirds(x):
    high = x.astype(BF16).astype(F32)
    middle = (x - high).astype(BF16).astype(F32)
    return high, middle, x - high - middle


def finish_kernel(got, tables, head_gain, out_weight, out, factors, joined):
    rows16, _ = iotas(SEQS)
    tails = got[:, 64:72, :].astype(F32)

    def whole(at):
        return tails[:, at, :] + tails[:, at + 1, :] + tails[:, at + 2, :]

    left = lax.broadcasted_iota(jnp.int32, (1, LANES), 1) < 64
    both = whole(0)
    maxima = jnp.where(left, both, 0.0)
    totals = jnp.where(left, pltpu.roll(both, 64, 1), 1.0)
    fresh = jnp.sum(whole(3), axis=0, keepdims=True)
    block = tables[32:33, :].astype(jnp.int32) // 1024
    in_block = jnp.max(
        jnp.where(rows16 == block, maxima, floor_value), axis=0, keepdims=True
    )
    in_block = jnp.maximum(in_block, fresh)
    top = jnp.maximum(jnp.max(maxima, axis=0, keepdims=True), fresh)
    factor = jnp.exp(maxima - top)
    fresh_factor = jnp.exp(fresh - in_block).astype(BF16).astype(F32) * jnp.exp(in_block - top)
    total = jnp.sum(totals * factor, axis=0, keepdims=True) + fresh_factor
    part = tables[33:34, :] / total
    factors[...] = jnp.zeros((LANES, LANES), F32)
    factors[0:SEQS, :] = factor * part
    factors[SEQS : SEQS + 1, :] = fresh_factor * part
    columns = factors[...].T
    sub, _ = iotas(16)
    for four in range(SEQS // 4):
        here = columns[four * 16 : four * 16 + 16, :]
        fresh_value = jnp.zeros((16, LANES), F32)
        for n in range(8):
            line = tails[four * 4 + n // 2, 6 + n % 2 : 7 + n % 2, :]
            fresh_value = jnp.where(sub // 2 == n, line, fresh_value)
        joint = here[:, SEQS : SEQS + 1] * fresh_value
        for peer in range(SEQS):
            joint = joint + here[:, peer : peer + 1] * got[
                peer, four * 16 : four * 16 + 16, :
            ].astype(F32)
        joined[four * 16 : four * 16 + 16, :] = joint
    sides = []
    for head in range(HEADS):
        mixed = joined[pl.ds(2 * head, SEQS, 4), :] + joined[pl.ds(2 * head + 1, SEQS, 4), :]
        mean = jnp.mean(mixed * mixed, axis=1, keepdims=True)
        sides.append((mixed * lax.rsqrt(mean + epsilon) * head_gain[...]).astype(BF16))
    head_out = jnp.concatenate(sides, axis=1)
    partial_out = jnp.dot(
        head_out, out_weight[...], preferred_element_type=F32
    ).astype(BF16)
    for dest in range(8):
        out[dest] = partial_out


def attend_call(tables, got, keys, values, name):
    return pl.pallas_call(
        attend_kernel,
        in_specs=[VM, VM, ANY, ANY],
        out_specs=VM,
        out_shape=jax.ShapeDtypeStruct((SEQS, 72, LANES), BF16),
        scratch_shapes=[
            pltpu.VMEM(keys.shape, BF16),
            pltpu.VMEM(values.shape, BF16),
            pltpu.SemaphoreType.DMA((2, SEQS)),
            pltpu.VMEM((32, LANES), F32),
            pltpu.VMEM((SEQS, LANES), F32),
            pltpu.VMEM((64, 256), BF16),
            pltpu.VMEM((64, 2048), F32),
            pltpu.VMEM((64, 2048), BF16),
        ],
        compiler_params=BIG,
        name=name,
    )(tables, got, in_hbm(keys), in_hbm(values))


def local(
    tokens,
    norm_gain,
    query_weight,
    key_weight,
    value_weight,
    out_weight,
    lambdas,
    head_gain,
    lengths,
    key_cache,
    value_cache,
):
    rates = np.tile(theta_base ** (-np.arange(DH // 2) / (DH // 2)), 4)
    sent, tables = pl.pallas_call(
        project_kernel,
        in_specs=[ANY] * 8,
        out_specs=[VM, VM],
        out_shape=[
            jax.ShapeDtypeStruct((SEQS, 40, LANES), F32),
            jax.ShapeDtypeStruct((40, LANES), F32),
        ],
        scratch_shapes=[
            pltpu.VMEM((SEQS, 256), BF16),
            pltpu.VMEM((1, 256), F32),
            pltpu.VMEM((1, SEQS), jnp.int32),
            pltpu.VMEM((1, HEADS), F32),
            pltpu.VMEM((1, LANES), F32),
            pltpu.VMEM((256, 768), BF16),
            pltpu.SemaphoreType.DMA((5,)),
            pltpu.SemaphoreType.DMA((3,)),
        ],
        compiler_params=SMALL,
        name="project",
    )(
        in_hbm(tokens),
        in_hbm(norm_gain.reshape(1, -1)),
        in_hbm(lengths.reshape(1, -1)),
        in_hbm(lambdas.reshape(1, -1)),
        in_hbm(jnp.asarray(rates, F32).reshape(1, -1)),
        in_hbm(query_weight),
        in_hbm(key_weight),
        in_hbm(value_weight),
    )
    got = lax.all_to_all(sent, "kv", split_axis=0, concat_axis=0, tiled=True)
    cache_shape = (SEQS, 2048, LANES)
    shared = attend_call(
        tables, got, key_cache.reshape(cache_shape), value_cache.reshape(cache_shape), "attend"
    )
    everyone = lax.all_to_all(shared, "kv", split_axis=0, concat_axis=0, tiled=True)
    partial_out = pl.pallas_call(
        finish_kernel,
        in_specs=[VM] * 4,
        out_specs=VM,
        out_shape=jax.ShapeDtypeStruct((8, SEQS, 256), BF16),
        scratch_shapes=[pltpu.VMEM((LANES, LANES), F32), pltpu.VMEM((64, LANES), F32)],
        compiler_params=SMALL,
        name="finish",
    )(everyone, tables, head_gain.reshape(1, -1), out_weight)
    shares = lax.all_to_all(partial_out, "tp", split_axis=0, concat_axis=0, tiled=True)
    return shares.astype(F32).sum(axis=0).astype(BF16)


def solution(mesh):
    return jax.shard_map(
        local,
        mesh=mesh,
        in_specs=(
            P(None, "kv"),
            P("kv"),
            P("kv", "tp"),
            P("kv", "tp"),
            P("kv", "tp"),
            P("tp", "kv"),
            P("tp"),
            P(),
            P(),
            P(None, "kv", "tp", None),
            P(None, "kv", "tp", None),
        ),
        out_specs=P(None, "kv"),
        check_vma=False,
    )
```

```python
import functools

import jax
import jax.numpy as jnp
import numpy as np
from jax import lax
from jax.experimental import pallas as pl
from jax.experimental.pallas import tpu as pltpu
from jax.sharding import PartitionSpec as P

D = 4096
DH = 64
HEADS = 2
SEQS = 16
LANES = 128

epsilon = 1e-05
theta_base = 500000.0
floor_value = -1e30

VM = pl.BlockSpec(memory_space=pltpu.VMEM)
SM = pl.BlockSpec(memory_space=pltpu.SMEM)
ANY = pl.BlockSpec(memory_space=pltpu.HBM)
F32 = jnp.float32
BF16 = jnp.bfloat16
SMALL = pltpu.CompilerParams(vmem_limit_bytes=8 * 1024 * 1024)
BIG = pltpu.CompilerParams(vmem_limit_bytes=30 * 1024 * 1024)


def in_hbm(x):
    return pltpu.with_memory_space_constraint(x, pltpu.HBM)


def iotas(rows):
    shape = (rows, LANES)
    return lax.broadcasted_iota(jnp.int32, shape, 0), lax.broadcasted_iota(jnp.int32, shape, 1)


def project_kernel(
    tokens_in, gain_in, lengths_in, lambdas_in, rates_in, query_in, key_in, value_in, out,
    out_one, out_two, out_three, tables,
    tokens, gain, lengths, lambdas, rates, weights, fresh, small, large,
):
    near = [
        pltpu.make_async_copy(source, target, small.at[n])
        for n, (source, target) in enumerate(
            (
                (tokens_in, tokens),
                (gain_in, gain),
                (lengths_in, lengths),
                (lambdas_in, lambdas),
                (rates_in, rates),
            )
        )
    ]
    far = [
        pltpu.make_async_copy(source, weights.at[:, 256 * n : 256 * n + 256], large.at[n])
        for n, source in enumerate((query_in, key_in, value_in))
    ]
    for copy in (*near, *far):
        copy.start()
    for copy in near:
        copy.wait()
    widened = tokens[...].astype(F32)
    squares = jnp.sum(widened * widened, axis=1, keepdims=True)
    normed = (widened * gain[...]).astype(BF16)
    row, lane = iotas(SEQS)
    square_row = jnp.sum(jnp.where(row == lane, squares, 0.0), axis=0, keepdims=True)
    row16 = lax.broadcasted_iota(jnp.int32, (SEQS, SEQS), 0)
    lane16 = lax.broadcasted_iota(jnp.int32, (SEQS, SEQS), 1)
    held = lengths[...].astype(F32)
    held_column = jnp.sum(jnp.where(row16 == lane16, held, 0.0), axis=1, keepdims=True)
    angles = held_column * rates[...]
    tables[0:16, :] = jnp.cos(angles)
    sine = jnp.sin(angles)
    tables[16:32, :] = jnp.where((lane // 32) % 2 == 0, -sine, sine)
    lane1 = lax.broadcasted_iota(jnp.int32, (1, LANES), 1)
    lambda_row = jnp.where((lane1 // 2) % 2 == 0, lambdas[:, 0:1], lambdas[:, 1:2])
    tables[32:40, :] = jnp.concatenate(
        [
            jnp.sum(jnp.where(row == lane // 4, held_column, 0.0), axis=0, keepdims=True),
            jnp.where(lane1 % 2 == 0, 1.0, -lambda_row),
            jnp.zeros((6, LANES), F32),
        ],
        axis=0,
    )
    for copy in far:
        copy.wait()
    products = jnp.dot(normed, weights[...], preferred_element_type=F32)
    query, key, value = products[:, :256], products[:, 256:512], products[:, 512:]
    fresh[0:16, :] = key[:, :LANES]
    fresh[16:32, :] = key[:, LANES:]
    fresh[32:48, :] = value[:, :LANES]
    fresh[48:64, :] = value[:, LANES:]
    column = lax.axis_index("kv") % 4
    head = jnp.concatenate([square_row, jnp.zeros((7, LANES), F32)], axis=0)
    for turn, target in enumerate((out, out_one, out_two, out_three)):
        target[0:16, :] = query[:, :LANES]
        target[16:32, :] = query[:, LANES:]
        target[32:40, :] = head
        other = column ^ turn
        target[40:56, :] = jnp.concatenate(
            [fresh[pl.ds(16 * part + other, 4, 4), :] for part in range(4)], axis=0
        )


def halfway_kernel(mine, one, two, three, out, out_one, out_two, out_three, total):
    total[...] = (mine[...] + one[...]) + (two[...] + three[...])
    plane = lax.axis_index("kv") // 4
    blank = jnp.zeros((3, LANES), F32)
    for turn, target in enumerate((out, out_one, out_two, out_three)):
        target[0:32, :] = total[0:32, :]
        target[32:40, :] = jnp.concatenate(
            [total[32:33, :], total[pl.ds(40 + (plane ^ turn), 4, 4), :], blank], axis=0
        )


def swapped(arrays, step):
    mine, *others = arrays
    return [
        mine,
        *(
            lax.ppermute(x, "kv", [(i, i ^ (step * (n + 1))) for i in range(16)])
            for n, x in enumerate(others)
        ),
    ]


def turned(x, cosine, sine):
    lane = lax.broadcasted_iota(jnp.int32, x.shape, 1)
    partner = jnp.where(
        (lane // 32) % 2 == 0, pltpu.roll(x, LANES - 32, 1), pltpu.roll(x, 32, 1)
    )
    return (x * cosine + partner * sine).astype(BF16)


def attend_kernel(
    tables, mine, one, two, three, first_keys, second_keys, values_in, out, values, arrived, query_rows, scale_rows,
    asked_rows, score_rows, weight_rows,
):
    copies = [
        pltpu.make_async_copy(values_in.at[seq], values.at[seq], arrived.at[seq])
        for seq in range(SEQS)
    ]
    for copy in copies:
        copy.start()

    def keys_of(seq):
        return first_keys[seq] if seq < 8 else second_keys[seq - 8]

    me = lax.axis_index("kv")
    cosine, sine = tables[0:16, :], tables[16:32, :]
    summed = (mine[...] + one[...]) + (two[...] + three[...])
    row, lane = iotas(SEQS)
    squares = jnp.sum(jnp.where(row == lane, summed[32:33, :], 0.0), axis=1, keepdims=True)
    scaling = jnp.broadcast_to(lax.rsqrt(squares / D + epsilon), (SEQS, LANES))
    scale_rows[...] = scaling
    for head in range(HEADS):
        turned_query = turned(
            summed[16 * head : 16 * head + 16, :] * scaling, cosine, sine
        )
        query_rows[head * SEQS : (head + 1) * SEQS, :] = turned_query.astype(F32)
    map_lanes = (lane // DH) == (row % 2)

    def row_of(head, seq):
        at = head * SEQS + seq
        return jnp.broadcast_to(query_rows[at : at + 1, :], (SEQS, LANES))

    for group in range(4):
        first = 4 * group
        left = jnp.where(
            row < 8,
            jnp.where(row < 2, row_of(0, first), row_of(1, first)),
            jnp.where(row < 10, row_of(0, first + 2), row_of(1, first + 2)),
        )
        right = jnp.where(
            row < 8,
            jnp.where(row < 6, row_of(0, first + 1), row_of(1, first + 1)),
            jnp.where(row < 14, row_of(0, first + 3), row_of(1, first + 3)),
        )
        left = jnp.where(map_lanes & (row % 8 < 4), left, 0.0)
        right = jnp.where(map_lanes & (row % 8 >= 4), right, 0.0)
        asked_rows[group * 16 : group * 16 + 16, :] = jnp.concatenate(
            [left, right], axis=1
        ).astype(BF16)

    columns = lax.broadcasted_iota(jnp.int32, (SEQS, 2048), 1)
    subs = lax.broadcasted_iota(jnp.int32, (SEQS, 2048), 0)
    own_head = (columns % 2) == ((subs // 2) % 2)
    lengths_of = tables[32:33, :].astype(jnp.int32)
    sums = [jnp.zeros((SEQS, LANES), F32)]

    def score(group):
        for pair in (2 * group, 2 * group + 1):
            at = slice(pair * 8, pair * 8 + 8)
            both_keys = jnp.concatenate([keys_of(2 * pair), keys_of(2 * pair + 1)], axis=1)
            score_rows[at, :] = lax.dot_general(
                asked_rows[at, :],
                both_keys,
                (((1,), (1,)), ((), ())),
                preferred_element_type=F32,
            )

    def weigh(group):
        at = slice(group * 16, group * 16 + 16)
        place = lane == group * 16 + row
        limit = jnp.sum(jnp.where(place, lengths_of, 0), axis=1, keepdims=True)
        visible = own_head & (columns < 2 * (limit - me * 1024))
        masked = jnp.where(visible, score_rows[at, :] * DH ** (-0.5), floor_value)
        highest = jnp.max(masked, axis=1, keepdims=True)
        weights = jnp.where(visible, jnp.exp(masked - highest), 0.0).astype(BF16)
        weight_rows[at, :] = weights
        total = jnp.sum(weights.astype(F32), axis=1, keepdims=True)
        beside = lane == 64 + group * 16 + row
        sums[0] = sums[0] + jnp.where(place, highest, jnp.where(beside, total, 0.0))

    def value(pair):
        return sides_of(weighed(pair, slice(0, 2048)))

    def weighed(pair, part):
        both_values = jnp.concatenate(
            [values[2 * pair, part, :], values[2 * pair + 1, part, :]], axis=1
        )
        return jnp.dot(
            weight_rows[pair * 8 : pair * 8 + 8, part],
            both_values,
            preferred_element_type=F32,
        )

    def sides_of(valued):
        return jnp.where(row[:8] < 4, valued[:, :LANES], valued[:, LANES:])

    def arrive(seqs):
        for seq in seqs:
            copies[seq].wait()

    def give(group, parts):
        sixteen = jnp.concatenate(parts, axis=0).astype(BF16)
        for dest in range(SEQS):
            out[dest, group * 16 : group * 16 + 16, :] = sixteen

    score(0)
    for group in range(1, 4):
        score(group)
        weigh(group - 1)
    arrive(range(4))
    give(0, [value(0), value(1)])
    weigh(3)
    scale = scale_rows[pl.ds(me, 1), :]
    row_cosine = tables[pl.ds(me, 1), :]
    row_sine = tables[pl.ds(SEQS + me, 1), :]
    lane1 = lax.broadcasted_iota(jnp.int32, (1, LANES), 1)
    fresh_scores = jnp.zeros((1, LANES), F32)
    for head in range(HEADS):
        query = query_rows[pl.ds(head * SEQS + me, 1), :]
        fresh_key = turned(summed[33 + head : 34 + head, :] * scale, row_cosine, row_sine)
        product = query * fresh_key.astype(F32)
        for side in range(2):
            fresh = jnp.sum(
                jnp.where(lane1 // DH == side, product, 0.0), axis=1, keepdims=True
            ) * DH ** (-0.5)
            at = me * 4 + head * 2 + side
            fresh_scores = fresh_scores + jnp.where(lane1 == at, fresh, 0.0)
    fresh_value = (summed[35:37, :] * scale).astype(BF16).astype(F32)
    tail = jnp.concatenate(
        [
            *thirds(jnp.sum(sums[0], axis=0, keepdims=True)),
            *thirds(fresh_scores),
            fresh_value,
        ],
        axis=0,
    ).astype(BF16)
    for dest in range(SEQS):
        out[dest, 64:72, :] = tail
    for group in range(1, 3):
        arrive(range(4 * group, 4 * group + 4))
        give(group, [value(2 * group), value(2 * group + 1)])
    arrive(range(12, 16))
    give(3, [value(6), value(7)])


def thirds(x):
    high = x.astype(BF16).astype(F32)
    middle = (x - high).astype(BF16).astype(F32)
    return high, middle, x - high - middle


def finish_kernel(got, tables, head_gain, out_weight, out, factors, joined):
    rows16, _ = iotas(SEQS)
    tails = got[:, 64:72, :].astype(F32)

    def whole(at):
        return tails[:, at, :] + tails[:, at + 1, :] + tails[:, at + 2, :]

    left = lax.broadcasted_iota(jnp.int32, (1, LANES), 1) < 64
    both = whole(0)
    maxima = jnp.where(left, both, 0.0)
    totals = jnp.where(left, pltpu.roll(both, 64, 1), 1.0)
    fresh = jnp.sum(whole(3), axis=0, keepdims=True)
    block = tables[32:33, :].astype(jnp.int32) // 1024
    in_block = jnp.max(
        jnp.where(rows16 == block, maxima, floor_value), axis=0, keepdims=True
    )
    in_block = jnp.maximum(in_block, fresh)
    top = jnp.maximum(jnp.max(maxima, axis=0, keepdims=True), fresh)
    factor = jnp.exp(maxima - top)
    fresh_factor = jnp.exp(fresh - in_block).astype(BF16).astype(F32) * jnp.exp(in_block - top)
    total = jnp.sum(totals * factor, axis=0, keepdims=True) + fresh_factor
    part = tables[33:34, :] / total
    factors[...] = jnp.zeros((LANES, LANES), F32)
    factors[0:SEQS, :] = factor * part
    factors[SEQS : SEQS + 1, :] = fresh_factor * part
    columns = factors[...].T
    sub, _ = iotas(16)
    for four in range(SEQS // 4):
        here = columns[four * 16 : four * 16 + 16, :]
        fresh_value = jnp.zeros((16, LANES), F32)
        for n in range(8):
            line = tails[four * 4 + n // 2, 6 + n % 2 : 7 + n % 2, :]
            fresh_value = jnp.where(sub // 2 == n, line, fresh_value)
        joint = here[:, SEQS : SEQS + 1] * fresh_value
        for peer in range(SEQS):
            joint = joint + here[:, peer : peer + 1] * got[
                peer, four * 16 : four * 16 + 16, :
            ].astype(F32)
        joined[four * 16 : four * 16 + 16, :] = joint
    sides = []
    for head in range(HEADS):
        mixed = joined[pl.ds(2 * head, SEQS, 4), :] + joined[pl.ds(2 * head + 1, SEQS, 4), :]
        mean = jnp.mean(mixed * mixed, axis=1, keepdims=True)
        sides.append((mixed * lax.rsqrt(mean + epsilon) * head_gain[...]).astype(BF16))
    head_out = jnp.concatenate(sides, axis=1)
    partial_out = jnp.dot(
        head_out, out_weight[...], preferred_element_type=F32
    ).astype(BF16)
    for dest in range(8):
        out[dest] = partial_out


def load_kernel(first, source, target, arrived):
    copies = [
        pltpu.make_async_copy(
            source.at[pl.ds(first + 2 * n, 2)], target.at[pl.ds(2 * n, 2)], arrived.at[n]
        )
        for n in range(4)
    ]
    for copy in copies:
        copy.start()
    for copy in copies:
        copy.wait()


def load_call(source, first, name):
    return pl.pallas_call(
        functools.partial(load_kernel, first),
        in_specs=[ANY],
        out_specs=VM,
        out_shape=pltpu.VMEM((8, *source.shape[1:]), BF16),
        scratch_shapes=[pltpu.SemaphoreType.DMA((4,))],
        compiler_params=SMALL,
        cost_estimate=pl.CostEstimate(flops=2**31, bytes_accessed=2**24, transcendentals=0),
        name=name,
    )(in_hbm(source))


def attend_call(tables, got, first_keys, second_keys, values, name):
    return pl.pallas_call(
        attend_kernel,
        in_specs=[*[VM] * 7, ANY],
        out_specs=VM,
        out_shape=jax.ShapeDtypeStruct((SEQS, 72, LANES), BF16),
        scratch_shapes=[
            pltpu.VMEM(values.shape, BF16),
            pltpu.SemaphoreType.DMA((SEQS,)),
            pltpu.VMEM((32, LANES), F32),
            pltpu.VMEM((SEQS, LANES), F32),
            pltpu.VMEM((64, 256), BF16),
            pltpu.VMEM((64, 2048), F32),
            pltpu.VMEM((64, 2048), BF16),
        ],
        compiler_params=BIG,
        name=name,
    )(tables, *got, first_keys, second_keys, in_hbm(values))


def local(
    tokens,
    norm_gain,
    query_weight,
    key_weight,
    value_weight,
    out_weight,
    lambdas,
    head_gain,
    lengths,
    key_cache,
    value_cache,
):
    rates = np.tile(theta_base ** (-np.arange(DH // 2) / (DH // 2)), 4)
    *sent, tables = pl.pallas_call(
        project_kernel,
        in_specs=[ANY] * 8,
        out_specs=[VM] * 5,
        out_shape=[
            *[jax.ShapeDtypeStruct((56, LANES), F32)] * 4,
            jax.ShapeDtypeStruct((40, LANES), F32),
        ],
        scratch_shapes=[
            pltpu.VMEM((SEQS, 256), BF16),
            pltpu.VMEM((1, 256), F32),
            pltpu.VMEM((1, SEQS), jnp.int32),
            pltpu.VMEM((1, HEADS), F32),
            pltpu.VMEM((1, LANES), F32),
            pltpu.VMEM((256, 768), BF16),
            pltpu.VMEM((64, LANES), F32),
            pltpu.SemaphoreType.DMA((5,)),
            pltpu.SemaphoreType.DMA((3,)),
        ],
        compiler_params=SMALL,
        name="project",
    )(
        in_hbm(tokens),
        in_hbm(norm_gain.reshape(1, -1)),
        in_hbm(lengths.reshape(1, -1)),
        in_hbm(lambdas.reshape(1, -1)),
        in_hbm(jnp.asarray(rates, F32).reshape(1, -1)),
        in_hbm(query_weight),
        in_hbm(key_weight),
        in_hbm(value_weight),
    )
    halves = pl.pallas_call(
        halfway_kernel,
        in_specs=[VM] * 4,
        out_specs=[VM] * 4,
        out_shape=[jax.ShapeDtypeStruct((40, LANES), F32)] * 4,
        scratch_shapes=[pltpu.VMEM((56, LANES), F32)],
        compiler_params=SMALL,
        name="halfway",
    )(*swapped(sent, 1))
    got = swapped(halves, 4)
    cache_shape = (SEQS, 2048, LANES)
    keys = key_cache.reshape(cache_shape)
    shared = attend_call(
        tables,
        got,
        load_call(keys, 0, "first"),
        load_call(keys, 8, "second"),
        value_cache.reshape(cache_shape),
        "attend",
    )
    everyone = lax.all_to_all(shared, "kv", split_axis=0, concat_axis=0, tiled=True)
    partial_out = pl.pallas_call(
        finish_kernel,
        in_specs=[VM] * 4,
        out_specs=VM,
        out_shape=jax.ShapeDtypeStruct((8, SEQS, 256), BF16),
        scratch_shapes=[pltpu.VMEM((LANES, LANES), F32), pltpu.VMEM((64, LANES), F32)],
        compiler_params=SMALL,
        name="finish",
    )(everyone, tables, head_gain.reshape(1, -1), out_weight)
    shares = lax.all_to_all(partial_out, "tp", split_axis=0, concat_axis=0, tiled=True)
    return shares.astype(F32).sum(axis=0).astype(BF16)


def solution(mesh):
    return jax.shard_map(
        local,
        mesh=mesh,
        in_specs=(
            P(None, "kv"),
            P("kv"),
            P("kv", "tp"),
            P("kv", "tp"),
            P("kv", "tp"),
            P("tp", "kv"),
            P("tp"),
            P(),
            P(),
            P(None, "kv", "tp", None),
            P(None, "kv", "tp", None),
        ),
        out_specs=P(None, "kv"),
        check_vma=False,
    )
```

```python
import jax
import jax.numpy as jnp
import numpy as np
from jax import lax
from jax.experimental import pallas as pl
from jax.experimental.pallas import tpu as pltpu
from jax.sharding import PartitionSpec as P

D = 4096
DH = 64
HEADS = 2
SEQS = 16
LANES = 128

epsilon = 1e-05
theta_base = 500000.0
floor_value = -1e30
EARLY = 1

VM = pl.BlockSpec(memory_space=pltpu.VMEM)
SM = pl.BlockSpec(memory_space=pltpu.SMEM)
ANY = pl.BlockSpec(memory_space=pltpu.HBM)
F32 = jnp.float32
BF16 = jnp.bfloat16
SMALL = pltpu.CompilerParams(vmem_limit_bytes=8 * 1024 * 1024)
BIG = pltpu.CompilerParams(vmem_limit_bytes=30 * 1024 * 1024)


def in_hbm(x):
    return pltpu.with_memory_space_constraint(x, pltpu.HBM)


def iotas(rows):
    shape = (rows, LANES)
    return lax.broadcasted_iota(jnp.int32, shape, 0), lax.broadcasted_iota(jnp.int32, shape, 1)


def project_kernel(
    tokens_in, gain_in, lengths_in, lambdas_in, rates_in, query_in, key_in, value_in, keys_in, out,
    tables, early_keys, tokens, gain, lengths, lambdas, rates, weights, small, large, early,
):
    near = [
        pltpu.make_async_copy(source, target, small.at[n])
        for n, (source, target) in enumerate(
            (
                (tokens_in, tokens),
                (gain_in, gain),
                (lengths_in, lengths),
                (lambdas_in, lambdas),
                (rates_in, rates),
            )
        )
    ]
    far = [
        pltpu.make_async_copy(source, weights.at[:, 256 * n : 256 * n + 256], large.at[n])
        for n, source in enumerate((query_in, key_in, value_in))
    ]
    ahead = [
        pltpu.make_async_copy(keys_in.at[n], early_keys.at[n], early.at[n]) for n in range(EARLY)
    ]
    for copy in (*near, *far, *ahead):
        copy.start()
    for copy in near:
        copy.wait()
    widened = tokens[...].astype(F32)
    squares = jnp.sum(widened * widened, axis=1, keepdims=True)
    normed = (widened * gain[...]).astype(BF16)
    row, lane = iotas(SEQS)
    square_row = jnp.sum(jnp.where(row == lane, squares, 0.0), axis=0, keepdims=True)
    row16 = lax.broadcasted_iota(jnp.int32, (SEQS, SEQS), 0)
    lane16 = lax.broadcasted_iota(jnp.int32, (SEQS, SEQS), 1)
    held = lengths[...].astype(F32)
    held_column = jnp.sum(jnp.where(row16 == lane16, held, 0.0), axis=1, keepdims=True)
    angles = held_column * rates[...]
    tables[0:16, :] = jnp.cos(angles)
    sine = jnp.sin(angles)
    tables[16:32, :] = jnp.where((lane // 32) % 2 == 0, -sine, sine)
    lane1 = lax.broadcasted_iota(jnp.int32, (1, LANES), 1)
    lambda_row = jnp.where((lane1 // 2) % 2 == 0, lambdas[:, 0:1], lambdas[:, 1:2])
    tables[32:40, :] = jnp.concatenate(
        [
            jnp.sum(jnp.where(row == lane // 4, held_column, 0.0), axis=0, keepdims=True),
            jnp.where(lane1 % 2 == 0, 1.0, -lambda_row),
            jnp.zeros((6, LANES), F32),
        ],
        axis=0,
    )
    for copy in far:
        copy.wait()
    products = jnp.dot(normed, weights[...], preferred_element_type=F32)
    query, key, value = products[:, :256], products[:, 256:512], products[:, 512:]
    blank = jnp.zeros((3, LANES), F32)
    for dest in range(SEQS):
        out[dest, 0:16, :] = query[:, :LANES]
        out[dest, 16:32, :] = query[:, LANES:]
        out[dest, 32:40, :] = jnp.concatenate(
            [
                square_row,
                key[dest : dest + 1, :LANES],
                key[dest : dest + 1, LANES:],
                value[dest : dest + 1, :LANES],
                value[dest : dest + 1, LANES:],
                blank,
            ],
            axis=0,
        )
    for copy in ahead:
        copy.wait()


def turned(x, cosine, sine):
    lane = lax.broadcasted_iota(jnp.int32, x.shape, 1)
    partner = jnp.where(
        (lane // 32) % 2 == 0, pltpu.roll(x, LANES - 32, 1), pltpu.roll(x, 32, 1)
    )
    return (x * cosine + partner * sine).astype(BF16)


def attend_kernel(
    tables, got, early_keys, keys_in, values_in, out, keys, values, arrived, query_rows, scale_rows,
    asked_rows, score_rows, weight_rows,
):
    key_copies = {
        seq: pltpu.make_async_copy(keys_in.at[seq], keys.at[seq - EARLY], arrived.at[0, seq])
        for seq in range(EARLY, SEQS)
    }
    value_copies = [
        pltpu.make_async_copy(values_in.at[seq], values.at[seq], arrived.at[1, seq])
        for seq in range(SEQS)
    ]
    for copy in (*key_copies.values(), *value_copies):
        copy.start()

    def keys_of(seq):
        return early_keys[seq] if seq < EARLY else keys[seq - EARLY]

    me = lax.axis_index("kv")
    cosine, sine = tables[0:16, :], tables[16:32, :]
    summed = jnp.sum(got[...], axis=0)
    row, lane = iotas(SEQS)
    squares = jnp.sum(jnp.where(row == lane, summed[32:33, :], 0.0), axis=1, keepdims=True)
    scaling = jnp.broadcast_to(lax.rsqrt(squares / D + epsilon), (SEQS, LANES))
    scale_rows[...] = scaling
    for head in range(HEADS):
        turned_query = turned(
            summed[16 * head : 16 * head + 16, :] * scaling, cosine, sine
        )
        query_rows[head * SEQS : (head + 1) * SEQS, :] = turned_query.astype(F32)
    map_lanes = (lane // DH) == (row % 2)

    def row_of(head, seq):
        at = head * SEQS + seq
        return jnp.broadcast_to(query_rows[at : at + 1, :], (SEQS, LANES))

    for group in range(4):
        first = 4 * group
        left = jnp.where(
            row < 8,
            jnp.where(row < 2, row_of(0, first), row_of(1, first)),
            jnp.where(row < 10, row_of(0, first + 2), row_of(1, first + 2)),
        )
        right = jnp.where(
            row < 8,
            jnp.where(row < 6, row_of(0, first + 1), row_of(1, first + 1)),
            jnp.where(row < 14, row_of(0, first + 3), row_of(1, first + 3)),
        )
        left = jnp.where(map_lanes & (row % 8 < 4), left, 0.0)
        right = jnp.where(map_lanes & (row % 8 >= 4), right, 0.0)
        asked_rows[group * 16 : group * 16 + 16, :] = jnp.concatenate(
            [left, right], axis=1
        ).astype(BF16)

    columns = lax.broadcasted_iota(jnp.int32, (SEQS, 2048), 1)
    subs = lax.broadcasted_iota(jnp.int32, (SEQS, 2048), 0)
    own_head = (columns % 2) == ((subs // 2) % 2)
    lengths_of = tables[32:33, :].astype(jnp.int32)
    sums = [jnp.zeros((SEQS, LANES), F32)]

    def score(group):
        for seq in range(4 * group, 4 * group + 4):
            if seq >= EARLY:
                key_copies[seq].wait()
        for pair in (2 * group, 2 * group + 1):
            at = slice(pair * 8, pair * 8 + 8)
            both_keys = jnp.concatenate([keys_of(2 * pair), keys_of(2 * pair + 1)], axis=1)
            score_rows[at, :] = lax.dot_general(
                asked_rows[at, :],
                both_keys,
                (((1,), (1,)), ((), ())),
                preferred_element_type=F32,
            )

    def weigh(group):
        at = slice(group * 16, group * 16 + 16)
        place = lane == group * 16 + row
        limit = jnp.sum(jnp.where(place, lengths_of, 0), axis=1, keepdims=True)
        visible = own_head & (columns < 2 * (limit - me * 1024))
        masked = jnp.where(visible, score_rows[at, :] * DH ** (-0.5), floor_value)
        highest = jnp.max(masked, axis=1, keepdims=True)
        weights = jnp.where(visible, jnp.exp(masked - highest), 0.0).astype(BF16)
        weight_rows[at, :] = weights
        total = jnp.sum(weights.astype(F32), axis=1, keepdims=True)
        beside = lane == 64 + group * 16 + row
        sums[0] = sums[0] + jnp.where(place, highest, jnp.where(beside, total, 0.0))

    def value(pair):
        return sides_of(weighed(pair, slice(0, 2048)))

    def weighed(pair, part):
        both_values = jnp.concatenate(
            [values[2 * pair, part, :], values[2 * pair + 1, part, :]], axis=1
        )
        return jnp.dot(
            weight_rows[pair * 8 : pair * 8 + 8, part],
            both_values,
            preferred_element_type=F32,
        )

    def sides_of(valued):
        return jnp.where(row[:8] < 4, valued[:, :LANES], valued[:, LANES:])

    def arrive(seqs):
        for seq in seqs:
            value_copies[seq].wait()

    def give(group, parts):
        sixteen = jnp.concatenate(parts, axis=0).astype(BF16)
        for dest in range(SEQS):
            out[dest, group * 16 : group * 16 + 16, :] = sixteen

    score(0)
    for group in range(1, 4):
        score(group)
        weigh(group - 1)
    arrive(range(4))
    give(0, [value(0), value(1)])
    weigh(3)
    scale = scale_rows[pl.ds(me, 1), :]
    row_cosine = tables[pl.ds(me, 1), :]
    row_sine = tables[pl.ds(SEQS + me, 1), :]
    lane1 = lax.broadcasted_iota(jnp.int32, (1, LANES), 1)
    fresh_scores = jnp.zeros((1, LANES), F32)
    for head in range(HEADS):
        query = query_rows[pl.ds(head * SEQS + me, 1), :]
        fresh_key = turned(summed[33 + head : 34 + head, :] * scale, row_cosine, row_sine)
        product = query * fresh_key.astype(F32)
        for side in range(2):
            fresh = jnp.sum(
                jnp.where(lane1 // DH == side, product, 0.0), axis=1, keepdims=True
            ) * DH ** (-0.5)
            at = me * 4 + head * 2 + side
            fresh_scores = fresh_scores + jnp.where(lane1 == at, fresh, 0.0)
    fresh_value = (summed[35:37, :] * scale).astype(BF16).astype(F32)
    tail = jnp.concatenate(
        [
            *thirds(jnp.sum(sums[0], axis=0, keepdims=True)),
            *thirds(fresh_scores),
            fresh_value,
        ],
        axis=0,
    ).astype(BF16)
    for dest in range(SEQS):
        out[dest, 64:72, :] = tail
    for group in range(1, 3):
        arrive(range(4 * group, 4 * group + 4))
        give(group, [value(2 * group), value(2 * group + 1)])
    arrive(range(12, 16))
    give(3, [value(6), value(7)])


def thirds(x):
    high = x.astype(BF16).astype(F32)
    middle = (x - high).astype(BF16).astype(F32)
    return high, middle, x - high - middle


def finish_kernel(got, tables, head_gain, out_weight, out, factors, joined):
    rows16, _ = iotas(SEQS)
    tails = got[:, 64:72, :].astype(F32)

    def whole(at):
        return tails[:, at, :] + tails[:, at + 1, :] + tails[:, at + 2, :]

    left = lax.broadcasted_iota(jnp.int32, (1, LANES), 1) < 64
    both = whole(0)
    maxima = jnp.where(left, both, 0.0)
    totals = jnp.where(left, pltpu.roll(both, 64, 1), 1.0)
    fresh = jnp.sum(whole(3), axis=0, keepdims=True)
    block = tables[32:33, :].astype(jnp.int32) // 1024
    in_block = jnp.max(
        jnp.where(rows16 == block, maxima, floor_value), axis=0, keepdims=True
    )
    in_block = jnp.maximum(in_block, fresh)
    top = jnp.maximum(jnp.max(maxima, axis=0, keepdims=True), fresh)
    factor = jnp.exp(maxima - top)
    fresh_factor = jnp.exp(fresh - in_block).astype(BF16).astype(F32) * jnp.exp(in_block - top)
    total = jnp.sum(totals * factor, axis=0, keepdims=True) + fresh_factor
    part = tables[33:34, :] / total
    factors[...] = jnp.zeros((LANES, LANES), F32)
    factors[0:SEQS, :] = factor * part
    factors[SEQS : SEQS + 1, :] = fresh_factor * part
    columns = factors[...].T
    sub, _ = iotas(16)
    for four in range(SEQS // 4):
        here = columns[four * 16 : four * 16 + 16, :]
        fresh_value = jnp.zeros((16, LANES), F32)
        for n in range(8):
            line = tails[four * 4 + n // 2, 6 + n % 2 : 7 + n % 2, :]
            fresh_value = jnp.where(sub // 2 == n, line, fresh_value)
        joint = here[:, SEQS : SEQS + 1] * fresh_value
        for peer in range(SEQS):
            joint = joint + here[:, peer : peer + 1] * got[
                peer, four * 16 : four * 16 + 16, :
            ].astype(F32)
        joined[four * 16 : four * 16 + 16, :] = joint
    sides = []
    for head in range(HEADS):
        mixed = joined[pl.ds(2 * head, SEQS, 4), :] + joined[pl.ds(2 * head + 1, SEQS, 4), :]
        mean = jnp.mean(mixed * mixed, axis=1, keepdims=True)
        sides.append((mixed * lax.rsqrt(mean + epsilon) * head_gain[...]).astype(BF16))
    head_out = jnp.concatenate(sides, axis=1)
    partial_out = jnp.dot(
        head_out, out_weight[...], preferred_element_type=F32
    ).astype(BF16)
    for dest in range(8):
        out[dest] = partial_out


def attend_call(tables, got, early_keys, keys, values, name):
    return pl.pallas_call(
        attend_kernel,
        in_specs=[VM, VM, VM, ANY, ANY],
        out_specs=VM,
        out_shape=jax.ShapeDtypeStruct((SEQS, 72, LANES), BF16),
        scratch_shapes=[
            pltpu.VMEM((SEQS - EARLY, *keys.shape[1:]), BF16),
            pltpu.VMEM(values.shape, BF16),
            pltpu.SemaphoreType.DMA((2, SEQS)),
            pltpu.VMEM((32, LANES), F32),
            pltpu.VMEM((SEQS, LANES), F32),
            pltpu.VMEM((64, 256), BF16),
            pltpu.VMEM((64, 2048), F32),
            pltpu.VMEM((64, 2048), BF16),
        ],
        compiler_params=BIG,
        name=name,
    )(tables, got, early_keys, in_hbm(keys), in_hbm(values))


def local(
    tokens,
    norm_gain,
    query_weight,
    key_weight,
    value_weight,
    out_weight,
    lambdas,
    head_gain,
    lengths,
    key_cache,
    value_cache,
):
    cache_shape = (SEQS, 2048, LANES)
    keys = key_cache.reshape(cache_shape)
    rates = np.tile(theta_base ** (-np.arange(DH // 2) / (DH // 2)), 4)
    sent, tables, early_keys = pl.pallas_call(
        project_kernel,
        in_specs=[ANY] * 9,
        out_specs=[VM] * 3,
        out_shape=[
            jax.ShapeDtypeStruct((SEQS, 40, LANES), F32),
            jax.ShapeDtypeStruct((40, LANES), F32),
            pltpu.VMEM((EARLY, *cache_shape[1:]), BF16),
        ],
        scratch_shapes=[
            pltpu.VMEM((SEQS, 256), BF16),
            pltpu.VMEM((1, 256), F32),
            pltpu.VMEM((1, SEQS), jnp.int32),
            pltpu.VMEM((1, HEADS), F32),
            pltpu.VMEM((1, LANES), F32),
            pltpu.VMEM((256, 768), BF16),
            pltpu.SemaphoreType.DMA((5,)),
            pltpu.SemaphoreType.DMA((3,)),
            pltpu.SemaphoreType.DMA((EARLY,)),
        ],
        compiler_params=SMALL,
        name="project",
    )(
        in_hbm(tokens),
        in_hbm(norm_gain.reshape(1, -1)),
        in_hbm(lengths.reshape(1, -1)),
        in_hbm(lambdas.reshape(1, -1)),
        in_hbm(jnp.asarray(rates, F32).reshape(1, -1)),
        in_hbm(query_weight),
        in_hbm(key_weight),
        in_hbm(value_weight),
        in_hbm(keys),
    )
    got = lax.all_to_all(sent, "kv", split_axis=0, concat_axis=0, tiled=True)
    shared = attend_call(
        tables, got, early_keys, keys, value_cache.reshape(cache_shape), "attend"
    )
    everyone = lax.all_to_all(shared, "kv", split_axis=0, concat_axis=0, tiled=True)
    partial_out = pl.pallas_call(
        finish_kernel,
        in_specs=[VM] * 4,
        out_specs=VM,
        out_shape=jax.ShapeDtypeStruct((8, SEQS, 256), BF16),
        scratch_shapes=[pltpu.VMEM((LANES, LANES), F32), pltpu.VMEM((64, LANES), F32)],
        compiler_params=SMALL,
        name="finish",
    )(everyone, tables, head_gain.reshape(1, -1), out_weight)
    shares = lax.all_to_all(partial_out, "tp", split_axis=0, concat_axis=0, tiled=True)
    return shares.astype(F32).sum(axis=0).astype(BF16)


def solution(mesh):
    return jax.shard_map(
        local,
        mesh=mesh,
        in_specs=(
            P(None, "kv"),
            P("kv"),
            P("kv", "tp"),
            P("kv", "tp"),
            P("kv", "tp"),
            P("tp", "kv"),
            P("tp"),
            P(),
            P(),
            P(None, "kv", "tp", None),
            P(None, "kv", "tp", None),
        ),
        out_specs=P(None, "kv"),
        check_vma=False,
    )
```

```python
import jax
import jax.numpy as jnp
import numpy as np
from jax import lax
from jax.experimental import pallas as pl
from jax.experimental.pallas import tpu as pltpu
from jax.sharding import PartitionSpec as P

D = 4096
DH = 64
HEADS = 2
SEQS = 16
LANES = 128

epsilon = 1e-05
theta_base = 500000.0
floor_value = -1e30

VM = pl.BlockSpec(memory_space=pltpu.VMEM)
SM = pl.BlockSpec(memory_space=pltpu.SMEM)
ANY = pl.BlockSpec(memory_space=pltpu.HBM)
F32 = jnp.float32
BF16 = jnp.bfloat16
EVEN = pltpu.CompilerParams(
    vmem_limit_bytes=8 * 1024 * 1024
)
SMALL = pltpu.CompilerParams(vmem_limit_bytes=8 * 1024 * 1024)
BIG = pltpu.CompilerParams(vmem_limit_bytes=30 * 1024 * 1024)


def in_hbm(x):
    return pltpu.with_memory_space_constraint(x, pltpu.HBM)


def iotas(rows):
    shape = (rows, LANES)
    return lax.broadcasted_iota(jnp.int32, shape, 0), lax.broadcasted_iota(jnp.int32, shape, 1)


def project_kernel(
    tokens_in, gain_in, lengths_in, lambdas_in, rates_in, query_in, key_in, value_in, out, tables,
    tokens, gain, lengths, lambdas, rates, weights, small, large,
):
    near = [
        pltpu.make_async_copy(source, target, small.at[n])
        for n, (source, target) in enumerate(
            (
                (tokens_in, tokens),
                (gain_in, gain),
                (lengths_in, lengths),
                (lambdas_in, lambdas),
                (rates_in, rates),
            )
        )
    ]
    far = [
        pltpu.make_async_copy(source, weights.at[:, 256 * n : 256 * n + 256], large.at[n])
        for n, source in enumerate((query_in, key_in, value_in))
    ]
    for copy in (*near, *far):
        copy.start()
    for copy in near:
        copy.wait()
    widened = tokens[...].astype(F32)
    squares = jnp.sum(widened * widened, axis=1, keepdims=True)
    normed = (widened * gain[...]).astype(BF16)
    row, lane = iotas(SEQS)
    square_row = jnp.sum(jnp.where(row == lane, squares, 0.0), axis=0, keepdims=True)
    row16 = lax.broadcasted_iota(jnp.int32, (SEQS, SEQS), 0)
    lane16 = lax.broadcasted_iota(jnp.int32, (SEQS, SEQS), 1)
    held = lengths[...].astype(F32)
    held_column = jnp.sum(jnp.where(row16 == lane16, held, 0.0), axis=1, keepdims=True)
    angles = held_column * rates[...]
    tables[0:16, :] = jnp.cos(angles)
    sine = jnp.sin(angles)
    tables[16:32, :] = jnp.where((lane // 32) % 2 == 0, -sine, sine)
    lane1 = lax.broadcasted_iota(jnp.int32, (1, LANES), 1)
    lambda_row = jnp.where((lane1 // 2) % 2 == 0, lambdas[:, 0:1], lambdas[:, 1:2])
    tables[32:40, :] = jnp.concatenate(
        [
            jnp.sum(jnp.where(row == lane // 4, held_column, 0.0), axis=0, keepdims=True),
            jnp.where(lane1 % 2 == 0, 1.0, -lambda_row),
            jnp.zeros((6, LANES), F32),
        ],
        axis=0,
    )
    for copy in far:
        copy.wait()
    products = jnp.dot(normed, weights[...], preferred_element_type=F32)
    query, key, value = products[:, :256], products[:, 256:512], products[:, 512:]
    blank = jnp.zeros((3, LANES), F32)
    for dest in range(SEQS):
        out[dest, 0:16, :] = query[:, :LANES]
        out[dest, 16:32, :] = query[:, LANES:]
        out[dest, 32:40, :] = jnp.concatenate(
            [
                square_row,
                key[dest : dest + 1, :LANES],
                key[dest : dest + 1, LANES:],
                value[dest : dest + 1, :LANES],
                value[dest : dest + 1, LANES:],
                blank,
            ],
            axis=0,
        )


def turned(x, cosine, sine):
    lane = lax.broadcasted_iota(jnp.int32, x.shape, 1)
    partner = jnp.where(
        (lane // 32) % 2 == 0, pltpu.roll(x, LANES - 32, 1), pltpu.roll(x, 32, 1)
    )
    return (x * cosine + partner * sine).astype(BF16)


def attend_kernel(
    tables, got, keys_in, values_in, out, keys, values, arrived, query_rows, scale_rows,
    asked_rows, score_rows, weight_rows,
):
    copies = []
    for kind, (source, target) in enumerate(((keys_in, keys), (values_in, values))):
        for seq in range(SEQS):
            copies.append(
                pltpu.make_async_copy(source.at[seq], target.at[seq], arrived.at[kind, seq])
            )
    for copy in copies:
        copy.start()
    me = lax.axis_index("kv")
    cosine, sine = tables[0:16, :], tables[16:32, :]
    summed = jnp.sum(got[...], axis=0)
    row, lane = iotas(SEQS)
    squares = jnp.sum(jnp.where(row == lane, summed[32:33, :], 0.0), axis=1, keepdims=True)
    scaling = jnp.broadcast_to(lax.rsqrt(squares / D + epsilon), (SEQS, LANES))
    scale_rows[...] = scaling
    for head in range(HEADS):
        turned_query = turned(
            summed[16 * head : 16 * head + 16, :] * scaling, cosine, sine
        )
        query_rows[head * SEQS : (head + 1) * SEQS, :] = turned_query.astype(F32)
    map_lanes = (lane // DH) == (row % 2)

    def row_of(head, seq):
        at = head * SEQS + seq
        return jnp.broadcast_to(query_rows[at : at + 1, :], (SEQS, LANES))

    for group in range(4):
        first = 4 * group
        left = jnp.where(
            row < 8,
            jnp.where(row < 2, row_of(0, first), row_of(1, first)),
            jnp.where(row < 10, row_of(0, first + 2), row_of(1, first + 2)),
        )
        right = jnp.where(
            row < 8,
            jnp.where(row < 6, row_of(0, first + 1), row_of(1, first + 1)),
            jnp.where(row < 14, row_of(0, first + 3), row_of(1, first + 3)),
        )
        left = jnp.where(map_lanes & (row % 8 < 4), left, 0.0)
        right = jnp.where(map_lanes & (row % 8 >= 4), right, 0.0)
        asked_rows[group * 16 : group * 16 + 16, :] = jnp.concatenate(
            [left, right], axis=1
        ).astype(BF16)

    columns = lax.broadcasted_iota(jnp.int32, (SEQS, 2048), 1)
    subs = lax.broadcasted_iota(jnp.int32, (SEQS, 2048), 0)
    own_head = (columns % 2) == ((subs // 2) % 2)
    lengths_of = tables[32:33, :].astype(jnp.int32)
    sums = [jnp.zeros((SEQS, LANES), F32)]

    def score(group):
        for copy in copies[4 * group : 4 * group + 4]:
            copy.wait()
        for pair in (2 * group, 2 * group + 1):
            at = slice(pair * 8, pair * 8 + 8)
            both_keys = jnp.concatenate([keys[2 * pair], keys[2 * pair + 1]], axis=1)
            score_rows[at, :] = lax.dot_general(
                asked_rows[at, :],
                both_keys,
                (((1,), (1,)), ((), ())),
                preferred_element_type=F32,
            )

    def weigh(group):
        at = slice(group * 16, group * 16 + 16)
        place = lane == group * 16 + row
        limit = jnp.sum(jnp.where(place, lengths_of, 0), axis=1, keepdims=True)
        visible = own_head & (columns < 2 * (limit - me * 1024))
        masked = jnp.where(visible, score_rows[at, :] * DH ** (-0.5), floor_value)
        highest = jnp.max(masked, axis=1, keepdims=True)
        weights = jnp.where(visible, jnp.exp(masked - highest), 0.0).astype(BF16)
        weight_rows[at, :] = weights
        total = jnp.sum(weights.astype(F32), axis=1, keepdims=True)
        beside = lane == 64 + group * 16 + row
        sums[0] = sums[0] + jnp.where(place, highest, jnp.where(beside, total, 0.0))

    def value(pair):
        return sides_of(weighed(pair, slice(0, 2048)))

    def weighed(pair, part):
        both_values = jnp.concatenate(
            [values[2 * pair, part, :], values[2 * pair + 1, part, :]], axis=1
        )
        return jnp.dot(
            weight_rows[pair * 8 : pair * 8 + 8, part],
            both_values,
            preferred_element_type=F32,
        )

    def sides_of(valued):
        return jnp.where(row[:8] < 4, valued[:, :LANES], valued[:, LANES:])

    def arrive(seqs):
        for seq in seqs:
            copies[SEQS + seq].wait()

    def give(group, parts):
        sixteen = jnp.concatenate(parts, axis=0).astype(BF16)
        for dest in range(SEQS):
            out[dest, group * 16 : group * 16 + 16, :] = sixteen

    score(0)
    for group in range(1, 4):
        score(group)
        weigh(group - 1)
    arrive(range(8))
    give(0, [value(0), value(1)])
    weigh(3)
    give(1, [value(2), value(3)])
    scale = scale_rows[pl.ds(me, 1), :]
    row_cosine = tables[pl.ds(me, 1), :]
    row_sine = tables[pl.ds(SEQS + me, 1), :]
    lane1 = lax.broadcasted_iota(jnp.int32, (1, LANES), 1)
    fresh_scores = jnp.zeros((1, LANES), F32)
    for head in range(HEADS):
        query = query_rows[pl.ds(head * SEQS + me, 1), :]
        fresh_key = turned(summed[33 + head : 34 + head, :] * scale, row_cosine, row_sine)
        product = query * fresh_key.astype(F32)
        for side in range(2):
            fresh = jnp.sum(
                jnp.where(lane1 // DH == side, product, 0.0), axis=1, keepdims=True
            ) * DH ** (-0.5)
            at = me * 4 + head * 2 + side
            fresh_scores = fresh_scores + jnp.where(lane1 == at, fresh, 0.0)
    fresh_value = (summed[35:37, :] * scale).astype(BF16).astype(F32)
    tail = jnp.concatenate(
        [
            *thirds(jnp.sum(sums[0], axis=0, keepdims=True)),
            *thirds(fresh_scores),
            fresh_value,
        ],
        axis=0,
    ).astype(BF16)
    for dest in range(SEQS):
        out[dest, 64:72, :] = tail
    for group in range(2, 3):
        arrive(range(4 * group, 4 * group + 4))
        give(group, [value(2 * group), value(2 * group + 1)])
    arrive(range(12, 16))
    give(3, [value(6), value(7)])


def thirds(x):
    high = x.astype(BF16).astype(F32)
    middle = (x - high).astype(BF16).astype(F32)
    return high, middle, x - high - middle


def finish_kernel(got, tables, head_gain, out_weight, out, factors, joined):
    rows16, _ = iotas(SEQS)
    tails = got[:, 64:72, :].astype(F32)

    def whole(at):
        return tails[:, at, :] + tails[:, at + 1, :] + tails[:, at + 2, :]

    left = lax.broadcasted_iota(jnp.int32, (1, LANES), 1) < 64
    both = whole(0)
    maxima = jnp.where(left, both, 0.0)
    totals = jnp.where(left, pltpu.roll(both, 64, 1), 1.0)
    fresh = jnp.sum(whole(3), axis=0, keepdims=True)
    block = tables[32:33, :].astype(jnp.int32) // 1024
    in_block = jnp.max(
        jnp.where(rows16 == block, maxima, floor_value), axis=0, keepdims=True
    )
    in_block = jnp.maximum(in_block, fresh)
    top = jnp.maximum(jnp.max(maxima, axis=0, keepdims=True), fresh)
    factor = jnp.exp(maxima - top)
    fresh_factor = jnp.exp(fresh - in_block).astype(BF16).astype(F32) * jnp.exp(in_block - top)
    total = jnp.sum(totals * factor, axis=0, keepdims=True) + fresh_factor
    part = tables[33:34, :] / total
    factors[...] = jnp.zeros((LANES, LANES), F32)
    factors[0:SEQS, :] = factor * part
    factors[SEQS : SEQS + 1, :] = fresh_factor * part
    columns = factors[...].T
    sub, _ = iotas(16)
    for four in range(SEQS // 4):
        here = columns[four * 16 : four * 16 + 16, :]
        fresh_value = jnp.zeros((16, LANES), F32)
        for n in range(8):
            line = tails[four * 4 + n // 2, 6 + n % 2 : 7 + n % 2, :]
            fresh_value = jnp.where(sub // 2 == n, line, fresh_value)
        joint = here[:, SEQS : SEQS + 1] * fresh_value
        for peer in range(SEQS):
            joint = joint + here[:, peer : peer + 1] * got[
                peer, four * 16 : four * 16 + 16, :
            ].astype(F32)
        joined[four * 16 : four * 16 + 16, :] = joint
    sides = []
    for head in range(HEADS):
        mixed = joined[pl.ds(2 * head, SEQS, 4), :] + joined[pl.ds(2 * head + 1, SEQS, 4), :]
        mean = jnp.mean(mixed * mixed, axis=1, keepdims=True)
        sides.append((mixed * lax.rsqrt(mean + epsilon) * head_gain[...]).astype(BF16))
    head_out = jnp.concatenate(sides, axis=1)
    partial_out = jnp.dot(
        head_out, out_weight[...], preferred_element_type=F32
    ).astype(BF16)
    for dest in range(8):
        out[dest] = partial_out


def attend_call(tables, got, keys, values, name):
    return pl.pallas_call(
        attend_kernel,
        in_specs=[VM, VM, ANY, ANY],
        out_specs=VM,
        out_shape=jax.ShapeDtypeStruct((SEQS, 72, LANES), BF16),
        scratch_shapes=[
            pltpu.VMEM(keys.shape, BF16),
            pltpu.VMEM(values.shape, BF16),
            pltpu.SemaphoreType.DMA((2, SEQS)),
            pltpu.VMEM((32, LANES), F32),
            pltpu.VMEM((SEQS, LANES), F32),
            pltpu.VMEM((64, 256), BF16),
            pltpu.VMEM((64, 2048), F32),
            pltpu.VMEM((64, 2048), BF16),
        ],
        compiler_params=BIG,
        name=name,
    )(tables, got, in_hbm(keys), in_hbm(values))


def local(
    tokens,
    norm_gain,
    query_weight,
    key_weight,
    value_weight,
    out_weight,
    lambdas,
    head_gain,
    lengths,
    key_cache,
    value_cache,
):
    rates = np.tile(theta_base ** (-np.arange(DH // 2) / (DH // 2)), 4)
    sent, tables = pl.pallas_call(
        project_kernel,
        in_specs=[ANY] * 8,
        out_specs=[VM, VM],
        out_shape=[
            jax.ShapeDtypeStruct((SEQS, 40, LANES), F32),
            jax.ShapeDtypeStruct((40, LANES), F32),
        ],
        scratch_shapes=[
            pltpu.VMEM((SEQS, 256), BF16),
            pltpu.VMEM((1, 256), F32),
            pltpu.VMEM((1, SEQS), jnp.int32),
            pltpu.VMEM((1, HEADS), F32),
            pltpu.VMEM((1, LANES), F32),
            pltpu.VMEM((256, 768), BF16),
            pltpu.SemaphoreType.DMA((5,)),
            pltpu.SemaphoreType.DMA((3,)),
        ],
        compiler_params=EVEN,
        name="project",
    )(
        in_hbm(tokens),
        in_hbm(norm_gain.reshape(1, -1)),
        in_hbm(lengths.reshape(1, -1)),
        in_hbm(lambdas.reshape(1, -1)),
        in_hbm(jnp.asarray(rates, F32).reshape(1, -1)),
        in_hbm(query_weight),
        in_hbm(key_weight),
        in_hbm(value_weight),
    )
    got = lax.all_to_all(sent, "kv", split_axis=0, concat_axis=0, tiled=True)
    cache_shape = (SEQS, 2048, LANES)
    shared = attend_call(
        tables, got, key_cache.reshape(cache_shape), value_cache.reshape(cache_shape), "attend"
    )
    everyone = lax.all_to_all(shared, "kv", split_axis=0, concat_axis=0, tiled=True)
    partial_out = pl.pallas_call(
        finish_kernel,
        in_specs=[VM] * 4,
        out_specs=VM,
        out_shape=jax.ShapeDtypeStruct((8, SEQS, 256), BF16),
        scratch_shapes=[pltpu.VMEM((LANES, LANES), F32), pltpu.VMEM((64, LANES), F32)],
        compiler_params=SMALL,
        name="finish",
    )(everyone, tables, head_gain.reshape(1, -1), out_weight)
    shares = lax.all_to_all(partial_out, "tp", split_axis=0, concat_axis=0, tiled=True)
    return shares.astype(F32).sum(axis=0).astype(BF16)


def solution(mesh):
    return jax.shard_map(
        local,
        mesh=mesh,
        in_specs=(
            P(None, "kv"),
            P("kv"),
            P("kv", "tp"),
            P("kv", "tp"),
            P("kv", "tp"),
            P("tp", "kv"),
            P("tp"),
            P(),
            P(),
            P(None, "kv", "tp", None),
            P(None, "kv", "tp", None),
        ),
        out_specs=P(None, "kv"),
        check_vma=False,
    )
```

```python
import jax
import jax.numpy as jnp
import numpy as np
from jax import lax
from jax.experimental import pallas as pl
from jax.experimental.pallas import tpu as pltpu
from jax.sharding import PartitionSpec as P

D = 4096
DH = 64
HEADS = 2
SEQS = 16
LANES = 128

epsilon = 1e-05
theta_base = 500000.0
floor_value = -1e30

VM = pl.BlockSpec(memory_space=pltpu.VMEM)
SM = pl.BlockSpec(memory_space=pltpu.SMEM)
ANY = pl.BlockSpec(memory_space=pltpu.HBM)
F32 = jnp.float32
BF16 = jnp.bfloat16
EVEN = pltpu.CompilerParams(
    vmem_limit_bytes=8 * 1024 * 1024
)
SMALL = pltpu.CompilerParams(vmem_limit_bytes=8 * 1024 * 1024)
BIG = pltpu.CompilerParams(vmem_limit_bytes=30 * 1024 * 1024)


def in_hbm(x):
    return pltpu.with_memory_space_constraint(x, pltpu.HBM)


def iotas(rows):
    shape = (rows, LANES)
    return lax.broadcasted_iota(jnp.int32, shape, 0), lax.broadcasted_iota(jnp.int32, shape, 1)


def project_kernel(
    tokens_in, gain_in, lengths_in, lambdas_in, rates_in, query_in, key_in, value_in, out, tables,
    tokens, gain, lengths, lambdas, rates, weights, small, large,
):
    near = [
        pltpu.make_async_copy(source, target, small.at[n])
        for n, (source, target) in enumerate(
            (
                (tokens_in, tokens),
                (gain_in, gain),
                (lengths_in, lengths),
                (lambdas_in, lambdas),
                (rates_in, rates),
            )
        )
    ]
    far = [
        pltpu.make_async_copy(source, weights.at[:, 256 * n : 256 * n + 256], large.at[n])
        for n, source in enumerate((query_in, key_in, value_in))
    ]
    for copy in (*near, *far):
        copy.start()
    for copy in near:
        copy.wait()
    widened = tokens[...].astype(F32)
    squares = jnp.sum(widened * widened, axis=1, keepdims=True)
    normed = (widened * gain[...]).astype(BF16)
    row, lane = iotas(SEQS)
    square_row = jnp.sum(jnp.where(row == lane, squares, 0.0), axis=0, keepdims=True)
    row16 = lax.broadcasted_iota(jnp.int32, (SEQS, SEQS), 0)
    lane16 = lax.broadcasted_iota(jnp.int32, (SEQS, SEQS), 1)
    held = lengths[...].astype(F32)
    held_column = jnp.sum(jnp.where(row16 == lane16, held, 0.0), axis=1, keepdims=True)
    angles = held_column * rates[...]
    tables[0:16, :] = jnp.cos(angles)
    sine = jnp.sin(angles)
    tables[16:32, :] = jnp.where((lane // 32) % 2 == 0, -sine, sine)
    lane1 = lax.broadcasted_iota(jnp.int32, (1, LANES), 1)
    lambda_row = jnp.where((lane1 // 2) % 2 == 0, lambdas[:, 0:1], lambdas[:, 1:2])
    tables[32:40, :] = jnp.concatenate(
        [
            jnp.sum(jnp.where(row == lane // 4, held_column, 0.0), axis=0, keepdims=True),
            jnp.where(lane1 % 2 == 0, 1.0, -lambda_row),
            jnp.zeros((6, LANES), F32),
        ],
        axis=0,
    )
    for copy in far:
        copy.wait()
    products = jnp.dot(normed, weights[...], preferred_element_type=F32)
    query, key, value = products[:, :256], products[:, 256:512], products[:, 512:]
    blank = jnp.zeros((3, LANES), F32)
    for dest in range(SEQS):
        out[dest, 0:16, :] = query[:, :LANES]
        out[dest, 16:32, :] = query[:, LANES:]
        out[dest, 32:40, :] = jnp.concatenate(
            [
                square_row,
                key[dest : dest + 1, :LANES],
                key[dest : dest + 1, LANES:],
                value[dest : dest + 1, :LANES],
                value[dest : dest + 1, LANES:],
                blank,
            ],
            axis=0,
        )


def turned(x, cosine, sine):
    lane = lax.broadcasted_iota(jnp.int32, x.shape, 1)
    partner = jnp.where(
        (lane // 32) % 2 == 0, pltpu.roll(x, LANES - 32, 1), pltpu.roll(x, 32, 1)
    )
    return (x * cosine + partner * sine).astype(BF16)


def attend_kernel(
    tables, got, keys_in, values_in, out, keys, values, arrived, query_rows, scale_rows,
    asked_rows, score_rows, weight_rows,
):
    copies = []
    for kind, (source, target) in enumerate(((keys_in, keys), (values_in, values))):
        for seq in range(SEQS):
            copies.append(
                pltpu.make_async_copy(source.at[seq], target.at[seq], arrived.at[kind, seq])
            )
    for copy in copies:
        copy.start()
    me = lax.axis_index("kv")
    cosine, sine = tables[0:16, :], tables[16:32, :]
    summed = jnp.sum(got[...], axis=0)
    row, lane = iotas(SEQS)
    squares = jnp.sum(jnp.where(row == lane, summed[32:33, :], 0.0), axis=1, keepdims=True)
    scaling = jnp.broadcast_to(lax.rsqrt(squares / D + epsilon), (SEQS, LANES))
    scale_rows[...] = scaling
    for head in range(HEADS):
        turned_query = turned(
            summed[16 * head : 16 * head + 16, :] * scaling, cosine, sine
        )
        query_rows[head * SEQS : (head + 1) * SEQS, :] = turned_query.astype(F32)
    map_lanes = (lane // DH) == (row % 2)

    def row_of(head, seq):
        at = head * SEQS + seq
        return jnp.broadcast_to(query_rows[at : at + 1, :], (SEQS, LANES))

    for group in range(4):
        first = 4 * group
        left = jnp.where(
            row < 8,
            jnp.where(row < 2, row_of(0, first), row_of(1, first)),
            jnp.where(row < 10, row_of(0, first + 2), row_of(1, first + 2)),
        )
        right = jnp.where(
            row < 8,
            jnp.where(row < 6, row_of(0, first + 1), row_of(1, first + 1)),
            jnp.where(row < 14, row_of(0, first + 3), row_of(1, first + 3)),
        )
        left = jnp.where(map_lanes & (row % 8 < 4), left, 0.0)
        right = jnp.where(map_lanes & (row % 8 >= 4), right, 0.0)
        asked_rows[group * 16 : group * 16 + 16, :] = jnp.concatenate(
            [left, right], axis=1
        ).astype(BF16)

    columns = lax.broadcasted_iota(jnp.int32, (SEQS, 2048), 1)
    subs = lax.broadcasted_iota(jnp.int32, (SEQS, 2048), 0)
    own_head = (columns % 2) == ((subs // 2) % 2)
    lengths_of = tables[32:33, :].astype(jnp.int32)
    sums = [jnp.zeros((SEQS, LANES), F32)]

    def score(group):
        for copy in copies[4 * group : 4 * group + 4]:
            copy.wait()
        for pair in (2 * group, 2 * group + 1):
            at = slice(pair * 8, pair * 8 + 8)
            both_keys = jnp.concatenate([keys[2 * pair], keys[2 * pair + 1]], axis=1)
            score_rows[at, :] = lax.dot_general(
                asked_rows[at, :],
                both_keys,
                (((1,), (1,)), ((), ())),
                preferred_element_type=F32,
            )

    def weigh(group):
        at = slice(group * 16, group * 16 + 16)
        place = lane == group * 16 + row
        limit = jnp.sum(jnp.where(place, lengths_of, 0), axis=1, keepdims=True)
        visible = own_head & (columns < 2 * (limit - me * 1024))
        masked = jnp.where(visible, score_rows[at, :] * DH ** (-0.5), floor_value)
        highest = jnp.max(masked, axis=1, keepdims=True)
        weights = jnp.where(visible, jnp.exp(masked - highest), 0.0).astype(BF16)
        weight_rows[at, :] = weights
        total = jnp.sum(weights.astype(F32), axis=1, keepdims=True)
        beside = lane == 64 + group * 16 + row
        sums[0] = sums[0] + jnp.where(place, highest, jnp.where(beside, total, 0.0))

    def value(pair):
        return sides_of(weighed(pair, slice(0, 2048)))

    def weighed(pair, part):
        both_values = jnp.concatenate(
            [values[2 * pair, part, :], values[2 * pair + 1, part, :]], axis=1
        )
        return jnp.dot(
            weight_rows[pair * 8 : pair * 8 + 8, part],
            both_values,
            preferred_element_type=F32,
        )

    def sides_of(valued):
        return jnp.where(row[:8] < 4, valued[:, :LANES], valued[:, LANES:])

    def arrive(seqs):
        for seq in seqs:
            copies[SEQS + seq].wait()

    def give(group, parts):
        sixteen = jnp.concatenate(parts, axis=0).astype(BF16)
        for dest in range(SEQS):
            out[dest, group * 16 : group * 16 + 16, :] = sixteen

    score(0)
    for group in range(1, 4):
        score(group)
        weigh(group - 1)
    arrive(range(4))
    give(0, [value(0), value(1)])
    weigh(3)
    scale = scale_rows[pl.ds(me, 1), :]
    row_cosine = tables[pl.ds(me, 1), :]
    row_sine = tables[pl.ds(SEQS + me, 1), :]
    lane1 = lax.broadcasted_iota(jnp.int32, (1, LANES), 1)
    fresh_scores = jnp.zeros((1, LANES), F32)
    for head in range(HEADS):
        query = query_rows[pl.ds(head * SEQS + me, 1), :]
        fresh_key = turned(summed[33 + head : 34 + head, :] * scale, row_cosine, row_sine)
        product = query * fresh_key.astype(F32)
        for side in range(2):
            fresh = jnp.sum(
                jnp.where(lane1 // DH == side, product, 0.0), axis=1, keepdims=True
            ) * DH ** (-0.5)
            at = me * 4 + head * 2 + side
            fresh_scores = fresh_scores + jnp.where(lane1 == at, fresh, 0.0)
    fresh_value = (summed[35:37, :] * scale).astype(BF16).astype(F32)
    tail = jnp.concatenate(
        [
            *thirds(jnp.sum(sums[0], axis=0, keepdims=True)),
            *thirds(fresh_scores),
            fresh_value,
        ],
        axis=0,
    ).astype(BF16)
    for dest in range(SEQS):
        out[dest, 64:72, :] = tail
    for group in range(1, 3):
        arrive(range(4 * group, 4 * group + 4))
        give(group, [value(2 * group), value(2 * group + 1)])
    arrive(range(12, 16))
    give(3, [value(6), value(7)])


def thirds(x):
    high = x.astype(BF16).astype(F32)
    middle = (x - high).astype(BF16).astype(F32)
    return high, middle, x - high - middle


def finish_kernel(got, tables, head_gain, out_weight, out, factors, joined):
    rows16, _ = iotas(SEQS)
    tails = got[:, 64:72, :].astype(F32)

    def whole(at):
        return tails[:, at, :] + tails[:, at + 1, :] + tails[:, at + 2, :]

    left = lax.broadcasted_iota(jnp.int32, (1, LANES), 1) < 64
    both = whole(0)
    maxima = jnp.where(left, both, 0.0)
    totals = jnp.where(left, pltpu.roll(both, 64, 1), 1.0)
    fresh = jnp.sum(whole(3), axis=0, keepdims=True)
    block = tables[32:33, :].astype(jnp.int32) // 1024
    in_block = jnp.max(
        jnp.where(rows16 == block, maxima, floor_value), axis=0, keepdims=True
    )
    in_block = jnp.maximum(in_block, fresh)
    top = jnp.maximum(jnp.max(maxima, axis=0, keepdims=True), fresh)
    factor = jnp.exp(maxima - top)
    fresh_factor = jnp.exp(fresh - in_block).astype(BF16).astype(F32) * jnp.exp(in_block - top)
    total = jnp.sum(totals * factor, axis=0, keepdims=True) + fresh_factor
    part = tables[33:34, :] / total
    factors[...] = jnp.zeros((LANES, LANES), F32)
    factors[0:SEQS, :] = factor * part
    factors[SEQS : SEQS + 1, :] = fresh_factor * part
    columns = factors[...].T
    sub, _ = iotas(16)
    for four in range(SEQS // 4):
        here = columns[four * 16 : four * 16 + 16, :]
        fresh_value = jnp.zeros((16, LANES), F32)
        for n in range(8):
            line = tails[four * 4 + n // 2, 6 + n % 2 : 7 + n % 2, :]
            fresh_value = jnp.where(sub // 2 == n, line, fresh_value)
        joint = here[:, SEQS : SEQS + 1] * fresh_value
        for peer in range(SEQS):
            joint = joint + here[:, peer : peer + 1] * got[
                peer, four * 16 : four * 16 + 16, :
            ].astype(F32)
        joined[four * 16 : four * 16 + 16, :] = joint
    sides = []
    for head in range(HEADS):
        mixed = joined[pl.ds(2 * head, SEQS, 4), :] + joined[pl.ds(2 * head + 1, SEQS, 4), :]
        mean = jnp.mean(mixed * mixed, axis=1, keepdims=True)
        sides.append((mixed * lax.rsqrt(mean + epsilon) * head_gain[...]).astype(BF16))
    head_out = jnp.concatenate(sides, axis=1)
    partial_out = jnp.dot(
        head_out, out_weight[...], preferred_element_type=F32
    ).astype(BF16)
    for dest in range(8):
        out[dest] = partial_out


def attend_call(tables, got, keys, values, name):
    return pl.pallas_call(
        attend_kernel,
        in_specs=[VM, VM, ANY, ANY],
        out_specs=VM,
        out_shape=jax.ShapeDtypeStruct((SEQS, 72, LANES), BF16),
        scratch_shapes=[
            pltpu.VMEM(keys.shape, BF16),
            pltpu.VMEM(values.shape, BF16),
            pltpu.SemaphoreType.DMA((2, SEQS)),
            pltpu.VMEM((32, LANES), F32),
            pltpu.VMEM((SEQS, LANES), F32),
            pltpu.VMEM((64, 256), BF16),
            pltpu.VMEM((64, 2048), F32),
            pltpu.VMEM((64, 2048), BF16),
        ],
        compiler_params=BIG,
        name=name,
    )(tables, got, in_hbm(keys), in_hbm(values))


def local(
    tokens,
    norm_gain,
    query_weight,
    key_weight,
    value_weight,
    out_weight,
    lambdas,
    head_gain,
    lengths,
    key_cache,
    value_cache,
):
    rates = np.tile(theta_base ** (-np.arange(DH // 2) / (DH // 2)), 4)
    sent, tables = pl.pallas_call(
        project_kernel,
        in_specs=[ANY] * 8,
        out_specs=[VM, VM],
        out_shape=[
            jax.ShapeDtypeStruct((SEQS, 40, LANES), F32),
            jax.ShapeDtypeStruct((40, LANES), F32),
        ],
        scratch_shapes=[
            pltpu.VMEM((SEQS, 256), BF16),
            pltpu.VMEM((1, 256), F32),
            pltpu.VMEM((1, SEQS), jnp.int32),
            pltpu.VMEM((1, HEADS), F32),
            pltpu.VMEM((1, LANES), F32),
            pltpu.VMEM((256, 768), BF16),
            pltpu.SemaphoreType.DMA((5,)),
            pltpu.SemaphoreType.DMA((3,)),
        ],
        compiler_params=EVEN,
        name="project",
    )(
        in_hbm(tokens),
        in_hbm(norm_gain.reshape(1, -1)),
        in_hbm(lengths.reshape(1, -1)),
        in_hbm(lambdas.reshape(1, -1)),
        in_hbm(jnp.asarray(rates, F32).reshape(1, -1)),
        in_hbm(query_weight),
        in_hbm(key_weight),
        in_hbm(value_weight),
    )
    got = lax.all_to_all(sent, "kv", split_axis=0, concat_axis=0, tiled=True)
    cache_shape = (SEQS, 2048, LANES)
    shared = attend_call(
        tables, got, key_cache.reshape(cache_shape), value_cache.reshape(cache_shape), "attend"
    )
    everyone = lax.all_to_all(shared, "kv", split_axis=0, concat_axis=0, tiled=True)
    partial_out = pl.pallas_call(
        finish_kernel,
        in_specs=[VM] * 4,
        out_specs=VM,
        out_shape=jax.ShapeDtypeStruct((8, SEQS, 256), BF16),
        scratch_shapes=[pltpu.VMEM((LANES, LANES), F32), pltpu.VMEM((64, LANES), F32)],
        compiler_params=SMALL,
        name="finish",
    )(everyone, tables, head_gain.reshape(1, -1), out_weight)
    shares = lax.all_to_all(partial_out, "tp", split_axis=0, concat_axis=0, tiled=True)
    return shares.astype(F32).sum(axis=0).astype(BF16)


def solution(mesh):
    return jax.shard_map(
        local,
        mesh=mesh,
        in_specs=(
            P(None, "kv"),
            P("kv"),
            P("kv", "tp"),
            P("kv", "tp"),
            P("kv", "tp"),
            P("tp", "kv"),
            P("tp"),
            P(),
            P(),
            P(None, "kv", "tp", None),
            P(None, "kv", "tp", None),
        ),
        out_specs=P(None, "kv"),
        check_vma=False,
    )
```
